512 devices in a mesh: sp: 128 (over z, y, core), tp: 4 (over x).
Axes of the slice: x: 4, y: 8, z: 8, core: 2. Of those that a mesh axis runs over, the one named last changes fastest.
Arguments:
- tokens: bfloat16 [32768, 2048], P(('sp', 'tp')), may hold values from -6 to 6
- pre_gain: float32 [2048], replicated, may hold values from 0.1 to 1.9
- w_query_ret: bfloat16 [2048, 768], P('sp', 'tp'), may hold values from -0.125 to 0.125
- w_key_ret: bfloat16 [2048, 768], P('sp', 'tp'), may hold values from -0.125 to 0.125
- w_value_ret: bfloat16 [2048, 768], P('sp', 'tp'), may hold values from -0.125 to 0.125
- w_query_att: bfloat16 [2048, 768], P('sp', 'tp'), may hold values from -0.5 to 0.5
- w_key_att: bfloat16 [2048, 256], P('sp', 'tp'), may hold values from -0.125 to 0.125
- w_value_att: bfloat16 [2048, 256], P('sp', 'tp'), may hold values from -0.125 to 0.125
- w_out_ret: bfloat16 [768, 2048], P('tp', 'sp'), may hold values from -0.15625 to 0.15625
- w_out_att: bfloat16 [768, 2048], P('tp', 'sp'), may hold values from -0.15625 to 0.15625
- retain_log: float32 [32768, 12], P('sp', 'tp')
- forget_total: float32 [12, 32768], P('tp'), as said below
Outputs:
- mixed: bfloat16 [32768, 2048], P(('sp', 'tp'))
The draws below stay inside these ranges and needn't reach their ends.
Inputs may be any that keep to these rules, and one draw needn't show every extreme that they name: `forget_total`: never rises along positions.
All inputs are finite; a program needn't handle non-finite values.
Results may differ from the reference program's by a relative error of at most 0.019.
Values may be sent and summed in bfloat16 or wider, within the bound.
No kernel may reach another device: no remote copies, remote signals or barrier semaphores. Data moves between devices by JAX's collectives and lax.ppermute only.
A program may use at most 64 MiB of HBM per device.

```python
import math
import jax
import jax.numpy as jnp
from jax import lax

D = 2048
HEAD = 64
R_HEADS = 12
F_HEADS = 12
KV_HEADS = 4
SPAN = 256
TOK_DEV = 256
TOKENS = 32768
N_TP = 4


def log_rates(key, heads):
    keys = jax.random.split(key, 6)
    order = jax.random.permutation(keys[0], heads)
    slow = order < heads // 2
    blocks = TOKENS // TOK_DEV
    spread = jnp.exp(jax.random.uniform(keys[1], (blocks, heads), jnp.float32, math.log(0.4), math.log(2.5)))
    spread = jnp.repeat(spread, TOK_DEV, axis=0)
    rough = jax.random.uniform(keys[2], (TOKENS, heads), jnp.float32, 0.5, 1.5)
    fast = jnp.exp(jax.random.uniform(keys[3], (heads,), jnp.float32, math.log(0.03), math.log(0.1)))
    base = jnp.where(slow, 0.2 * math.log(10.0) / TOKENS, fast)
    rates = base[None, :] * spread * rough
    places = jax.random.randint(keys[4], (2, heads), 0, TOKENS)
    losses = jax.random.uniform(keys[5], (2, heads), jnp.float32, 0.2, 0.4)
    struck = jnp.arange(TOKENS, dtype=jnp.int32)[:, None, None] == places[None, :, :]
    rates = rates - jnp.sum(jnp.where(struck, jnp.log(1.0 - losses)[None, :, :], 0.0), axis=1)
    return -rates


def draw_retain_log(key, part):
    return log_rates(jax.random.fold_in(key, 11), R_HEADS)


def draw_forget_total(key, part):
    return jnp.transpose(jnp.cumsum(log_rates(jax.random.fold_in(key, 23), F_HEADS), axis=0))


def block_levels(own_key, extent, cuts, least, high):
    factor_of, own = 1.0, jax.random.fold_in(own_key, 6)
    for dim, shards_of in cuts:
        heights = jnp.exp(jax.random.uniform(jax.random.fold_in(own, dim), (shards_of,), jnp.float32, least / len(cuts), high / len(cuts)))
        factor_of = factor_of * jnp.repeat(heights, extent[dim] // shards_of).reshape([-1 if axis == dim else 1 for axis in range(len(extent))])
    return factor_of


def scatter_about(stream_key, dims, deviation, reach, cuts=(), kind=jnp.bfloat16):
    values = deviation * jax.random.normal(stream_key, dims, jnp.float32)
    if cuts:
        values = values * block_levels(stream_key, dims, cuts, -0.22, 0.18)
    return jnp.clip(values, -reach, reach).astype(kind)


def setup_inputs(seed: int = 0) -> dict:
    seeds = jax.random.split(jax.random.key(seed), 13)
    tokens = scatter_about(seeds[0], (TOKENS, D), 1.0, 6.0, ((0, 512),))
    pre_gain = jnp.clip(1.0 + 0.18 * jax.random.normal(seeds[1], (D,), jnp.float32), 0.1, 1.9)
    w_query_ret = scatter_about(seeds[2], (D, R_HEADS * HEAD), D ** -0.5, 0.125, ((0, 128), (1, 4)))
    w_key_ret = scatter_about(seeds[3], (D, R_HEADS * HEAD), D ** -0.5, 0.125, ((0, 128), (1, 4)))
    w_value_ret = scatter_about(seeds[4], (D, R_HEADS * HEAD), D ** -0.5, 0.125, ((0, 128), (1, 4)))
    w_query_att = scatter_about(seeds[5], (D, F_HEADS * HEAD), (D // 16) ** -0.5, 0.5, ((0, 128), (1, 4)))
    w_key_att = scatter_about(seeds[6], (D, KV_HEADS * HEAD), D ** -0.5, 0.125, ((0, 128), (1, 4)))
    w_value_att = scatter_about(seeds[7], (D, KV_HEADS * HEAD), D ** -0.5, 0.125, ((0, 128), (1, 4)))
    w_out_ret = scatter_about(seeds[8], (R_HEADS * HEAD, D), (2 * R_HEADS * HEAD) ** -0.5, 0.15625, ((0, 4), (1, 128)))
    w_out_att = scatter_about(seeds[9], (F_HEADS * HEAD, D), (2 * F_HEADS * HEAD) ** -0.5, 0.15625, ((0, 4), (1, 128)))
    retain_log = draw_retain_log(jax.random.fold_in(seeds[12], 71), 0)
    forget_total = draw_forget_total(jax.random.fold_in(seeds[12], 71), 0)
    return dict(tokens=tokens, pre_gain=pre_gain, w_query_ret=w_query_ret, w_key_ret=w_key_ret, w_value_ret=w_value_ret, w_query_att=w_query_att, w_key_att=w_key_att, w_value_att=w_value_att, w_out_ret=w_out_ret, w_out_att=w_out_att, retain_log=retain_log, forget_total=forget_total)


EPS = 1e-06
THETA = 10000.0

def rotate(field, positions):
    half = field.shape[-1] // 2
    inverse = THETA ** (-jnp.arange(half, dtype=jnp.float32) / half)
    angles = positions[:, None] * inverse[None, :]
    cosine = jnp.cos(angles)[:, None, :]
    sine = jnp.sin(angles)[:, None, :]
    first_half = field[..., :half]
    second_half = field[..., half:]
    return jnp.concatenate([first_half * cosine - second_half * sine, first_half * sine + second_half * cosine], axis=-1)

def head_norm(values):
    centre = lax.optimization_barrier(jnp.mean(values, axis=-1, keepdims=True))
    spread = lax.optimization_barrier(jnp.mean(jnp.square(values - centre), axis=-1, keepdims=True))
    return (values - centre) * lax.rsqrt(spread + EPS)

def lowered(values):
    return lax.optimization_barrier(values.astype(jnp.bfloat16)).astype(jnp.float32)

def retain_block(state, inputs):
    query, key_rows, value_rows, logs = inputs
    within = jnp.cumsum(logs, axis=0)
    span = logs.shape[0]
    causal = jnp.arange(span)[:, None] >= jnp.arange(span)[None, :]
    scores = jnp.einsum('thd,shd->hts', query.astype(jnp.float32), key_rows.astype(jnp.float32))
    gap = jnp.where(causal, jnp.transpose(within)[:, :, None] - jnp.transpose(within)[:, None, :], 0.0)
    weights = jnp.where(causal, scores * jnp.exp(gap), 0.0).astype(jnp.bfloat16)
    local = jnp.einsum('hts,shd->thd', weights.astype(jnp.float32), value_rows.astype(jnp.float32))
    lifted = lowered(query.astype(jnp.float32) * jnp.exp(within)[:, :, None])
    carried = jnp.einsum('thd,hde->the', lifted, lowered(state))
    last = within[-1]
    faded = lowered(key_rows.astype(jnp.float32) * jnp.exp(last[None, :] - within)[:, :, None])
    update = jnp.einsum('shd,she->hde', faded, value_rows.astype(jnp.float32))
    return (jnp.exp(last)[:, None, None] * state + update, local + carried)

def project(normed, weight):
    return jnp.dot(normed, weight, preferred_element_type=jnp.float32)

def reference(tokens, pre_gain, w_query_ret, w_key_ret, w_value_ret, w_query_att, w_key_att, w_value_att, w_out_ret, w_out_att, retain_log, forget_total):
    rows = tokens.astype(jnp.float32)
    normed = (rows * lax.rsqrt(lax.optimization_barrier(jnp.mean(rows * rows, axis=-1, keepdims=True)) + EPS) * pre_gain.astype(jnp.float32)).astype(jnp.bfloat16)
    positions = jnp.arange(TOKENS, dtype=jnp.int32).astype(jnp.float32)
    shape = (TOKENS, R_HEADS, HEAD)
    ret_query = (rotate(project(normed, w_query_ret).reshape(shape), positions) * HEAD ** (-0.5)).astype(jnp.bfloat16)
    ret_key = rotate(project(normed, w_key_ret).reshape(shape), positions).astype(jnp.bfloat16)
    ret_value = project(normed, w_value_ret).astype(jnp.bfloat16).reshape(shape)
    blocks = TOKENS // SPAN
    start_state = jnp.zeros((R_HEADS, HEAD, HEAD), jnp.float32)
    inputs = (ret_query.reshape(blocks, SPAN, R_HEADS, HEAD), ret_key.reshape(blocks, SPAN, R_HEADS, HEAD), ret_value.reshape(blocks, SPAN, R_HEADS, HEAD), retain_log.reshape(blocks, SPAN, R_HEADS))
    _, inside = lax.scan(retain_block, start_state, inputs)
    retained = head_norm(inside.reshape(shape)).astype(jnp.bfloat16).reshape(TOKENS, R_HEADS * HEAD)
    group = F_HEADS // KV_HEADS
    pieces = TOKENS // TOK_DEV
    att_query = (project(normed, w_query_att) * HEAD ** (-0.5)).astype(jnp.bfloat16).reshape(pieces, TOK_DEV, KV_HEADS, group, HEAD)
    att_key = project(normed, w_key_att).astype(jnp.bfloat16).reshape(pieces, TOK_DEV, KV_HEADS, HEAD)
    att_value = project(normed, w_value_att).astype(jnp.bfloat16).reshape(pieces, TOK_DEV, KV_HEADS, HEAD)
    gates = forget_total.reshape(KV_HEADS, group, pieces, TOK_DEV)
    local_places = jnp.arange(TOK_DEV, dtype=jnp.int32)

    def attend_block(index):
        query_rows = lax.dynamic_index_in_dim(att_query, index, 0, keepdims=False).astype(jnp.float32)
        gate_rows = lax.dynamic_index_in_dim(gates, index, 2, keepdims=False)
        query_places = index * TOK_DEV + local_places

        def add_keys(other, carry):
            weighted, total = carry
            key_rows = lax.dynamic_index_in_dim(att_key, other, 0, keepdims=False).astype(jnp.float32)
            value_rows = lax.dynamic_index_in_dim(att_value, other, 0, keepdims=False).astype(jnp.float32)
            gate_keys = lax.dynamic_index_in_dim(gates, other, 2, keepdims=False)
            scores = jnp.einsum('tcgd,scd->cgts', query_rows, key_rows)
            logits = scores + gate_rows[:, :, :, None] - gate_keys[:, :, None, :]
            allowed = (other * TOK_DEV + local_places)[None, :] <= query_places[:, None]
            weights = jnp.exp(jnp.where(allowed, logits, -jnp.inf))
            total = total + lax.optimization_barrier(jnp.sum(weights, axis=-1))
            weighted = weighted + jnp.einsum('cgts,scd->cgtd', weights.astype(jnp.bfloat16).astype(jnp.float32), value_rows)
            return (weighted, total)
        init = (jnp.zeros((KV_HEADS, group, TOK_DEV, HEAD), jnp.float32), jnp.zeros((KV_HEADS, group, TOK_DEV), jnp.float32))
        weighted, total = lax.fori_loop(0, index + 1, add_keys, init)
        return (weighted / total[..., None]).astype(jnp.bfloat16)
    outputs = lax.map(attend_block, jnp.arange(pieces, dtype=jnp.int32))
    attended = jnp.transpose(outputs, (0, 3, 1, 2, 4)).reshape(TOKENS, F_HEADS * HEAD)
    ret_width = R_HEADS // N_TP * HEAD
    att_width = F_HEADS // N_TP * HEAD
    summed = jnp.zeros((TOKENS, D), jnp.float32)
    for part in range(N_TP):
        term = jnp.dot(retained[:, part * ret_width:(part + 1) * ret_width], w_out_ret[part * ret_width:(part + 1) * ret_width], preferred_element_type=jnp.float32)
        term = term + jnp.dot(attended[:, part * att_width:(part + 1) * att_width], w_out_att[part * att_width:(part + 1) * att_width], preferred_element_type=jnp.float32)
        summed = summed + lax.optimization_barrier(term.astype(jnp.bfloat16)).astype(jnp.float32)
    return summed.astype(jnp.bfloat16)
```

```python
import jax
import jax.numpy as jnp
from jax import lax
from jax.experimental import pallas as pl
from jax.experimental.pallas import tpu as pltpu
from jax.sharding import Mesh
from jax.sharding import PartitionSpec as P

HEAD = 64
SPAN = 256
SP = ("z", "y", "c")
EPS = 1e-06
THETA = 10000.0
LOG2E = 1.4426950408889634
F32 = jnp.float32
BF16 = jnp.bfloat16
SKEW = [[((m - y) % 8) * 8 + y for y in range(8)] for m in range(8)]
NT = (((1,), (1,)), ((), ()))
TN = (((0,), (0,)), ((), ()))
VMEM = pl.BlockSpec(memory_space=pltpu.VMEM)
SMEM = pl.BlockSpec(memory_space=pltpu.SMEM)
PARAMS = pltpu.CompilerParams(vmem_limit_bytes=56 * 1024 * 1024)


def copies_from(shard, axis, groups=None):
    count = len(groups[0]) if groups else lax.axis_size(axis)
    copies = jnp.broadcast_to(shard, (count, *shard.shape))
    return lax.all_to_all(
        copies, axis, split_axis=0, concat_axis=0, tiled=True, axis_index_groups=groups
    )


def swapped_cores(value):
    return lax.ppermute(value, "c", [(0, 1), (1, 0)])


def three_parts(values):
    high = lax.reduce_precision(values, 8, 7)
    rest = values - high
    middle = lax.reduce_precision(rest, 8, 7)
    low = lax.reduce_precision(rest - middle, 8, 7)
    return [part.astype(BF16) for part in (high, middle, low)]


def front_kernel(
    rows, w_own, w_oth, cosine, sine, decay, decay_row, q_out, kv_out, local_out, lifted_out, state_out, proj
):
    proj[...] = jnp.dot(
        rows[:, 0].reshape(SPAN, -1), w_own[...], preferred_element_type=F32
    ) + jnp.dot(rows[:, 1].reshape(SPAN, -1), w_oth[...], preferred_element_type=F32)
    cos = cosine[...]
    sin = sine[...]
    place = lax.broadcasted_iota(jnp.int32, (SPAN, SPAN), 0)
    other = lax.broadcasted_iota(jnp.int32, (SPAN, SPAN), 1)
    causal = place >= other

    def turned(at):
        first = proj[:, at : at + 32]
        second = proj[:, at + 32 : at + 64]
        return jnp.concatenate(
            [first * cos - second * sin, first * sin + second * cos], axis=1
        )

    for h in range(3):
        query = (turned(h * HEAD) * HEAD ** (-0.5)).astype(BF16)
        key = turned(192 + h * HEAD).astype(BF16)
        value = proj[:, 384 + h * HEAD : 384 + (h + 1) * HEAD].astype(BF16)
        column = decay[:, h : h + 1]
        row = decay_row[h : h + 1, :]
        last = decay[SPAN - 1 : SPAN, h : h + 1]
        scores = lax.dot_general(query, key, NT, preferred_element_type=F32)
        gap = jnp.where(causal, column - row, 0.0)
        weights = jnp.where(causal, scores * jnp.exp(gap), 0.0).astype(BF16)
        local_out[:, h * HEAD : (h + 1) * HEAD] = jnp.dot(
            weights, value, preferred_element_type=F32
        )
        faded = (key.astype(F32) * jnp.exp(last - column)).astype(BF16)
        update = lax.dot_general(faded, value, TN, preferred_element_type=F32)
        state_out[(h // 2) * HEAD : (h // 2 + 1) * HEAD, (h % 2) * HEAD : (h % 2 + 1) * HEAD] = (
            update.astype(BF16)
        )
        lifted_out[:, h * HEAD : (h + 1) * HEAD] = (
            query.astype(F32) * jnp.exp(column)
        ).astype(BF16)
    ends = decay_row[:, SPAN - 1 : SPAN]
    high = ends.astype(BF16).astype(F32)
    middle = (ends - high).astype(BF16).astype(F32)
    low = ends - high - middle
    lane = lax.broadcasted_iota(jnp.int32, (8, HEAD), 1)
    tail = jnp.where(lane == 0, high, jnp.where(lane == 1, middle, jnp.where(lane == 2, low, 0.0)))
    state_out[HEAD:, HEAD:] = jnp.concatenate(
        [tail, jnp.zeros((HEAD - 8, HEAD), F32)], axis=0
    ).astype(BF16)
    q_out[...] = jnp.transpose(proj[:, 576:768] * (HEAD ** (-0.5) * LOG2E)).astype(BF16)
    both = proj[:, 768:896]
    flipped = jnp.transpose(both)[HEAD:, :].astype(BF16)
    kv_out[:128] = jnp.concatenate([both[:128, :HEAD], both[128:, :HEAD]], axis=1).astype(BF16)
    kv_out[128:] = jnp.concatenate([flipped[:, :128], flipped[:, 128:]], axis=0)


def attend_kernel(
    plan, query, kv_own, kv_oth, key_gate, query_gate, out, keys, values, queries, total
):
    extra = lax.broadcasted_iota(jnp.int32, (16, 2 * SPAN), 0)
    ones = jnp.where(extra == 0, 1.0, 0.0).astype(BF16)
    for y in range(8):
        for side, held in enumerate((kv_own, kv_oth)):
            packed = held[y, :128]
            at = side * SPAN
            keys[y, at : at + 128, :HEAD] = packed[:, :HEAD]
            keys[y, at + 128 : at + SPAN, :HEAD] = packed[:, HEAD:]
            keys[y, at : at + SPAN, HEAD:] = key_gate[side, y]
            values[y, :HEAD, at : at + 128] = held[y, 128:192]
            values[y, :HEAD, at + 128 : at + SPAN] = held[y, 192:]
        values[y, HEAD:, :] = ones
    for z in range(8):
        for h in range(3):
            queries[z, :HEAD, h * SPAN : (h + 1) * SPAN] = query[z, h * HEAD : (h + 1) * HEAD]
        queries[z, HEAD:, :] = query_gate[z]
    total[...] = jnp.zeros_like(total)
    mine_z, mine_y, mine_c = (plan[65], plan[66], plan[67])

    scores = jnp.dot(keys[mine_y], queries[mine_z], preferred_element_type=F32)
    place = lax.broadcasted_iota(jnp.int32, (2 * SPAN, 3 * SPAN), 0)
    wanted = lax.broadcasted_iota(jnp.int32, (2 * SPAN, 3 * SPAN), 1) % SPAN
    limit = jnp.where(place < SPAN, wanted, mine_c * (4 * SPAN) - 1)
    weights = jnp.where(place <= limit, jnp.exp2(scores), 0.0).astype(BF16)
    total[mine_z] += jnp.dot(values[mine_y], weights, preferred_element_type=F32)

    def unit(i, carry):
        code = plan[i]
        z = code // 8
        y = code % 8
        weights = jnp.exp2(
            jnp.dot(keys[y], queries[z], preferred_element_type=F32)
        ).astype(BF16)
        total[z] += jnp.dot(values[y], weights, preferred_element_type=F32)
        return carry

    lax.fori_loop(0, plan[64], unit, 0)
    for z in range(8):
        rows = []
        for h in range(3):
            out[z, h * HEAD : (h + 1) * HEAD] = total[z, :HEAD, h * SPAN : (h + 1) * SPAN].astype(
                BF16
            )
            rows.append(total[z, HEAD : HEAD + 1, h * SPAN : (h + 1) * SPAN])
        high = [row.astype(BF16).astype(F32) for row in rows]
        low = [row - big for row, big in zip(rows, high)]
        out[z, 192:] = jnp.concatenate(high + low + [jnp.zeros((10, SPAN), F32)], axis=0).astype(
            BF16
        )


def combine_kernel(states, above, below, out):
    def add(j, carry):
        upper, lower = carry
        upper = upper + states[j, :HEAD].astype(F32) * above[pl.ds(j, 1), :]
        lower = lower + states[j, HEAD:].astype(F32) * below[pl.ds(j, 1), :]
        return (upper, lower)

    zero = jnp.zeros((HEAD, 128), F32)
    upper, lower = lax.fori_loop(0, states.shape[0], add, (zero, zero))
    out[:HEAD] = upper.astype(BF16)
    out[HEAD:] = lower.astype(BF16)


def back_kernel(parts, local, lifted, state, w_out, out, mixed):
    total = parts[0].astype(F32)
    for z in range(1, 8):
        total = total + parts[z].astype(F32)
    for h in range(3):
        held = state[
            (h // 2) * HEAD : (h // 2 + 1) * HEAD, (h % 2) * HEAD : (h % 2 + 1) * HEAD
        ]
        raw = local[:, h * HEAD : (h + 1) * HEAD] + jnp.dot(
            lifted[:, h * HEAD : (h + 1) * HEAD], held, preferred_element_type=F32
        )
        centred = raw - jnp.mean(raw, axis=-1, keepdims=True)
        spread = jnp.mean(centred * centred, axis=-1, keepdims=True)
        mixed[:, h * HEAD : (h + 1) * HEAD] = (centred * lax.rsqrt(spread + EPS)).astype(BF16)
        weight = total[192 + h : 193 + h] + total[195 + h : 196 + h]
        attended = total[h * HEAD : (h + 1) * HEAD] / weight
        mixed[:, 192 + h * HEAD : 192 + (h + 1) * HEAD] = jnp.transpose(attended).astype(BF16)
    out[...] = lax.dot_general(
        mixed[...], w_out[...], NT, preferred_element_type=F32
    ).astype(BF16)


def body(
    tokens,
    pre_gain,
    w_query_ret,
    w_key_ret,
    w_value_ret,
    w_query_att,
    w_key_att,
    w_value_att,
    w_out_ret,
    w_out_att,
    retain_log,
    forget_total,
):
    z, y, c = (lax.axis_index("z"), lax.axis_index("y"), lax.axis_index("c"))
    shard = jnp.concatenate(
        [
            w_query_ret,
            w_key_ret,
            w_value_ret,
            w_query_att,
            w_key_att,
            w_value_att,
            w_out_ret.T,
            w_out_att.T,
        ],
        axis=1,
    )
    width = shard.shape[1]
    w_row = copies_from(shard, "y").reshape(-1, width)
    w_own = lax.all_gather(w_row, "z", axis=0, tiled=True)
    w_oth = swapped_cores(w_own)

    raw = tokens.astype(F32)
    normed = (
        raw * lax.rsqrt(jnp.mean(raw * raw, axis=-1, keepdims=True) + EPS) * pre_gain
    ).astype(BF16)
    halves = jnp.transpose(normed.reshape(64, 64, 2, 16), (2, 0, 1, 3)).reshape(2, 64, 1024)
    halves = jnp.where(c == 0, halves, halves[::-1])
    rows = copies_from(halves, "tp")

    here = z * 16 + y * 2 + c
    positions = (here * SPAN + jnp.arange(SPAN, dtype=jnp.int32)).astype(F32)
    inverse = THETA ** (-jnp.arange(32, dtype=F32) / 32)
    angles = positions[:, None] * inverse[None, :]
    cosine, sine = (jnp.cos(angles), jnp.sin(angles))
    decay = jnp.cumsum(retain_log, axis=0)
    decay_row = jnp.pad(decay.T, ((0, 5), (0, 0)))

    gate = (forget_total * LOG2E).reshape(3, 8, 8, 2, SPAN)
    spans = jnp.arange(8, dtype=jnp.int32)
    key_z = (z + y - spans) % 8
    chosen = (spans[:, None] == key_z[None, :])[None, :, :, None, None]
    key_side = jnp.sum(jnp.where(chosen, gate, 0.0), axis=1)
    key_side = jnp.where(c == 0, key_side, key_side[:, :, ::-1])
    minus = jnp.stack(three_parts(-key_side), axis=1).reshape(9, 8, 2, SPAN)
    key_gate = jnp.concatenate(
        [minus, jnp.ones((3, 8, 2, SPAN), BF16), jnp.zeros((52, 8, 2, SPAN), BF16)], axis=0
    )
    key_gate = jnp.transpose(key_gate, (2, 1, 3, 0))
    mine = lax.dynamic_index_in_dim(
        lax.dynamic_index_in_dim(gate, y, 2, keepdims=False), c, 2, keepdims=False
    )
    plus = jnp.stack(three_parts(mine), axis=0)
    plus = jnp.transpose(plus, (2, 0, 1, 3)).reshape(8, 3, 3 * SPAN)
    own_head = (
        (jnp.arange(9)[:, None] // 3) == (jnp.arange(3 * SPAN)[None, :] // SPAN)
    ).astype(BF16)
    query_gate = jnp.concatenate(
        [
            jnp.broadcast_to(own_head, (8, 9, 3 * SPAN)),
            plus,
            jnp.zeros((8, 52, 3 * SPAN), BF16),
        ],
        axis=1,
    )
    needed = (
        (key_z[None, :] < spans[:, None])
        | ((key_z[None, :] == spans[:, None]) & (spans[None, :] < y))
    ).reshape(64)
    slot = jnp.cumsum(needed.astype(jnp.int32)) - 1
    order = jnp.arange(64, dtype=jnp.int32)
    units = jnp.sum(
        jnp.where(needed[None, :] & (slot[None, :] == order[:, None]), order[None, :], 0), axis=1
    )
    plan = jnp.concatenate([units, jnp.stack([jnp.sum(needed.astype(jnp.int32)), z, y, c])])

    q_send, kv_send, local, lifted, state = pl.pallas_call(
        front_kernel,
        grid=(1,),
        in_specs=[
            VMEM,
            pl.BlockSpec((1024, 896), lambda i: (0, 0)),
            pl.BlockSpec((1024, 896), lambda i: (0, 0)),
            VMEM,
            VMEM,
            VMEM,
            VMEM,
        ],
        out_specs=[VMEM] * 5,
        out_shape=[
            jax.ShapeDtypeStruct((192, SPAN), BF16),
            jax.ShapeDtypeStruct((SPAN, 128), BF16),
            jax.ShapeDtypeStruct((SPAN, 192), F32),
            jax.ShapeDtypeStruct((SPAN, 192), BF16),
            jax.ShapeDtypeStruct((128, 128), BF16),
        ],
        scratch_shapes=[pltpu.VMEM((SPAN, 896), F32)],
        compiler_params=PARAMS,
        name="front",
    )(rows, w_own, w_oth, cosine, sine, decay, decay_row)

    states = lax.all_gather(state, SP, axis=0)
    kv_own = copies_from(kv_send, ("z", "y"), SKEW)
    kv_oth = swapped_cores(kv_own)
    queries = copies_from(q_send, "z")

    partial = pl.pallas_call(
        attend_kernel,
        in_specs=[SMEM, VMEM, VMEM, VMEM, VMEM, VMEM],
        out_specs=VMEM,
        out_shape=jax.ShapeDtypeStruct((8, 208, SPAN), BF16),
        scratch_shapes=[
            pltpu.VMEM((8, 2 * SPAN, 128), BF16),
            pltpu.VMEM((8, 80, 2 * SPAN), BF16),
            pltpu.VMEM((8, 128, 3 * SPAN), BF16),
            pltpu.VMEM((8, 80, 3 * SPAN), F32),
        ],
        compiler_params=PARAMS,
        name="attend",
    )(plan, queries, kv_own, kv_oth, key_gate, query_gate)
    parts = lax.all_to_all(partial, "z", 0, 0, tiled=True)

    ends = jnp.sum(states[:, HEAD : HEAD + 3, HEAD : HEAD + 3].astype(F32), axis=-1)
    index = jnp.arange(128, dtype=jnp.int32)
    between = (index[None, :] > index[:, None]) & (index[None, :] < here)
    span_log = jnp.sum(jnp.where(between[:, :, None], ends[None], 0.0), axis=1)
    factor = jnp.where((index < here)[:, None], jnp.exp(span_log), 0.0)
    above = jnp.repeat(factor[:, :2], HEAD, axis=1)
    below = jnp.pad(jnp.repeat(factor[:, 2:], HEAD, axis=1), ((0, 0), (0, HEAD)))
    incoming = pl.pallas_call(
        combine_kernel,
        in_specs=[VMEM] * 3,
        out_specs=VMEM,
        out_shape=jax.ShapeDtypeStruct((128, 128), BF16),
        compiler_params=PARAMS,
        name="combine",
    )(states, above, below)

    out_own = w_own[:, 896:].reshape(64, 16, 384)
    out_oth = w_oth[:, 896:].reshape(64, 16, 384)
    w_out = jnp.where(
        c == 0, jnp.stack([out_own, out_oth], axis=1), jnp.stack([out_oth, out_own], axis=1)
    ).reshape(2048, 384)
    share = pl.pallas_call(
        back_kernel,
        in_specs=[VMEM] * 5,
        out_specs=VMEM,
        out_shape=jax.ShapeDtypeStruct((SPAN, 2048), BF16),
        scratch_shapes=[pltpu.VMEM((SPAN, 384), BF16)],
        compiler_params=PARAMS,
        name="back",
    )(parts, local, lifted, incoming, w_out)
    shares = lax.all_to_all(share.reshape(4, 64, 2048), "tp", 0, 0, tiled=True)
    return jnp.sum(shares.astype(F32), axis=0).astype(BF16)


def solution(mesh):
    finer = Mesh(mesh.devices.reshape(8, 8, 2, mesh.shape["tp"]), ("z", "y", "c", "tp"))
    everyone = ("z", "y", "c", "tp")
    placed = (
        P(everyone, None),
        P(),
        P(SP, "tp"),
        P(SP, "tp"),
        P(SP, "tp"),
        P(SP, "tp"),
        P(SP, "tp"),
        P(SP, "tp"),
        P("tp", SP),
        P("tp", SP),
        P(SP, "tp"),
        P("tp", None),
    )
    return jax.shard_map(
        body, mesh=finer, in_specs=placed, out_specs=P(everyone, None), check_vma=False
    )
```

```python
import jax
import jax.numpy as jnp
from jax import lax
from jax.experimental import pallas as pl
from jax.experimental.pallas import tpu as pltpu
from jax.sharding import Mesh
from jax.sharding import PartitionSpec as P

HEAD = 64
SPAN = 256
SP = ("z", "y", "c")
EPS = 1e-06
THETA = 10000.0
LOG2E = 1.4426950408889634
F32 = jnp.float32
BF16 = jnp.bfloat16
SKEW = [[((m - y) % 8) * 8 + y for y in range(8)] for m in range(8)]
NT = (((1,), (1,)), ((), ()))
TN = (((0,), (0,)), ((), ()))
VMEM = pl.BlockSpec(memory_space=pltpu.VMEM)
SMEM = pl.BlockSpec(memory_space=pltpu.SMEM)
PARAMS = pltpu.CompilerParams(vmem_limit_bytes=56 * 1024 * 1024)


def copies_from(shard, axis, groups=None):
    count = len(groups[0]) if groups else lax.axis_size(axis)
    copies = jnp.broadcast_to(shard, (count, *shard.shape))
    return lax.all_to_all(
        copies, axis, split_axis=0, concat_axis=0, tiled=True, axis_index_groups=groups
    )


def swapped_cores(value):
    return lax.ppermute(value, "c", [(0, 1), (1, 0)])


def three_parts(values):
    high = lax.reduce_precision(values, 8, 7)
    rest = values - high
    middle = lax.reduce_precision(rest, 8, 7)
    low = lax.reduce_precision(rest - middle, 8, 7)
    return [part.astype(BF16) for part in (high, middle, low)]


def front_kernel(
    rows, w_own, w_oth, cosine, sine, decay, decay_row, q_out, kv_out, local_out, lifted_out, state_out, proj
):
    proj[...] = jnp.dot(
        rows[:, 0].reshape(SPAN, -1), w_own[...], preferred_element_type=F32
    ) + jnp.dot(rows[:, 1].reshape(SPAN, -1), w_oth[...], preferred_element_type=F32)
    cos = cosine[...]
    sin = sine[...]
    place = lax.broadcasted_iota(jnp.int32, (SPAN, SPAN), 0)
    other = lax.broadcasted_iota(jnp.int32, (SPAN, SPAN), 1)
    causal = place >= other

    def turned(at):
        first = proj[:, at : at + 32]
        second = proj[:, at + 32 : at + 64]
        return jnp.concatenate(
            [first * cos - second * sin, first * sin + second * cos], axis=1
        )

    for h in range(3):
        query = (turned(h * HEAD) * HEAD ** (-0.5)).astype(BF16)
        key = turned(192 + h * HEAD).astype(BF16)
        value = proj[:, 384 + h * HEAD : 384 + (h + 1) * HEAD].astype(BF16)
        column = decay[:, h : h + 1]
        row = decay_row[h : h + 1, :]
        last = decay[SPAN - 1 : SPAN, h : h + 1]
        scores = lax.dot_general(query, key, NT, preferred_element_type=F32)
        gap = jnp.where(causal, column - row, 0.0)
        weights = jnp.where(causal, scores * jnp.exp(gap), 0.0).astype(BF16)
        local_out[:, h * HEAD : (h + 1) * HEAD] = jnp.dot(
            weights, value, preferred_element_type=F32
        )
        faded = (key.astype(F32) * jnp.exp(last - column)).astype(BF16)
        update = lax.dot_general(faded, value, TN, preferred_element_type=F32)
        state_out[(h // 2) * HEAD : (h // 2 + 1) * HEAD, (h % 2) * HEAD : (h % 2 + 1) * HEAD] = (
            update.astype(BF16)
        )
        lifted_out[:, h * HEAD : (h + 1) * HEAD] = (
            query.astype(F32) * jnp.exp(column)
        ).astype(BF16)
    ends = decay_row[:, SPAN - 1 : SPAN]
    high = ends.astype(BF16).astype(F32)
    middle = (ends - high).astype(BF16).astype(F32)
    low = ends - high - middle
    lane = lax.broadcasted_iota(jnp.int32, (8, HEAD), 1)
    tail = jnp.where(lane == 0, high, jnp.where(lane == 1, middle, jnp.where(lane == 2, low, 0.0)))
    state_out[HEAD:, HEAD:] = jnp.concatenate(
        [tail, jnp.zeros((HEAD - 8, HEAD), F32)], axis=0
    ).astype(BF16)
    q_out[...] = jnp.transpose(proj[:, 576:768] * (HEAD ** (-0.5) * LOG2E)).astype(BF16)
    both = proj[:, 768:896]
    flipped = jnp.transpose(both)[HEAD:, :].astype(BF16)
    kv_out[:128] = jnp.concatenate([both[:128, :HEAD], both[128:, :HEAD]], axis=1).astype(BF16)
    kv_out[128:] = jnp.concatenate([flipped[:, :128], flipped[:, 128:]], axis=0)


def attend_kernel(
    plan, queries, kv_own, kv_oth, key_gate, out, keys, values, total
):
    mine_z, mine_y, mine_c = (plan[65], plan[66], plan[67])
    extra = lax.broadcasted_iota(jnp.int32, (16, 2 * SPAN), 0)
    ones = jnp.where(extra == 0, 1.0, 0.0).astype(BF16)
    for y in range(8):
        for side, held in enumerate((kv_own, kv_oth)):
            packed = held[y, :128]
            at = side * SPAN
            keys[y, at : at + 128, :HEAD] = packed[:, :HEAD]
            keys[y, at + 128 : at + SPAN, :HEAD] = packed[:, HEAD:]
            keys[y, at : at + SPAN, HEAD:] = key_gate[side, y]
            values[y, :HEAD, at : at + 128] = held[y, 128:192]
            values[y, :HEAD, at + 128 : at + SPAN] = held[y, 192:]
        values[y, HEAD:, :] = ones
    total[...] = jnp.zeros_like(total)

    place = lax.broadcasted_iota(jnp.int32, (2 * SPAN, SPAN), 0)
    wanted = lax.broadcasted_iota(jnp.int32, (2 * SPAN, SPAN), 1)
    allowed = place <= jnp.where(place < SPAN, wanted, mine_c * (4 * SPAN) - 1)
    for h in range(3):
        scores = jnp.dot(keys[mine_y], queries[0, h], preferred_element_type=F32)
        weights = jnp.where(allowed, jnp.exp2(scores), 0.0).astype(BF16)
        total[mine_z, :, h * SPAN : (h + 1) * SPAN] += jnp.dot(
            values[mine_y], weights, preferred_element_type=F32
        )

    def units(places):
        at = []
        for i in places:
            code = plan[i]
            at.append((code // 8, code % 8))
        chunks = [(z, y, h) for z, y in at for h in range(3)]

        def scored(z, y, h):
            return jnp.dot(keys[y], queries[(mine_z + 8 - z) % 8, h], preferred_element_type=F32)

        ready = scored(*chunks[0])
        for n, (z, y, h) in enumerate(chunks):
            ahead = scored(*chunks[n + 1]) if n + 1 < len(chunks) else None
            weights = jnp.exp2(ready).astype(BF16)
            total[z, :, h * SPAN : (h + 1) * SPAN] += jnp.dot(
                values[y], weights, preferred_element_type=F32
            )
            ready = ahead

    def pair(i, carry):
        units((2 * i, 2 * i + 1))
        return carry

    count = plan[64]
    lax.fori_loop(0, count // 2, pair, 0)

    @pl.when(count % 2 == 1)
    def _():
        units((count - 1,))

    for z in range(8):
        rows = []
        for h in range(3):
            out[z, h * HEAD : (h + 1) * HEAD] = total[z, :HEAD, h * SPAN : (h + 1) * SPAN].astype(
                BF16
            )
            rows.append(total[z, HEAD : HEAD + 1, h * SPAN : (h + 1) * SPAN])
        high = [row.astype(BF16).astype(F32) for row in rows]
        low = [row - big for row, big in zip(rows, high)]
        out[z, 192:] = jnp.concatenate(high + low + [jnp.zeros((10, SPAN), F32)], axis=0).astype(
            BF16
        )


def combine_kernel(states, above, below, out):
    def add(j, carry):
        upper, lower = carry
        upper = upper + states[j, :HEAD].astype(F32) * above[pl.ds(j, 1), :]
        lower = lower + states[j, HEAD:].astype(F32) * below[pl.ds(j, 1), :]
        return (upper, lower)

    zero = jnp.zeros((HEAD, 128), F32)
    upper, lower = lax.fori_loop(0, states.shape[0], add, (zero, zero))
    out[:HEAD] = upper.astype(BF16)
    out[HEAD:] = lower.astype(BF16)


def back_kernel(parts, local, lifted, state, w_out, out, mixed):
    total = parts[0].astype(F32)
    for z in range(1, 8):
        total = total + parts[z].astype(F32)
    for h in range(3):
        held = state[
            (h // 2) * HEAD : (h // 2 + 1) * HEAD, (h % 2) * HEAD : (h % 2 + 1) * HEAD
        ]
        raw = local[:, h * HEAD : (h + 1) * HEAD] + jnp.dot(
            lifted[:, h * HEAD : (h + 1) * HEAD], held, preferred_element_type=F32
        )
        centred = raw - jnp.mean(raw, axis=-1, keepdims=True)
        spread = jnp.mean(centred * centred, axis=-1, keepdims=True)
        mixed[:, h * HEAD : (h + 1) * HEAD] = (centred * lax.rsqrt(spread + EPS)).astype(BF16)
        weight = total[192 + h : 193 + h] + total[195 + h : 196 + h]
        attended = total[h * HEAD : (h + 1) * HEAD] / weight
        mixed[:, 192 + h * HEAD : 192 + (h + 1) * HEAD] = jnp.transpose(attended).astype(BF16)
    out[...] = lax.dot_general(
        mixed[...], w_out[...], NT, preferred_element_type=F32
    ).astype(BF16)


def body(
    tokens,
    pre_gain,
    w_query_ret,
    w_key_ret,
    w_value_ret,
    w_query_att,
    w_key_att,
    w_value_att,
    w_out_ret,
    w_out_att,
    retain_log,
    forget_total,
):
    z, y, c = (lax.axis_index("z"), lax.axis_index("y"), lax.axis_index("c"))
    shard = jnp.concatenate(
        [
            w_query_ret,
            w_key_ret,
            w_value_ret,
            w_query_att,
            w_key_att,
            w_value_att,
            w_out_ret.T,
            w_out_att.T,
        ],
        axis=1,
    )
    width = shard.shape[1]
    w_row = copies_from(shard, "y").reshape(-1, width)
    w_own = lax.all_gather(w_row, "z", axis=0, tiled=True)
    w_oth = swapped_cores(w_own)

    raw = tokens.astype(F32)
    normed = (
        raw * lax.rsqrt(jnp.mean(raw * raw, axis=-1, keepdims=True) + EPS) * pre_gain
    ).astype(BF16)
    halves = jnp.transpose(normed.reshape(64, 64, 2, 16), (2, 0, 1, 3)).reshape(2, 64, 1024)
    rows = copies_from(halves, "tp")
    rows = jnp.where(c == 0, rows, rows[:, ::-1])

    here = z * 16 + y * 2 + c
    positions = (here * SPAN + jnp.arange(SPAN, dtype=jnp.int32)).astype(F32)
    inverse = THETA ** (-jnp.arange(32, dtype=F32) / 32)
    angles = positions[:, None] * inverse[None, :]
    cosine, sine = (jnp.cos(angles), jnp.sin(angles))
    decay = jnp.cumsum(retain_log, axis=0)
    decay_row = jnp.pad(decay.T, ((0, 5), (0, 0)))

    gate = (forget_total * LOG2E).reshape(3, 8, 8, 2, SPAN)
    spans = jnp.arange(8, dtype=jnp.int32)
    key_z = (z + y - spans) % 8
    chosen = (spans[:, None] == key_z[None, :])[None, :, :, None, None]
    key_side = jnp.sum(jnp.where(chosen, gate, 0.0), axis=1)
    key_side = jnp.where(c == 0, key_side, key_side[:, :, ::-1])
    minus = jnp.stack(three_parts(-key_side), axis=1).reshape(9, 8, 2, SPAN)
    key_gate = jnp.concatenate(
        [minus, jnp.ones((3, 8, 2, SPAN), BF16), jnp.zeros((52, 8, 2, SPAN), BF16)], axis=0
    )
    key_gate = jnp.transpose(key_gate, (2, 1, 3, 0))
    mine = lax.dynamic_index_in_dim(
        lax.dynamic_index_in_dim(gate, y, 2, keepdims=False), c, 2, keepdims=False
    )
    wanted = (spans[:, None] == ((z - spans) % 8)[None, :])[None, :, :, None]
    mine = jnp.sum(jnp.where(wanted, mine[:, :, None, :], 0.0), axis=1)
    plus = jnp.transpose(jnp.stack(three_parts(mine), axis=0), (2, 1, 0, 3))
    own_head = (
        jnp.arange(9, dtype=jnp.int32)[None, :] // 3 == jnp.arange(3, dtype=jnp.int32)[:, None]
    ).astype(BF16)
    query_gate = jnp.concatenate(
        [
            jnp.broadcast_to(own_head[None, :, :, None], (8, 3, 9, SPAN)),
            plus,
            jnp.zeros((8, 3, 52, SPAN), BF16),
        ],
        axis=2,
    )
    needed = (
        (key_z[None, :] < spans[:, None])
        | ((key_z[None, :] == spans[:, None]) & (spans[None, :] < y))
    ).reshape(64)
    slot = jnp.cumsum(needed.astype(jnp.int32)) - 1
    order = jnp.arange(64, dtype=jnp.int32)
    units = jnp.sum(
        jnp.where(needed[None, :] & (slot[None, :] == order[:, None]), order[None, :], 0), axis=1
    )
    plan = jnp.concatenate([units, jnp.stack([jnp.sum(needed.astype(jnp.int32)), z, y, c])])

    q_send, kv_send, local, lifted, state = pl.pallas_call(
        front_kernel,
        grid=(1,),
        in_specs=[
            VMEM,
            pl.BlockSpec((1024, 896), lambda i: (0, 0)),
            pl.BlockSpec((1024, 896), lambda i: (0, 0)),
            VMEM,
            VMEM,
            VMEM,
            VMEM,
        ],
        out_specs=[VMEM] * 5,
        out_shape=[
            jax.ShapeDtypeStruct((192, SPAN), BF16),
            jax.ShapeDtypeStruct((SPAN, 128), BF16),
            jax.ShapeDtypeStruct((SPAN, 192), F32),
            jax.ShapeDtypeStruct((SPAN, 192), BF16),
            jax.ShapeDtypeStruct((128, 128), BF16),
        ],
        scratch_shapes=[pltpu.VMEM((SPAN, 896), F32)],
        compiler_params=PARAMS,
        name="front",
    )(rows, w_own, w_oth, cosine, sine, decay, decay_row)

    states = lax.all_gather(state, SP, axis=0)
    kv_own = copies_from(kv_send, ("z", "y"), SKEW)
    kv_oth = swapped_cores(kv_own)
    queries = [q_send]
    for k in range(1, 8):
        queries.append(lax.ppermute(q_send, "z", [(i, (i + k) % 8) for i in range(8)]))
    queries = jnp.stack([part.reshape(3, HEAD, SPAN) for part in queries])
    queries = jnp.concatenate([queries, query_gate], axis=2)

    partial = pl.pallas_call(
        attend_kernel,
        in_specs=[SMEM] + [VMEM] * 4,
        out_specs=VMEM,
        out_shape=jax.ShapeDtypeStruct((8, 208, SPAN), BF16),
        scratch_shapes=[
            pltpu.VMEM((8, 2 * SPAN, 128), BF16),
            pltpu.VMEM((8, 80, 2 * SPAN), BF16),
            pltpu.VMEM((8, 80, 3 * SPAN), F32),
        ],
        compiler_params=PARAMS,
        name="attend",
    )(plan, queries, kv_own, kv_oth, key_gate)
    parts = lax.all_to_all(partial, "z", 0, 0, tiled=True)

    ends = jnp.sum(states[:, HEAD : HEAD + 3, HEAD : HEAD + 3].astype(F32), axis=-1)
    index = jnp.arange(128, dtype=jnp.int32)
    between = (index[None, :] > index[:, None]) & (index[None, :] < here)
    span_log = jnp.sum(jnp.where(between[:, :, None], ends[None], 0.0), axis=1)
    factor = jnp.where((index < here)[:, None], jnp.exp(span_log), 0.0)
    above = jnp.repeat(factor[:, :2], HEAD, axis=1)
    below = jnp.pad(jnp.repeat(factor[:, 2:], HEAD, axis=1), ((0, 0), (0, HEAD)))
    incoming = pl.pallas_call(
        combine_kernel,
        in_specs=[VMEM] * 3,
        out_specs=VMEM,
        out_shape=jax.ShapeDtypeStruct((128, 128), BF16),
        compiler_params=PARAMS,
        name="combine",
    )(states, above, below)

    out_own = w_own[:, 896:].reshape(64, 16, 384)
    out_oth = w_oth[:, 896:].reshape(64, 16, 384)
    w_out = jnp.where(
        c == 0, jnp.stack([out_own, out_oth], axis=1), jnp.stack([out_oth, out_own], axis=1)
    ).reshape(2048, 384)
    share = pl.pallas_call(
        back_kernel,
        in_specs=[VMEM] * 5,
        out_specs=VMEM,
        out_shape=jax.ShapeDtypeStruct((SPAN, 2048), BF16),
        scratch_shapes=[pltpu.VMEM((SPAN, 384), BF16)],
        compiler_params=PARAMS,
        name="back",
    )(parts, local, lifted, incoming, w_out)
    shares = lax.all_to_all(share.reshape(4, 64, 2048), "tp", 0, 0, tiled=True)
    return jnp.sum(shares.astype(F32), axis=0).astype(BF16)


def solution(mesh):
    finer = Mesh(mesh.devices.reshape(8, 8, 2, mesh.shape["tp"]), ("z", "y", "c", "tp"))
    everyone = ("z", "y", "c", "tp")
    placed = (
        P(everyone, None),
        P(),
        P(SP, "tp"),
        P(SP, "tp"),
        P(SP, "tp"),
        P(SP, "tp"),
        P(SP, "tp"),
        P(SP, "tp"),
        P("tp", SP),
        P("tp", SP),
        P(SP, "tp"),
        P("tp", None),
    )
    return jax.shard_map(
        body, mesh=finer, in_specs=placed, out_specs=P(everyone, None), check_vma=False
    )
```

```python
import jax
import jax.numpy as jnp
from jax import lax
from jax.experimental import pallas as pl
from jax.experimental.pallas import tpu as pltpu
from jax.sharding import Mesh
from jax.sharding import PartitionSpec as P

HEAD = 64
SPAN = 256
SP = ("z", "y", "c")
EPS = 1e-06
THETA = 10000.0
LOG2E = 1.4426950408889634
F32 = jnp.float32
BF16 = jnp.bfloat16
SKEW = [[((m - y) % 8) * 8 + y for y in range(8)] for m in range(8)]
NT = (((1,), (1,)), ((), ()))
TN = (((0,), (0,)), ((), ()))
VMEM = pl.BlockSpec(memory_space=pltpu.VMEM)
SMEM = pl.BlockSpec(memory_space=pltpu.SMEM)
PARAMS = pltpu.CompilerParams(vmem_limit_bytes=56 * 1024 * 1024)


def copies_from(shard, axis, groups=None):
    count = len(groups[0]) if groups else lax.axis_size(axis)
    copies = jnp.broadcast_to(shard, (count, *shard.shape))
    return lax.all_to_all(
        copies, axis, split_axis=0, concat_axis=0, tiled=True, axis_index_groups=groups
    )


def swapped_cores(value):
    return lax.ppermute(value, "c", [(0, 1), (1, 0)])


def three_parts(values):
    high = lax.reduce_precision(values, 8, 7)
    rest = values - high
    middle = lax.reduce_precision(rest, 8, 7)
    low = lax.reduce_precision(rest - middle, 8, 7)
    return [part.astype(BF16) for part in (high, middle, low)]


def project_kernel(rows, weights, own_out, oth_out):
    product = jnp.dot(rows[...], weights[...], preferred_element_type=F32)
    own_out[...] = product[:SPAN]
    oth_out[...] = product[SPAN:]


def front_kernel(
    first_part, second_part, cosine, sine, decay, decay_row, q_out, kv_out, local_out, lifted_out, proj
):
    proj[...] = first_part[...] + second_part[...]
    cos = cosine[...]
    sin = sine[...]
    place = lax.broadcasted_iota(jnp.int32, (SPAN, SPAN), 0)
    other = lax.broadcasted_iota(jnp.int32, (SPAN, SPAN), 1)
    causal = place >= other

    def turned(at):
        first = proj[:, at : at + 32]
        second = proj[:, at + 32 : at + 64]
        return jnp.concatenate(
            [first * cos - second * sin, first * sin + second * cos], axis=1
        )

    for h in range(3):
        query = (turned(h * HEAD) * HEAD ** (-0.5)).astype(BF16)
        key = turned(192 + h * HEAD).astype(BF16)
        value = proj[:, 384 + h * HEAD : 384 + (h + 1) * HEAD].astype(BF16)
        column = decay[:, h : h + 1]
        row = decay_row[h : h + 1, :]
        last = decay[SPAN - 1 : SPAN, h : h + 1]
        scores = lax.dot_general(query, key, NT, preferred_element_type=F32)
        gap = jnp.where(causal, column - row, 0.0)
        weights = jnp.where(causal, scores * jnp.exp(gap), 0.0).astype(BF16)
        local_out[:, h * HEAD : (h + 1) * HEAD] = jnp.dot(
            weights, value, preferred_element_type=F32
        )
        faded = (key.astype(F32) * jnp.exp(last - column)).astype(BF16)
        update = lax.dot_general(faded, value, TN, preferred_element_type=F32)
        update = update.astype(BF16)
        kv_out[SPAN + 32 * h : SPAN + 32 * (h + 1)] = jnp.concatenate(
            [update[:32], update[32:]], axis=1
        )
        lifted_out[:, h * HEAD : (h + 1) * HEAD] = (
            query.astype(F32) * jnp.exp(column)
        ).astype(BF16)
    q_out[192:] = jnp.zeros((HEAD, SPAN), BF16)
    q_out[:192] = jnp.transpose(proj[:, 576:768] * (HEAD ** (-0.5) * LOG2E)).astype(BF16)
    both = proj[:, 768:896]
    flipped = jnp.transpose(both)[HEAD:, :].astype(BF16)
    kv_out[:128] = jnp.concatenate([both[:128, :HEAD], both[128:, :HEAD]], axis=1).astype(BF16)
    kv_out[128:SPAN] = jnp.concatenate([flipped[:, :128], flipped[:, 128:]], axis=0)


def attend_kernel(
    plan, fade, received, query_gate, kv_own, kv_oth, key_gate, out, keys, values, queries, total
):
    mine_z, mine_y, mine_c = (plan[65], plan[66], plan[67])
    extra = lax.broadcasted_iota(jnp.int32, (16, 2 * SPAN), 0)
    ones = jnp.where(extra == 0, 1.0, 0.0).astype(BF16)
    for y in range(8):
        for side, held in enumerate((kv_own, kv_oth)):
            packed = held[y, :128]
            at = side * SPAN
            keys[y, at : at + 128, :HEAD] = packed[:, :HEAD]
            keys[y, at + 128 : at + SPAN, :HEAD] = packed[:, HEAD:]
            keys[y, at : at + SPAN, HEAD:] = key_gate[side, y]
            values[y, :HEAD, at : at + 128] = held[y, 128:192]
            values[y, :HEAD, at + 128 : at + SPAN] = held[y, 192:SPAN]
        values[y, HEAD:, :] = ones
    for z in range(8):
        for h in range(3):
            queries[z, h, :HEAD] = received[z, h * HEAD : (h + 1) * HEAD]
            queries[z, h, HEAD:] = query_gate[z, h]
    total[...] = jnp.zeros_like(total)

    place = lax.broadcasted_iota(jnp.int32, (2 * SPAN, SPAN), 0)
    wanted = lax.broadcasted_iota(jnp.int32, (2 * SPAN, SPAN), 1)
    allowed = place <= jnp.where(place < SPAN, wanted, mine_c * (4 * SPAN) - 1)
    for h in range(3):
        scores = jnp.dot(keys[mine_y], queries[mine_z, h], preferred_element_type=F32)
        weights = jnp.where(allowed, jnp.exp2(scores), 0.0).astype(BF16)
        total[mine_z, :, h * SPAN : (h + 1) * SPAN] += jnp.dot(
            values[mine_y], weights, preferred_element_type=F32
        )

    def units(places):
        at = []
        for i in places:
            code = plan[i]
            at.append((code // 8, code % 8))
        chunks = [(z, y, h) for z, y in at for h in range(3)]

        def scored(z, y, h):
            return jnp.dot(keys[y], queries[z, h], preferred_element_type=F32)

        ready = scored(*chunks[0])
        for n, (z, y, h) in enumerate(chunks):
            ahead = scored(*chunks[n + 1]) if n + 1 < len(chunks) else None
            weights = jnp.exp2(ready).astype(BF16)
            total[z, :, h * SPAN : (h + 1) * SPAN] += jnp.dot(
                values[y], weights, preferred_element_type=F32
            )
            ready = ahead

    def pair(i, carry):
        units((2 * i, 2 * i + 1))
        return carry

    count = plan[64]
    lax.fori_loop(0, count // 2, pair, 0)

    @pl.when(count % 2 == 1)
    def _():
        units((count - 1,))

    for z in range(8):
        rows = []
        for h in range(3):
            out[z, h * HEAD : (h + 1) * HEAD] = total[z, :HEAD, h * SPAN : (h + 1) * SPAN].astype(
                BF16
            )
            rows.append(total[z, HEAD : HEAD + 1, h * SPAN : (h + 1) * SPAN])
        high = [row.astype(BF16).astype(F32) for row in rows]
        low = [row - big for row, big in zip(rows, high)]
        out[z, 192:208] = jnp.concatenate(
            high + low + [jnp.zeros((10, SPAN), F32)], axis=0
        ).astype(BF16)
    for z in range(8):
        sums = []
        for h in range(3):
            at = SPAN + 32 * h
            state = jnp.zeros((32, 128), F32)
            for side, held in enumerate((kv_own, kv_oth)):
                for y in range(8):
                    state = state + held[y, at : at + 32].astype(F32) * fade[
                        ((z * 2 + side) * 8 + y) * 3 + h
                    ]
            sums.append(state)
        sums = jnp.concatenate(sums, axis=0).astype(BF16)
        out[z, 208:, :128] = sums[:48]
        out[z, 208:, 128:] = sums[48:]


def back_kernel(parts, local, lifted, w_out, out, mixed):
    total = parts[0].astype(F32)
    for z in range(1, 8):
        total = total + parts[z].astype(F32)
    states = jnp.concatenate([total[208:, :128], total[208:, 128:]], axis=0)
    for h in range(3):
        held = states[32 * h : 32 * (h + 1)]
        held = jnp.concatenate([held[:, :HEAD], held[:, HEAD:]], axis=0).astype(BF16)
        raw = local[:, h * HEAD : (h + 1) * HEAD] + jnp.dot(
            lifted[:, h * HEAD : (h + 1) * HEAD], held, preferred_element_type=F32
        )
        centred = raw - jnp.mean(raw, axis=-1, keepdims=True)
        spread = jnp.mean(centred * centred, axis=-1, keepdims=True)
        mixed[:, h * HEAD : (h + 1) * HEAD] = (centred * lax.rsqrt(spread + EPS)).astype(BF16)
        weight = total[192 + h : 193 + h] + total[195 + h : 196 + h]
        attended = total[h * HEAD : (h + 1) * HEAD] / weight
        mixed[:, 192 + h * HEAD : 192 + (h + 1) * HEAD] = jnp.transpose(attended).astype(BF16)
    out[...] = lax.dot_general(
        mixed[...], w_out[...], NT, preferred_element_type=F32
    ).astype(BF16)


def body(
    tokens,
    pre_gain,
    w_query_ret,
    w_key_ret,
    w_value_ret,
    w_query_att,
    w_key_att,
    w_value_att,
    w_out_ret,
    w_out_att,
    retain_log,
    forget_total,
):
    z, y, c = (lax.axis_index("z"), lax.axis_index("y"), lax.axis_index("c"))
    shard = jnp.concatenate(
        [
            w_query_ret,
            w_key_ret,
            w_value_ret,
            w_query_att,
            w_key_att,
            w_value_att,
            w_out_ret.T,
            w_out_att.T,
        ],
        axis=1,
    )
    width = shard.shape[1]
    w_row = copies_from(shard, "y").reshape(-1, width)
    w_own = lax.all_gather(w_row, "z", axis=0, tiled=True)

    raw = tokens.astype(F32)
    normed = (
        raw * lax.rsqrt(jnp.mean(raw * raw, axis=-1, keepdims=True) + EPS) * pre_gain
    ).astype(BF16)
    halves = jnp.transpose(normed.reshape(64, 64, 2, 16), (2, 0, 1, 3)).reshape(2, 64, 1024)
    rows = copies_from(halves, "tp")
    kept = jnp.where(c == 0, rows[:, 0], rows[:, 1]).reshape(SPAN, 1024)
    sent = jnp.where(c == 0, rows[:, 1], rows[:, 0]).reshape(SPAN, 1024)
    came = swapped_cores(sent)
    rows = jnp.concatenate([kept, came], axis=0)

    here = z * 16 + y * 2 + c
    positions = (here * SPAN + jnp.arange(SPAN, dtype=jnp.int32)).astype(F32)
    inverse = THETA ** (-jnp.arange(32, dtype=F32) / 32)
    angles = positions[:, None] * inverse[None, :]
    cosine, sine = (jnp.cos(angles), jnp.sin(angles))
    decay = jnp.cumsum(retain_log, axis=0)
    decay_row = jnp.pad(decay.T, ((0, 5), (0, 0)))
    ends = lax.all_gather(decay[-1], "c")
    ends = copies_from(copies_from(ends, "y"), "z").reshape(128, 3)

    gate = (forget_total * LOG2E).reshape(3, 8, 8, 2, SPAN)
    spans = jnp.arange(8, dtype=jnp.int32)
    key_z = (z + y - spans) % 8
    chosen = (spans[:, None] == key_z[None, :])[None, :, :, None, None]
    key_side = jnp.sum(jnp.where(chosen, gate, 0.0), axis=1)
    key_side = jnp.where(c == 0, key_side, key_side[:, :, ::-1])
    minus = jnp.stack(three_parts(-key_side), axis=1).reshape(9, 8, 2, SPAN)
    key_gate = jnp.concatenate(
        [minus, jnp.ones((3, 8, 2, SPAN), BF16), jnp.zeros((52, 8, 2, SPAN), BF16)], axis=0
    )
    key_gate = jnp.transpose(key_gate, (2, 1, 3, 0))
    mine = lax.dynamic_index_in_dim(
        lax.dynamic_index_in_dim(gate, y, 2, keepdims=False), c, 2, keepdims=False
    )
    plus = jnp.transpose(jnp.stack(three_parts(mine), axis=0), (2, 1, 0, 3))
    own_head = (
        jnp.arange(9, dtype=jnp.int32)[None, :] // 3 == jnp.arange(3, dtype=jnp.int32)[:, None]
    ).astype(BF16)
    query_gate = jnp.concatenate(
        [
            jnp.broadcast_to(own_head[None, :, :, None], (8, 3, 9, SPAN)),
            plus,
            jnp.zeros((8, 3, 52, SPAN), BF16),
        ],
        axis=2,
    )
    blocks = key_z * 16 + spans * 2
    blocks = jnp.stack([blocks + c, blocks + 1 - c])
    targets = spans * 16 + y * 2 + c
    index = jnp.arange(128, dtype=jnp.int32)
    between = (index > blocks[None, :, :, None]) & (index < targets[:, None, None, None])
    fade = jnp.sum(jnp.where(between[..., None], ends, 0.0), axis=3)
    earlier = blocks[None] < targets[:, None, None]
    fade = jnp.where(earlier[..., None], jnp.exp(fade), 0.0).reshape(384)
    needed = (
        (key_z[None, :] < spans[:, None])
        | ((key_z[None, :] == spans[:, None]) & (spans[None, :] < y))
    ).reshape(64)
    slot = jnp.cumsum(needed.astype(jnp.int32)) - 1
    order = jnp.arange(64, dtype=jnp.int32)
    units = jnp.sum(
        jnp.where(needed[None, :] & (slot[None, :] == order[:, None]), order[None, :], 0), axis=1
    )
    plan = jnp.concatenate([units, jnp.stack([jnp.sum(needed.astype(jnp.int32)), z, y, c])])

    own_part, oth_part = pl.pallas_call(
        project_kernel,
        grid=(1,),
        in_specs=[VMEM, pl.BlockSpec((1024, 896), lambda i: (0, 0))],
        out_specs=[VMEM] * 2,
        out_shape=[jax.ShapeDtypeStruct((SPAN, 896), F32)] * 2,
        compiler_params=PARAMS,
        name="project",
    )(rows, w_own)
    q_send, kv_send, local, lifted = pl.pallas_call(
        front_kernel,
        in_specs=[VMEM] * 6,
        out_specs=[VMEM] * 4,
        out_shape=[
            jax.ShapeDtypeStruct((SPAN, SPAN), BF16),
            jax.ShapeDtypeStruct((SPAN + 96, 128), BF16),
            jax.ShapeDtypeStruct((SPAN, 192), F32),
            jax.ShapeDtypeStruct((SPAN, 192), BF16),
        ],
        scratch_shapes=[pltpu.VMEM((SPAN, 896), F32)],
        compiler_params=PARAMS,
        name="front",
    )(own_part, swapped_cores(oth_part), cosine, sine, decay, decay_row)

    queries = lax.all_gather(q_send, "z", axis=0)
    kv_own = copies_from(kv_send, ("z", "y"), SKEW)
    kv_oth = swapped_cores(kv_own)

    partial = pl.pallas_call(
        attend_kernel,
        in_specs=[SMEM] * 2 + [VMEM] * 5,
        out_specs=VMEM,
        out_shape=jax.ShapeDtypeStruct((8, SPAN, SPAN), BF16),
        scratch_shapes=[
            pltpu.VMEM((8, 2 * SPAN, 128), BF16),
            pltpu.VMEM((8, 80, 2 * SPAN), BF16),
            pltpu.VMEM((8, 3, 128, SPAN), BF16),
            pltpu.VMEM((8, 80, 3 * SPAN), F32),
        ],
        compiler_params=PARAMS,
        name="attend",
    )(plan, fade, queries, query_gate, kv_own, kv_oth, key_gate)
    parts = lax.all_to_all(partial, "z", 0, 0, tiled=True)

    out_own = w_own[:, 896:]
    out_oth = swapped_cores(out_own).reshape(64, 16, 384)
    out_own = out_own.reshape(64, 16, 384)
    w_out = jnp.where(
        c == 0, jnp.stack([out_own, out_oth], axis=1), jnp.stack([out_oth, out_own], axis=1)
    ).reshape(2048, 384)
    share = pl.pallas_call(
        back_kernel,
        in_specs=[VMEM] * 4,
        out_specs=VMEM,
        out_shape=jax.ShapeDtypeStruct((SPAN, 2048), BF16),
        scratch_shapes=[pltpu.VMEM((SPAN, 384), BF16)],
        compiler_params=PARAMS,
        name="back",
    )(parts, local, lifted, w_out)
    shares = lax.all_to_all(share.reshape(4, 64, 2048), "tp", 0, 0, tiled=True)
    return jnp.sum(shares.astype(F32), axis=0).astype(BF16)


def solution(mesh):
    finer = Mesh(mesh.devices.reshape(8, 8, 2, mesh.shape["tp"]), ("z", "y", "c", "tp"))
    everyone = ("z", "y", "c", "tp")
    placed = (
        P(everyone, None),
        P(),
        P(SP, "tp"),
        P(SP, "tp"),
        P(SP, "tp"),
        P(SP, "tp"),
        P(SP, "tp"),
        P(SP, "tp"),
        P("tp", SP),
        P("tp", SP),
        P(SP, "tp"),
        P("tp", None),
    )
    return jax.shard_map(
        body, mesh=finer, in_specs=placed, out_specs=P(everyone, None), check_vma=False
    )
```

```python
import jax
import jax.numpy as jnp
from jax import lax
from jax.experimental import pallas as pl
from jax.experimental.pallas import tpu as pltpu
from jax.sharding import Mesh
from jax.sharding import PartitionSpec as P

HEAD = 64
SPAN = 256
SP = ("z", "y", "c")
EPS = 1e-06
THETA = 10000.0
LOG2E = 1.4426950408889634
F32 = jnp.float32
BF16 = jnp.bfloat16
SKEW = [[((m - y) % 8) * 8 + y for y in range(8)] for m in range(8)]
NT = (((1,), (1,)), ((), ()))
TN = (((0,), (0,)), ((), ()))
VMEM = pl.BlockSpec(memory_space=pltpu.VMEM)
SMEM = pl.BlockSpec(memory_space=pltpu.SMEM)
PARAMS = pltpu.CompilerParams(vmem_limit_bytes=56 * 1024 * 1024)


def copies_from(shard, axis, groups=None):
    count = len(groups[0]) if groups else lax.axis_size(axis)
    copies = jnp.broadcast_to(shard, (count, *shard.shape))
    return lax.all_to_all(
        copies, axis, split_axis=0, concat_axis=0, tiled=True, axis_index_groups=groups
    )


def swapped_cores(value):
    return lax.ppermute(value, "c", [(0, 1), (1, 0)])


def three_parts(values):
    high = lax.reduce_precision(values, 8, 7)
    rest = values - high
    middle = lax.reduce_precision(rest, 8, 7)
    low = lax.reduce_precision(rest - middle, 8, 7)
    return [part.astype(BF16) for part in (high, middle, low)]


def project_kernel(rows, weights, own_out, oth_out):
    product = jnp.dot(rows[...], weights[...], preferred_element_type=F32)
    own_out[...] = product[:SPAN]
    oth_out[...] = product[SPAN:]


def turned(proj, at, cos, sin):
    first = proj[:, at : at + 32]
    second = proj[:, at + 32 : at + 64]
    return jnp.concatenate([first * cos - second * sin, first * sin + second * cos], axis=1)


def front_kernel(first_part, second_part, cosine, sine, decay, q_out, kv_out, proj_out):
    proj_out[...] = first_part[...] + second_part[...]
    cos = cosine[...]
    sin = sine[...]
    for h in range(3):
        key = turned(proj_out, 192 + h * HEAD, cos, sin).astype(BF16)
        value = proj_out[:, 384 + h * HEAD : 384 + (h + 1) * HEAD].astype(BF16)
        column = decay[:, h : h + 1]
        last = decay[SPAN - 1 : SPAN, h : h + 1]
        faded = (key.astype(F32) * jnp.exp(last - column)).astype(BF16)
        update = lax.dot_general(faded, value, TN, preferred_element_type=F32).astype(BF16)
        kv_out[SPAN + 32 * h : SPAN + 32 * (h + 1)] = jnp.concatenate(
            [update[:32], update[32:]], axis=1
        )
    q_out[192:] = jnp.zeros((HEAD, SPAN), BF16)
    q_out[:192] = jnp.transpose(proj_out[:, 576:768] * (HEAD ** (-0.5) * LOG2E)).astype(BF16)
    both = proj_out[:, 768:896]
    flipped = jnp.transpose(both)[HEAD:, :].astype(BF16)
    kv_out[:128] = jnp.concatenate([both[:128, :HEAD], both[128:, :HEAD]], axis=1).astype(BF16)
    kv_out[128:SPAN] = jnp.concatenate([flipped[:, :128], flipped[:, 128:]], axis=0)


def local_kernel(proj, cosine, sine, decay, decay_row, local_out, lifted_out):
    cos = cosine[...]
    sin = sine[...]
    place = lax.broadcasted_iota(jnp.int32, (SPAN, SPAN), 0)
    other = lax.broadcasted_iota(jnp.int32, (SPAN, SPAN), 1)
    causal = place >= other
    for h in range(3):
        query = (turned(proj, h * HEAD, cos, sin) * HEAD ** (-0.5)).astype(BF16)
        key = turned(proj, 192 + h * HEAD, cos, sin).astype(BF16)
        value = proj[:, 384 + h * HEAD : 384 + (h + 1) * HEAD].astype(BF16)
        column = decay[:, h : h + 1]
        scores = lax.dot_general(query, key, NT, preferred_element_type=F32)
        gap = jnp.where(causal, column - decay_row[h : h + 1, :], 0.0)
        weights = jnp.where(causal, scores * jnp.exp(gap), 0.0).astype(BF16)
        local_out[:, h * HEAD : (h + 1) * HEAD] = jnp.dot(
            weights, value, preferred_element_type=F32
        )
        lifted_out[:, h * HEAD : (h + 1) * HEAD] = (
            query.astype(F32) * jnp.exp(column)
        ).astype(BF16)


def attend_kernel(
    plan, fade, received, query_gate, kv_own, kv_oth, key_gate, out, keys, values, queries, total
):
    mine_z, mine_y, mine_c = (plan[65], plan[66], plan[67])
    extra = lax.broadcasted_iota(jnp.int32, (16, 2 * SPAN), 0)
    ones = jnp.where(extra == 0, 1.0, 0.0).astype(BF16)
    for y in range(8):
        for side, held in enumerate((kv_own, kv_oth)):
            packed = held[y, :128]
            at = side * SPAN
            keys[y, at : at + 128, :HEAD] = packed[:, :HEAD]
            keys[y, at + 128 : at + SPAN, :HEAD] = packed[:, HEAD:]
            keys[y, at : at + SPAN, HEAD:] = key_gate[side, y]
            values[y, :HEAD, at : at + 128] = held[y, 128:192]
            values[y, :HEAD, at + 128 : at + SPAN] = held[y, 192:SPAN]
        values[y, HEAD:, :] = ones
    for z in range(8):
        for h in range(3):
            queries[z, h, :HEAD] = received[z, h * HEAD : (h + 1) * HEAD]
            queries[z, h, HEAD:] = query_gate[z, h]
    total[...] = jnp.zeros_like(total)

    place = lax.broadcasted_iota(jnp.int32, (2 * SPAN, SPAN), 0)
    wanted = lax.broadcasted_iota(jnp.int32, (2 * SPAN, SPAN), 1)
    allowed = place <= jnp.where(place < SPAN, wanted, mine_c * (4 * SPAN) - 1)
    for h in range(3):
        scores = jnp.dot(keys[mine_y], queries[mine_z, h], preferred_element_type=F32)
        weights = jnp.where(allowed, jnp.exp2(scores), 0.0).astype(BF16)
        total[mine_z, :, h * SPAN : (h + 1) * SPAN] += jnp.dot(
            values[mine_y], weights, preferred_element_type=F32
        )

    def units(places):
        at = []
        for i in places:
            code = plan[i]
            at.append((code // 8, code % 8))
        chunks = [(z, y, h) for z, y in at for h in range(3)]

        def scored(z, y, h):
            return jnp.dot(keys[y], queries[z, h], preferred_element_type=F32)

        ready = scored(*chunks[0])
        for n, (z, y, h) in enumerate(chunks):
            ahead = scored(*chunks[n + 1]) if n + 1 < len(chunks) else None
            weights = jnp.exp2(ready).astype(BF16)
            total[z, :, h * SPAN : (h + 1) * SPAN] += jnp.dot(
                values[y], weights, preferred_element_type=F32
            )
            ready = ahead

    def pair(i, carry):
        units((2 * i, 2 * i + 1))
        return carry

    count = plan[64]
    lax.fori_loop(0, count // 2, pair, 0)

    @pl.when(count % 2 == 1)
    def _():
        units((count - 1,))

    for z in range(8):
        rows = []
        for h in range(3):
            out[z, h * HEAD : (h + 1) * HEAD] = total[z, :HEAD, h * SPAN : (h + 1) * SPAN].astype(
                BF16
            )
            rows.append(total[z, HEAD : HEAD + 1, h * SPAN : (h + 1) * SPAN])
        high = [row.astype(BF16).astype(F32) for row in rows]
        low = [row - big for row, big in zip(rows, high)]
        out[z, 192:208] = jnp.concatenate(
            high + low + [jnp.zeros((10, SPAN), F32)], axis=0
        ).astype(BF16)
    for z in range(8):
        sums = []
        for h in range(3):
            at = SPAN + 32 * h
            state = jnp.zeros((32, 128), F32)
            for side, held in enumerate((kv_own, kv_oth)):
                for y in range(8):
                    state = state + held[y, at : at + 32].astype(F32) * fade[
                        ((z * 2 + side) * 8 + y) * 3 + h
                    ]
            sums.append(state)
        sums = jnp.concatenate(sums, axis=0).astype(BF16)
        out[z, 208:, :128] = sums[:48]
        out[z, 208:, 128:] = sums[48:]


def back_kernel(parts, local, lifted, w_out, out, mixed):
    total = parts[0].astype(F32)
    for z in range(1, 8):
        total = total + parts[z].astype(F32)
    states = jnp.concatenate([total[208:, :128], total[208:, 128:]], axis=0)
    for h in range(3):
        held = states[32 * h : 32 * (h + 1)]
        held = jnp.concatenate([held[:, :HEAD], held[:, HEAD:]], axis=0).astype(BF16)
        raw = local[:, h * HEAD : (h + 1) * HEAD] + jnp.dot(
            lifted[:, h * HEAD : (h + 1) * HEAD], held, preferred_element_type=F32
        )
        centred = raw - jnp.mean(raw, axis=-1, keepdims=True)
        spread = jnp.mean(centred * centred, axis=-1, keepdims=True)
        mixed[:, h * HEAD : (h + 1) * HEAD] = (centred * lax.rsqrt(spread + EPS)).astype(BF16)
        weight = total[192 + h : 193 + h] + total[195 + h : 196 + h]
        attended = total[h * HEAD : (h + 1) * HEAD] / weight
        mixed[:, 192 + h * HEAD : 192 + (h + 1) * HEAD] = jnp.transpose(attended).astype(BF16)
    out[...] = lax.dot_general(
        mixed[...], w_out[...], NT, preferred_element_type=F32
    ).astype(BF16)


def body(
    tokens,
    pre_gain,
    w_query_ret,
    w_key_ret,
    w_value_ret,
    w_query_att,
    w_key_att,
    w_value_att,
    w_out_ret,
    w_out_att,
    retain_log,
    forget_total,
):
    z, y, c = (lax.axis_index("z"), lax.axis_index("y"), lax.axis_index("c"))
    decay = jnp.cumsum(retain_log, axis=0)
    ends = jnp.concatenate(three_parts(decay[-1]))
    shard = jnp.concatenate(
        [
            w_query_ret,
            w_key_ret,
            w_value_ret,
            w_query_att,
            w_key_att,
            w_value_att,
            w_out_ret.T,
            w_out_att.T,
            jnp.pad(ends[None, :], ((0, 15), (0, 119))),
        ],
        axis=1,
    )
    w_row = copies_from(shard, "y")
    line_ends = jnp.sum(w_row[:, 0, 1280:1289].reshape(8, 3, 3).astype(F32), axis=1)
    w_row = w_row[:, :, :1280].reshape(128, 1280)
    w_own = lax.all_gather(w_row, "z", axis=0, tiled=True)

    raw = tokens.astype(F32)
    normed = (
        raw * lax.rsqrt(jnp.mean(raw * raw, axis=-1, keepdims=True) + EPS) * pre_gain
    ).astype(BF16)
    halves = jnp.transpose(normed.reshape(64, 64, 2, 16), (2, 0, 1, 3)).reshape(2, 64, 1024)
    rows = copies_from(halves, "tp")
    kept = jnp.where(c == 0, rows[:, 0], rows[:, 1]).reshape(SPAN, 1024)
    sent = jnp.where(c == 0, rows[:, 1], rows[:, 0]).reshape(SPAN, 1024)
    came = swapped_cores(sent)
    rows = jnp.concatenate([kept, came], axis=0)

    here = z * 16 + y * 2 + c
    positions = (here * SPAN + jnp.arange(SPAN, dtype=jnp.int32)).astype(F32)
    inverse = THETA ** (-jnp.arange(32, dtype=F32) / 32)
    angles = positions[:, None] * inverse[None, :]
    cosine, sine = (jnp.cos(angles), jnp.sin(angles))
    decay_row = jnp.pad(decay.T, ((0, 5), (0, 0)))
    ends_own = copies_from(line_ends, "z")
    ends_oth = swapped_cores(ends_own)
    ends = jnp.where(
        c == 0,
        jnp.stack([ends_own, ends_oth], axis=2),
        jnp.stack([ends_oth, ends_own], axis=2),
    ).reshape(128, 3)

    gate = (forget_total * LOG2E).reshape(3, 8, 8, 2, SPAN)
    spans = jnp.arange(8, dtype=jnp.int32)
    key_z = (z + y - spans) % 8
    chosen = (spans[:, None] == key_z[None, :])[None, :, :, None, None]
    key_side = jnp.sum(jnp.where(chosen, gate, 0.0), axis=1)
    key_side = jnp.where(c == 0, key_side, key_side[:, :, ::-1])
    minus = jnp.stack(three_parts(-key_side), axis=1).reshape(9, 8, 2, SPAN)
    key_gate = jnp.concatenate(
        [minus, jnp.ones((3, 8, 2, SPAN), BF16), jnp.zeros((52, 8, 2, SPAN), BF16)], axis=0
    )
    key_gate = jnp.transpose(key_gate, (2, 1, 3, 0))
    mine = lax.dynamic_index_in_dim(
        lax.dynamic_index_in_dim(gate, y, 2, keepdims=False), c, 2, keepdims=False
    )
    plus = jnp.transpose(jnp.stack(three_parts(mine), axis=0), (2, 1, 0, 3))
    own_head = (
        jnp.arange(9, dtype=jnp.int32)[None, :] // 3 == jnp.arange(3, dtype=jnp.int32)[:, None]
    ).astype(BF16)
    query_gate = jnp.concatenate(
        [
            jnp.broadcast_to(own_head[None, :, :, None], (8, 3, 9, SPAN)),
            plus,
            jnp.zeros((8, 3, 52, SPAN), BF16),
        ],
        axis=2,
    )
    blocks = key_z * 16 + spans * 2
    blocks = jnp.stack([blocks + c, blocks + 1 - c])
    targets = spans * 16 + y * 2 + c
    index = jnp.arange(128, dtype=jnp.int32)
    between = (index > blocks[None, :, :, None]) & (index < targets[:, None, None, None])
    fade = jnp.sum(jnp.where(between[..., None], ends, 0.0), axis=3)
    earlier = blocks[None] < targets[:, None, None]
    fade = jnp.where(earlier[..., None], jnp.exp(fade), 0.0).reshape(384)
    needed = (
        (key_z[None, :] < spans[:, None])
        | ((key_z[None, :] == spans[:, None]) & (spans[None, :] < y))
    ).reshape(64)
    slot = jnp.cumsum(needed.astype(jnp.int32)) - 1
    order = jnp.arange(64, dtype=jnp.int32)
    units = jnp.sum(
        jnp.where(needed[None, :] & (slot[None, :] == order[:, None]), order[None, :], 0), axis=1
    )
    plan = jnp.concatenate([units, jnp.stack([jnp.sum(needed.astype(jnp.int32)), z, y, c])])

    own_part, oth_part = pl.pallas_call(
        project_kernel,
        grid=(1,),
        in_specs=[VMEM, pl.BlockSpec((1024, 896), lambda i: (0, 0))],
        out_specs=[VMEM] * 2,
        out_shape=[jax.ShapeDtypeStruct((SPAN, 896), F32)] * 2,
        compiler_params=PARAMS,
        name="project",
    )(rows, w_own)
    q_send, kv_send, proj = pl.pallas_call(
        front_kernel,
        in_specs=[VMEM] * 5,
        out_specs=[VMEM] * 3,
        out_shape=[
            jax.ShapeDtypeStruct((SPAN, SPAN), BF16),
            jax.ShapeDtypeStruct((SPAN + 96, 128), BF16),
            jax.ShapeDtypeStruct((SPAN, 896), F32),
        ],
        compiler_params=PARAMS,
        name="front",
    )(own_part, swapped_cores(oth_part), cosine, sine, decay)

    queries = lax.all_gather(q_send, "z", axis=0)
    kv_own = copies_from(kv_send, ("z", "y"), SKEW)
    kv_oth = swapped_cores(kv_own)
    local, lifted = pl.pallas_call(
        local_kernel,
        in_specs=[VMEM] * 5,
        out_specs=[VMEM] * 2,
        out_shape=[jax.ShapeDtypeStruct((SPAN, 192), F32), jax.ShapeDtypeStruct((SPAN, 192), BF16)],
        compiler_params=PARAMS,
        name="local",
    )(proj, cosine, sine, decay, decay_row)
    out_own = w_own[:, 896:]
    out_oth = swapped_cores(out_own).reshape(64, 16, 384)
    out_own = out_own.reshape(64, 16, 384)
    w_out = jnp.where(
        c == 0, jnp.stack([out_own, out_oth], axis=1), jnp.stack([out_oth, out_own], axis=1)
    ).reshape(2048, 384)

    partial = pl.pallas_call(
        attend_kernel,
        in_specs=[SMEM] * 2 + [VMEM] * 5,
        out_specs=VMEM,
        out_shape=jax.ShapeDtypeStruct((8, SPAN, SPAN), BF16),
        scratch_shapes=[
            pltpu.VMEM((8, 2 * SPAN, 128), BF16),
            pltpu.VMEM((8, 80, 2 * SPAN), BF16),
            pltpu.VMEM((8, 3, 128, SPAN), BF16),
            pltpu.VMEM((8, 80, 3 * SPAN), F32),
        ],
        compiler_params=PARAMS,
        name="attend",
    )(plan, fade, queries, query_gate, kv_own, kv_oth, key_gate)
    parts = lax.all_to_all(partial, "z", 0, 0, tiled=True)

    share = pl.pallas_call(
        back_kernel,
        in_specs=[VMEM] * 4,
        out_specs=VMEM,
        out_shape=jax.ShapeDtypeStruct((SPAN, 2048), BF16),
        scratch_shapes=[pltpu.VMEM((SPAN, 384), BF16)],
        compiler_params=PARAMS,
        name="back",
    )(parts, local, lifted, w_out)
    shares = lax.all_to_all(share.reshape(4, 64, 2048), "tp", 0, 0, tiled=True)
    return jnp.sum(shares.astype(F32), axis=0).astype(BF16)


def solution(mesh):
    finer = Mesh(mesh.devices.reshape(8, 8, 2, mesh.shape["tp"]), ("z", "y", "c", "tp"))
    everyone = ("z", "y", "c", "tp")
    placed = (
        P(everyone, None),
        P(),
        P(SP, "tp"),
        P(SP, "tp"),
        P(SP, "tp"),
        P(SP, "tp"),
        P(SP, "tp"),
        P(SP, "tp"),
        P("tp", SP),
        P("tp", SP),
        P(SP, "tp"),
        P("tp", None),
    )
    return jax.shard_map(
        body, mesh=finer, in_specs=placed, out_specs=P(everyone, None), check_vma=False
    )
```

```python
import jax
import jax.numpy as jnp
from jax import lax
from jax.experimental import pallas as pl
from jax.experimental.pallas import tpu as pltpu
from jax.sharding import Mesh
from jax.sharding import PartitionSpec as P

HEAD = 64
SPAN = 256
SP = ("z", "y", "c")
EPS = 1e-06
THETA = 10000.0
LOG2E = 1.4426950408889634
F32 = jnp.float32
BF16 = jnp.bfloat16
ROTATION = [(z * 8 + y, ((z + y) % 8) * 8 + y) for z in range(8) for y in range(8)]
NT = (((1,), (1,)), ((), ()))
TN = (((0,), (0,)), ((), ()))
VMEM = pl.BlockSpec(memory_space=pltpu.VMEM)
SMEM = pl.BlockSpec(memory_space=pltpu.SMEM)
PARAMS = pltpu.CompilerParams(vmem_limit_bytes=56 * 1024 * 1024)


def copies_from(shard, axis):
    copies = jnp.broadcast_to(shard, (lax.axis_size(axis), *shard.shape))
    return lax.all_to_all(copies, axis, split_axis=0, concat_axis=0, tiled=True)


def swapped_cores(value):
    return lax.ppermute(value, "c", [(0, 1), (1, 0)])


def three_parts(values):
    high = lax.reduce_precision(values, 8, 7)
    rest = values - high
    middle = lax.reduce_precision(rest, 8, 7)
    low = lax.reduce_precision(rest - middle, 8, 7)
    return [part.astype(BF16) for part in (high, middle, low)]


def project_kernel(rows, weights, own_out, oth_out):
    product = jnp.dot(rows[...], weights[...], preferred_element_type=F32)
    own_out[...] = product[:SPAN]
    oth_out[...] = product[SPAN:]


def turned(proj, at, cos, sin):
    first = proj[:, at : at + 32]
    second = proj[:, at + 32 : at + 64]
    return jnp.concatenate([first * cos - second * sin, first * sin + second * cos], axis=1)


def front_kernel(first_part, second_part, cosine, sine, decay, q_out, kv_out, proj_out):
    proj_out[...] = first_part[...] + second_part[...]
    cos = cosine[...]
    sin = sine[...]
    for h in range(3):
        key = turned(proj_out, 192 + h * HEAD, cos, sin).astype(BF16)
        value = proj_out[:, 384 + h * HEAD : 384 + (h + 1) * HEAD].astype(BF16)
        column = decay[:, h : h + 1]
        last = decay[SPAN - 1 : SPAN, h : h + 1]
        faded = (key.astype(F32) * jnp.exp(last - column)).astype(BF16)
        update = lax.dot_general(faded, value, TN, preferred_element_type=F32).astype(BF16)
        kv_out[SPAN + 32 * h : SPAN + 32 * (h + 1)] = jnp.concatenate(
            [update[:32], update[32:]], axis=1
        )
    q_out[192:] = jnp.zeros((HEAD, SPAN), BF16)
    q_out[:192] = jnp.transpose(proj_out[:, 576:768] * (HEAD ** (-0.5) * LOG2E)).astype(BF16)
    both = proj_out[:, 768:896]
    flipped = jnp.transpose(both)[HEAD:, :].astype(BF16)
    kv_out[:128] = jnp.concatenate([both[:128, :HEAD], both[128:, :HEAD]], axis=1).astype(BF16)
    kv_out[128:SPAN] = jnp.concatenate([flipped[:, :128], flipped[:, 128:]], axis=0)


def local_kernel(proj, cosine, sine, decay, decay_row, local_out, lifted_out):
    cos = cosine[...]
    sin = sine[...]
    place = lax.broadcasted_iota(jnp.int32, (SPAN, SPAN), 0)
    other = lax.broadcasted_iota(jnp.int32, (SPAN, SPAN), 1)
    causal = place >= other
    for h in range(3):
        query = (turned(proj, h * HEAD, cos, sin) * HEAD ** (-0.5)).astype(BF16)
        key = turned(proj, 192 + h * HEAD, cos, sin).astype(BF16)
        value = proj[:, 384 + h * HEAD : 384 + (h + 1) * HEAD].astype(BF16)
        column = decay[:, h : h + 1]
        scores = lax.dot_general(query, key, NT, preferred_element_type=F32)
        gap = jnp.where(causal, column - decay_row[h : h + 1, :], 0.0)
        weights = jnp.where(causal, scores * jnp.exp(gap), 0.0).astype(BF16)
        local_out[:, h * HEAD : (h + 1) * HEAD] = jnp.dot(
            weights, value, preferred_element_type=F32
        )
        lifted_out[:, h * HEAD : (h + 1) * HEAD] = (
            query.astype(F32) * jnp.exp(column)
        ).astype(BF16)


def attend_kernel(
    plan,
    fade,
    received,
    query_gate,
    kv_own,
    kv_oth,
    key_gate,
    out,
    keys,
    values,
    queries,
    total,
    even,
    odd,
):
    extra = lax.broadcasted_iota(jnp.int32, (16, 2 * SPAN), 0)
    ones = jnp.where(extra == 0, 1.0, 0.0).astype(BF16)
    for y in range(8):
        for side, held in enumerate((kv_own, kv_oth)):
            packed = held[y, :128]
            at = side * SPAN
            keys[y, at : at + 128, :HEAD] = packed[:, :HEAD]
            keys[y, at + 128 : at + SPAN, :HEAD] = packed[:, HEAD:]
            keys[y, at : at + SPAN, HEAD:] = key_gate[side, y]
            values[y, :HEAD, at : at + 128] = held[y, 128:192]
            values[y, :HEAD, at + 128 : at + SPAN] = held[y, 192:SPAN]
        values[y, HEAD:, :] = ones
    for z in range(8):
        for h in range(3):
            queries[z, h, :HEAD] = received[z, h * HEAD : (h + 1) * HEAD]
            queries[z, h, HEAD:] = query_gate[z, h]
    total[...] = jnp.zeros_like(total)

    place = lax.broadcasted_iota(jnp.int32, (2 * SPAN, SPAN), 0)
    wanted = lax.broadcasted_iota(jnp.int32, (2 * SPAN, SPAN), 1)
    allowed = place <= jnp.where(place < SPAN, wanted, plan[66] * (4 * SPAN) - 1)

    def weigh(i, held, h):
        z, y = (plan[i] // 8, plan[i] % 8)
        at = h * SPAN
        total[z, :, at : at + SPAN] += jnp.dot(
            values[y], held[:, at : at + SPAN], preferred_element_type=F32
        )

    def score(i, held, h, mask=None):
        z, y = (plan[i] // 8, plan[i] % 8)
        for at in (0, SPAN):
            weights = jnp.exp2(
                jnp.dot(keys[y, at : at + SPAN], queries[z, h], preferred_element_type=F32)
            )
            if mask is not None:
                weights = jnp.where(mask[at : at + SPAN], weights, 0.0)
            held[at : at + SPAN, h * SPAN : (h + 1) * SPAN] = weights.astype(BF16)

    for h in range(3):
        score(0, even, h, allowed)

    def pair(i, carry):
        for h in range(3):
            score(2 * i + 1, odd, h)
            weigh(2 * i, even, h)
        for h in range(3):
            score(2 * i + 2, even, h)
            weigh(2 * i + 1, odd, h)
        return carry

    count = plan[65]
    lax.fori_loop(0, count // 2, pair, 0)

    @pl.when(count % 2 == 1)
    def _():
        for h in range(3):
            weigh(count - 1, even, h)

    for z in range(8):
        rows = []
        for h in range(3):
            out[z, h * HEAD : (h + 1) * HEAD] = total[z, :HEAD, h * SPAN : (h + 1) * SPAN].astype(
                BF16
            )
            rows.append(total[z, HEAD : HEAD + 1, h * SPAN : (h + 1) * SPAN])
        high = [row.astype(BF16).astype(F32) for row in rows]
        low = [row - big for row, big in zip(rows, high)]
        out[z, 192:208] = jnp.concatenate(
            high + low + [jnp.zeros((10, SPAN), F32)], axis=0
        ).astype(BF16)
    for z in range(8):
        sums = []
        for h in range(3):
            at = SPAN + 32 * h
            state = jnp.zeros((32, 128), F32)
            for side, held in enumerate((kv_own, kv_oth)):
                for y in range(8):
                    state = state + held[y, at : at + 32].astype(F32) * fade[
                        ((z * 2 + side) * 8 + y) * 3 + h
                    ]
            sums.append(state)
        sums = jnp.concatenate(sums, axis=0).astype(BF16)
        out[z, 208:, :128] = sums[:48]
        out[z, 208:, 128:] = sums[48:]


def back_kernel(parts, local, lifted, w_out, out, mixed):
    total = parts[0].astype(F32)
    for z in range(1, 8):
        total = total + parts[z].astype(F32)
    states = jnp.concatenate([total[208:, :128], total[208:, 128:]], axis=0)
    for h in range(3):
        held = states[32 * h : 32 * (h + 1)]
        held = jnp.concatenate([held[:, :HEAD], held[:, HEAD:]], axis=0).astype(BF16)
        raw = local[:, h * HEAD : (h + 1) * HEAD] + jnp.dot(
            lifted[:, h * HEAD : (h + 1) * HEAD], held, preferred_element_type=F32
        )
        centred = raw - jnp.mean(raw, axis=-1, keepdims=True)
        spread = jnp.mean(centred * centred, axis=-1, keepdims=True)
        mixed[:, h * HEAD : (h + 1) * HEAD] = (centred * lax.rsqrt(spread + EPS)).astype(BF16)
        weight = total[192 + h : 193 + h] + total[195 + h : 196 + h]
        attended = total[h * HEAD : (h + 1) * HEAD] / weight
        mixed[:, 192 + h * HEAD : 192 + (h + 1) * HEAD] = jnp.transpose(attended).astype(BF16)
    out[...] = lax.dot_general(
        mixed[...], w_out[...], NT, preferred_element_type=F32
    ).astype(BF16)


def body(
    tokens,
    pre_gain,
    w_query_ret,
    w_key_ret,
    w_value_ret,
    w_query_att,
    w_key_att,
    w_value_att,
    w_out_ret,
    w_out_att,
    retain_log,
    forget_total,
):
    z, y, c = (lax.axis_index("z"), lax.axis_index("y"), lax.axis_index("c"))
    decay = jnp.cumsum(retain_log, axis=0)
    ends = jnp.concatenate(three_parts(decay[-1]))
    shard = jnp.concatenate(
        [
            w_query_ret,
            w_key_ret,
            w_value_ret,
            w_query_att,
            w_key_att,
            w_value_att,
            w_out_ret.T,
            w_out_att.T,
            jnp.pad(ends[None, :], ((0, 15), (0, 119))),
        ],
        axis=1,
    )
    w_row = copies_from(shard, "y")
    line_ends = jnp.sum(w_row[:, 0, 1280:1289].reshape(8, 3, 3).astype(F32), axis=1)
    w_row = w_row[:, :, :1280].reshape(128, 1280)
    w_own = lax.all_gather(w_row, "z", axis=0, tiled=True)

    raw = tokens.astype(F32)
    normed = (
        raw * lax.rsqrt(jnp.mean(raw * raw, axis=-1, keepdims=True) + EPS) * pre_gain
    ).astype(BF16)
    halves = jnp.transpose(normed.reshape(64, 64, 2, 16), (2, 0, 1, 3)).reshape(2, 64, 1024)
    rows = copies_from(halves, "tp")
    kept = jnp.where(c == 0, rows[:, 0], rows[:, 1]).reshape(SPAN, 1024)
    sent = jnp.where(c == 0, rows[:, 1], rows[:, 0]).reshape(SPAN, 1024)
    came = swapped_cores(sent)
    rows = jnp.concatenate([kept, came], axis=0)

    here = z * 16 + y * 2 + c
    positions = (here * SPAN + jnp.arange(SPAN, dtype=jnp.int32)).astype(F32)
    inverse = THETA ** (-jnp.arange(32, dtype=F32) / 32)
    angles = positions[:, None] * inverse[None, :]
    cosine, sine = (jnp.cos(angles), jnp.sin(angles))
    decay_row = jnp.pad(decay.T, ((0, 5), (0, 0)))
    ends_own = copies_from(line_ends, "z")
    ends_oth = swapped_cores(ends_own)
    ends = jnp.where(
        c == 0,
        jnp.stack([ends_own, ends_oth], axis=2),
        jnp.stack([ends_oth, ends_own], axis=2),
    ).reshape(128, 3)

    gate = (forget_total * LOG2E).reshape(3, 8, 8, 2, SPAN)
    spans = jnp.arange(8, dtype=jnp.int32)
    key_z = (z - spans) % 8
    chosen = (spans[:, None] == key_z[None, :])[None, :, :, None, None]
    key_side = jnp.sum(jnp.where(chosen, gate, 0.0), axis=1)
    key_side = jnp.where(c == 0, key_side, key_side[:, :, ::-1])
    minus = jnp.stack(three_parts(-key_side), axis=1).reshape(9, 8, 2, SPAN)
    key_gate = jnp.concatenate(
        [minus, jnp.ones((3, 8, 2, SPAN), BF16), jnp.zeros((52, 8, 2, SPAN), BF16)], axis=0
    )
    key_gate = jnp.transpose(key_gate, (2, 1, 3, 0))
    mine = lax.dynamic_index_in_dim(
        lax.dynamic_index_in_dim(gate, y, 2, keepdims=False), c, 2, keepdims=False
    )
    plus = jnp.transpose(jnp.stack(three_parts(mine), axis=0), (2, 1, 0, 3))
    own_head = (
        jnp.arange(9, dtype=jnp.int32)[None, :] // 3 == jnp.arange(3, dtype=jnp.int32)[:, None]
    ).astype(BF16)
    query_gate = jnp.concatenate(
        [
            jnp.broadcast_to(own_head[None, :, :, None], (8, 3, 9, SPAN)),
            plus,
            jnp.zeros((8, 3, 52, SPAN), BF16),
        ],
        axis=2,
    )
    blocks = key_z * 16 + spans * 2
    blocks = jnp.stack([blocks + c, blocks + 1 - c])
    targets = spans * 16 + y * 2 + c
    index = jnp.arange(128, dtype=jnp.int32)
    between = (index > blocks[None, :, :, None]) & (index < targets[:, None, None, None])
    fade = jnp.sum(jnp.where(between[..., None], ends, 0.0), axis=3)
    earlier = blocks[None] < targets[:, None, None]
    fade = jnp.where(earlier[..., None], jnp.exp(fade), 0.0).reshape(384)
    needed = (
        (key_z[None, :] < spans[:, None])
        | ((key_z[None, :] == spans[:, None]) & (spans[None, :] < y))
    ).reshape(64)
    slot = jnp.cumsum(needed.astype(jnp.int32)) - 1
    order = jnp.arange(64, dtype=jnp.int32)
    units = jnp.sum(
        jnp.where(needed[None, :] & (slot[None, :] == order[:, None]), order[None, :], 0), axis=1
    )
    own = jnp.stack([(z - y) % 8 * 8 + y])
    plan = jnp.concatenate([own, units, jnp.stack([jnp.sum(needed.astype(jnp.int32)) + 1, c])])

    own_part, oth_part = pl.pallas_call(
        project_kernel,
        grid=(1,),
        in_specs=[VMEM, pl.BlockSpec((1024, 896), lambda i: (0, 0))],
        out_specs=[VMEM] * 2,
        out_shape=[jax.ShapeDtypeStruct((SPAN, 896), F32)] * 2,
        compiler_params=PARAMS,
        name="project",
    )(rows, w_own)
    q_send, kv_send, proj = pl.pallas_call(
        front_kernel,
        in_specs=[VMEM] * 5,
        out_specs=[VMEM] * 3,
        out_shape=[
            jax.ShapeDtypeStruct((SPAN, SPAN), BF16),
            jax.ShapeDtypeStruct((SPAN + 96, 128), BF16),
            jax.ShapeDtypeStruct((SPAN, 896), F32),
        ],
        compiler_params=PARAMS,
        name="front",
    )(own_part, swapped_cores(oth_part), cosine, sine, decay)

    queries = lax.all_gather(q_send, "z", axis=0)
    kv_own = copies_from(lax.ppermute(kv_send, ("z", "y"), ROTATION), "y")
    kv_oth = swapped_cores(kv_own)
    local, lifted = pl.pallas_call(
        local_kernel,
        in_specs=[VMEM] * 5,
        out_specs=[VMEM] * 2,
        out_shape=[jax.ShapeDtypeStruct((SPAN, 192), F32), jax.ShapeDtypeStruct((SPAN, 192), BF16)],
        compiler_params=PARAMS,
        name="local",
    )(proj, cosine, sine, decay, decay_row)
    out_own = w_own[:, 896:]
    out_oth = swapped_cores(out_own).reshape(64, 16, 384)
    out_own = out_own.reshape(64, 16, 384)
    w_out = jnp.where(
        c == 0, jnp.stack([out_own, out_oth], axis=1), jnp.stack([out_oth, out_own], axis=1)
    ).reshape(2048, 384)

    partial = pl.pallas_call(
        attend_kernel,
        in_specs=[SMEM] * 2 + [VMEM] * 5,
        out_specs=VMEM,
        out_shape=jax.ShapeDtypeStruct((8, SPAN, SPAN), BF16),
        scratch_shapes=[
            pltpu.VMEM((8, 2 * SPAN, 128), BF16),
            pltpu.VMEM((8, 80, 2 * SPAN), BF16),
            pltpu.VMEM((8, 3, 128, SPAN), BF16),
            pltpu.VMEM((8, 80, 3 * SPAN), F32),
            pltpu.VMEM((2 * SPAN, 3 * SPAN), BF16),
            pltpu.VMEM((2 * SPAN, 3 * SPAN), BF16),
        ],
        compiler_params=PARAMS,
        name="attend",
    )(plan, fade, queries, query_gate, kv_own, kv_oth, key_gate)
    parts = lax.all_to_all(partial, "z", 0, 0, tiled=True)

    share = pl.pallas_call(
        back_kernel,
        in_specs=[VMEM] * 4,
        out_specs=VMEM,
        out_shape=jax.ShapeDtypeStruct((SPAN, 2048), BF16),
        scratch_shapes=[pltpu.VMEM((SPAN, 384), BF16)],
        compiler_params=PARAMS,
        name="back",
    )(parts, local, lifted, w_out)
    shares = lax.all_to_all(share.reshape(4, 64, 2048), "tp", 0, 0, tiled=True)
    return jnp.sum(shares.astype(F32), axis=0).astype(BF16)


def solution(mesh):
    finer = Mesh(mesh.devices.reshape(8, 8, 2, mesh.shape["tp"]), ("z", "y", "c", "tp"))
    everyone = ("z", "y", "c", "tp")
    placed = (
        P(everyone, None),
        P(),
        P(SP, "tp"),
        P(SP, "tp"),
        P(SP, "tp"),
        P(SP, "tp"),
        P(SP, "tp"),
        P(SP, "tp"),
        P("tp", SP),
        P("tp", SP),
        P(SP, "tp"),
        P("tp", None),
    )
    return jax.shard_map(
        body, mesh=finer, in_specs=placed, out_specs=P(everyone, None), check_vma=False
    )
```

```python
import jax
import jax.numpy as jnp
from jax import lax
from jax.experimental import pallas as pl
from jax.experimental.pallas import tpu as pltpu
from jax.sharding import Mesh
from jax.sharding import PartitionSpec as P

HEAD = 64
SPAN = 256
SP = ("z", "y", "c")
EPS = 1e-06
THETA = 10000.0
LOG2E = 1.4426950408889634
F32 = jnp.float32
BF16 = jnp.bfloat16
ROTATION = [(z * 8 + y, ((z + y) % 8) * 8 + y) for z in range(8) for y in range(8)]
NT = (((1,), (1,)), ((), ()))
TN = (((0,), (0,)), ((), ()))
VMEM = pl.BlockSpec(memory_space=pltpu.VMEM)
SMEM = pl.BlockSpec(memory_space=pltpu.SMEM)
PARAMS = pltpu.CompilerParams(vmem_limit_bytes=56 * 1024 * 1024)


def copies_from(shard, axis):
    copies = jnp.broadcast_to(shard, (lax.axis_size(axis), *shard.shape))
    return lax.all_to_all(copies, axis, split_axis=0, concat_axis=0, tiled=True)


def swapped_cores(value):
    return lax.ppermute(value, "c", [(0, 1), (1, 0)])


def three_parts(values):
    high = lax.reduce_precision(values, 8, 7)
    rest = values - high
    middle = lax.reduce_precision(rest, 8, 7)
    low = lax.reduce_precision(rest - middle, 8, 7)
    return [part.astype(BF16) for part in (high, middle, low)]


def project_kernel(rows, weights, own_out, oth_out):
    product = jnp.dot(rows[...], weights[...], preferred_element_type=F32)
    own_out[...] = product[:SPAN]
    oth_out[...] = product[SPAN:]


def turned(proj, at, cos, sin):
    first = proj[:, at : at + 32]
    second = proj[:, at + 32 : at + 64]
    return jnp.concatenate([first * cos - second * sin, first * sin + second * cos], axis=1)


def front_kernel(first_part, second_part, cosine, sine, decay, q_out, kv_out, proj_out):
    proj_out[...] = first_part[...] + second_part[...]
    cos = cosine[...]
    sin = sine[...]
    for h in range(3):
        key = turned(proj_out, 192 + h * HEAD, cos, sin).astype(BF16)
        value = proj_out[:, 384 + h * HEAD : 384 + (h + 1) * HEAD].astype(BF16)
        column = decay[:, h : h + 1]
        last = decay[SPAN - 1 : SPAN, h : h + 1]
        faded = (key.astype(F32) * jnp.exp(last - column)).astype(BF16)
        update = lax.dot_general(faded, value, TN, preferred_element_type=F32).astype(BF16)
        kv_out[SPAN + 32 * h : SPAN + 32 * (h + 1)] = jnp.concatenate(
            [update[:32], update[32:]], axis=1
        )
    q_out[192:] = jnp.zeros((HEAD, SPAN), BF16)
    q_out[:192] = jnp.transpose(proj_out[:, 576:768] * (HEAD ** (-0.5) * LOG2E)).astype(BF16)
    both = proj_out[:, 768:896]
    flipped = jnp.transpose(both)[HEAD:, :].astype(BF16)
    kv_out[:128] = jnp.concatenate([both[:128, :HEAD], both[128:, :HEAD]], axis=1).astype(BF16)
    kv_out[128:SPAN] = jnp.concatenate([flipped[:, :128], flipped[:, 128:]], axis=0)


def local_kernel(proj, cosine, sine, decay, decay_row, local_out, lifted_out):
    cos = cosine[...]
    sin = sine[...]
    place = lax.broadcasted_iota(jnp.int32, (SPAN, SPAN), 0)
    other = lax.broadcasted_iota(jnp.int32, (SPAN, SPAN), 1)
    causal = place >= other
    for h in range(3):
        query = (turned(proj, h * HEAD, cos, sin) * HEAD ** (-0.5)).astype(BF16)
        key = turned(proj, 192 + h * HEAD, cos, sin).astype(BF16)
        value = proj[:, 384 + h * HEAD : 384 + (h + 1) * HEAD].astype(BF16)
        column = decay[:, h : h + 1]
        scores = lax.dot_general(query, key, NT, preferred_element_type=F32)
        gap = jnp.where(causal, column - decay_row[h : h + 1, :], 0.0)
        weights = jnp.where(causal, scores * jnp.exp(gap), 0.0).astype(BF16)
        local_out[:, h * HEAD : (h + 1) * HEAD] = jnp.dot(
            weights, value, preferred_element_type=F32
        )
        lifted_out[:, h * HEAD : (h + 1) * HEAD] = (
            query.astype(F32) * jnp.exp(column)
        ).astype(BF16)


def prepare_kernel(fade, kv_own, kv_oth, key_gate, keys, values, states):
    extra = lax.broadcasted_iota(jnp.int32, (16, 2 * SPAN), 0)
    ones = jnp.where(extra == 0, 1.0, 0.0).astype(BF16)
    for y in range(8):
        for side, held in enumerate((kv_own, kv_oth)):
            packed = held[y, :128]
            at = side * SPAN
            keys[y, at : at + 128, :HEAD] = packed[:, :HEAD]
            keys[y, at + 128 : at + SPAN, :HEAD] = packed[:, HEAD:]
            keys[y, at : at + SPAN, HEAD:] = key_gate[side, y]
            values[y, :HEAD, at : at + 128] = held[y, 128:192]
            values[y, :HEAD, at + 128 : at + SPAN] = held[y, 192:SPAN]
        values[y, HEAD:, :] = ones
    for z in range(8):
        sums = []
        for h in range(3):
            at = SPAN + 32 * h
            state = jnp.zeros((32, 128), F32)
            for side, held in enumerate((kv_own, kv_oth)):
                for y in range(8):
                    state = state + held[y, at : at + 32].astype(F32) * fade[
                        ((z * 2 + side) * 8 + y) * 3 + h
                    ]
            sums.append(state)
        sums = jnp.concatenate(sums, axis=0).astype(BF16)
        states[z, :, :128] = sums[:48]
        states[z, :, 128:] = sums[48:]


def attend_kernel(
    plan, received, query_gate, keys, values, states, out, queries, total, even, odd
):
    for z in range(8):
        for h in range(3):
            queries[z, h, :HEAD] = received[z, h * HEAD : (h + 1) * HEAD]
            queries[z, h, HEAD:] = query_gate[z, h]
    total[...] = jnp.zeros_like(total)

    place = lax.broadcasted_iota(jnp.int32, (2 * SPAN, SPAN), 0)
    wanted = lax.broadcasted_iota(jnp.int32, (2 * SPAN, SPAN), 1)
    allowed = place <= jnp.where(place < SPAN, wanted, plan[66] * (4 * SPAN) - 1)

    def weigh(i, held, h):
        z, y = (plan[i] // 8, plan[i] % 8)
        at = h * SPAN
        total[z, :, at : at + SPAN] += jnp.dot(
            values[y], held[:, at : at + SPAN], preferred_element_type=F32
        )

    def score(i, held, h, mask=None):
        z, y = (plan[i] // 8, plan[i] % 8)
        for at in (0, SPAN):
            weights = jnp.exp2(
                jnp.dot(keys[y, at : at + SPAN], queries[z, h], preferred_element_type=F32)
            )
            if mask is not None:
                weights = jnp.where(mask[at : at + SPAN], weights, 0.0)
            held[at : at + SPAN, h * SPAN : (h + 1) * SPAN] = weights.astype(BF16)

    for h in range(3):
        score(0, even, h, allowed)

    def pair(i, carry):
        for h in range(3):
            score(2 * i + 1, odd, h)
            weigh(2 * i, even, h)
        for h in range(3):
            score(2 * i + 2, even, h)
            weigh(2 * i + 1, odd, h)
        return carry

    count = plan[65]
    lax.fori_loop(0, count // 2, pair, 0)

    @pl.when(count % 2 == 1)
    def _():
        for h in range(3):
            weigh(count - 1, even, h)

    for z in range(8):
        rows = []
        for h in range(3):
            out[z, h * HEAD : (h + 1) * HEAD] = total[z, :HEAD, h * SPAN : (h + 1) * SPAN].astype(
                BF16
            )
            rows.append(total[z, HEAD : HEAD + 1, h * SPAN : (h + 1) * SPAN])
        high = [row.astype(BF16).astype(F32) for row in rows]
        low = [row - big for row, big in zip(rows, high)]
        out[z, 192:208] = jnp.concatenate(
            high + low + [jnp.zeros((10, SPAN), F32)], axis=0
        ).astype(BF16)
        out[z, 208:] = states[z]


def back_kernel(parts, local, lifted, w_out, out, mixed):
    total = parts[0].astype(F32)
    for z in range(1, 8):
        total = total + parts[z].astype(F32)
    states = jnp.concatenate([total[208:, :128], total[208:, 128:]], axis=0)
    for h in range(3):
        held = states[32 * h : 32 * (h + 1)]
        held = jnp.concatenate([held[:, :HEAD], held[:, HEAD:]], axis=0).astype(BF16)
        raw = local[:, h * HEAD : (h + 1) * HEAD] + jnp.dot(
            lifted[:, h * HEAD : (h + 1) * HEAD], held, preferred_element_type=F32
        )
        centred = raw - jnp.mean(raw, axis=-1, keepdims=True)
        spread = jnp.mean(centred * centred, axis=-1, keepdims=True)
        mixed[:, h * HEAD : (h + 1) * HEAD] = (centred * lax.rsqrt(spread + EPS)).astype(BF16)
        weight = total[192 + h : 193 + h] + total[195 + h : 196 + h]
        attended = total[h * HEAD : (h + 1) * HEAD] / weight
        mixed[:, 192 + h * HEAD : 192 + (h + 1) * HEAD] = jnp.transpose(attended).astype(BF16)
    out[...] = lax.dot_general(
        mixed[...], w_out[...], NT, preferred_element_type=F32
    ).astype(BF16)


def body(
    tokens,
    pre_gain,
    w_query_ret,
    w_key_ret,
    w_value_ret,
    w_query_att,
    w_key_att,
    w_value_att,
    w_out_ret,
    w_out_att,
    retain_log,
    forget_total,
):
    z, y, c = (lax.axis_index("z"), lax.axis_index("y"), lax.axis_index("c"))
    ends = jnp.concatenate(three_parts(jnp.sum(retain_log, axis=0)))
    shard = jnp.concatenate(
        [
            w_query_ret,
            w_key_ret,
            w_value_ret,
            w_query_att,
            w_key_att,
            w_value_att,
            w_out_ret.T,
            w_out_att.T,
            jnp.pad(ends[None, :], ((0, 15), (0, 119))),
        ],
        axis=1,
    )
    w_row = copies_from(shard, "y")
    line_ends = jnp.sum(w_row[:, 0, 1280:1289].reshape(8, 3, 3).astype(F32), axis=1)
    w_row = w_row[:, :, :1280].reshape(128, 1280)
    w_own = lax.all_gather(w_row, "z", axis=0, tiled=True)

    raw = tokens.astype(F32)
    normed = (
        raw * lax.rsqrt(jnp.mean(raw * raw, axis=-1, keepdims=True) + EPS) * pre_gain
    ).astype(BF16)
    halves = jnp.transpose(normed.reshape(64, 64, 2, 16), (2, 0, 1, 3)).reshape(2, 64, 1024)
    rows = copies_from(halves, "tp")
    kept = jnp.where(c == 0, rows[:, 0], rows[:, 1]).reshape(SPAN, 1024)
    sent = jnp.where(c == 0, rows[:, 1], rows[:, 0]).reshape(SPAN, 1024)
    came = swapped_cores(sent)
    rows = jnp.concatenate([kept, came], axis=0)

    here = z * 16 + y * 2 + c
    positions = (here * SPAN + jnp.arange(SPAN, dtype=jnp.int32)).astype(F32)
    inverse = THETA ** (-jnp.arange(32, dtype=F32) / 32)
    angles = positions[:, None] * inverse[None, :]
    cosine, sine = (jnp.cos(angles), jnp.sin(angles))
    decay = jnp.cumsum(retain_log, axis=0)
    decay_row = jnp.pad(decay.T, ((0, 5), (0, 0)))
    ends_own = copies_from(line_ends, "z")
    ends_oth = swapped_cores(ends_own)
    ends = jnp.where(
        c == 0,
        jnp.stack([ends_own, ends_oth], axis=2),
        jnp.stack([ends_oth, ends_own], axis=2),
    ).reshape(128, 3)

    gate = (forget_total * LOG2E).reshape(3, 8, 8, 2, SPAN)
    spans = jnp.arange(8, dtype=jnp.int32)
    key_z = (z - spans) % 8
    chosen = (spans[:, None] == key_z[None, :])[None, :, :, None, None]
    key_side = jnp.sum(jnp.where(chosen, gate, 0.0), axis=1)
    key_side = jnp.where(c == 0, key_side, key_side[:, :, ::-1])
    minus = jnp.stack(three_parts(-key_side), axis=1).reshape(9, 8, 2, SPAN)
    key_gate = jnp.concatenate(
        [minus, jnp.ones((3, 8, 2, SPAN), BF16), jnp.zeros((52, 8, 2, SPAN), BF16)], axis=0
    )
    key_gate = jnp.transpose(key_gate, (2, 1, 3, 0))
    mine = lax.dynamic_index_in_dim(
        lax.dynamic_index_in_dim(gate, y, 2, keepdims=False), c, 2, keepdims=False
    )
    plus = jnp.transpose(jnp.stack(three_parts(mine), axis=0), (2, 1, 0, 3))
    own_head = (
        jnp.arange(9, dtype=jnp.int32)[None, :] // 3 == jnp.arange(3, dtype=jnp.int32)[:, None]
    ).astype(BF16)
    query_gate = jnp.concatenate(
        [
            jnp.broadcast_to(own_head[None, :, :, None], (8, 3, 9, SPAN)),
            plus,
            jnp.zeros((8, 3, 52, SPAN), BF16),
        ],
        axis=2,
    )
    blocks = key_z * 16 + spans * 2
    blocks = jnp.stack([blocks + c, blocks + 1 - c])
    targets = spans * 16 + y * 2 + c
    index = jnp.arange(128, dtype=jnp.int32)
    between = (index > blocks[None, :, :, None]) & (index < targets[:, None, None, None])
    fade = jnp.sum(jnp.where(between[..., None], ends, 0.0), axis=3)
    earlier = blocks[None] < targets[:, None, None]
    fade = jnp.where(earlier[..., None], jnp.exp(fade), 0.0).reshape(384)
    needed = (
        (key_z[None, :] < spans[:, None])
        | ((key_z[None, :] == spans[:, None]) & (spans[None, :] < y))
    ).reshape(64)
    slot = jnp.cumsum(needed.astype(jnp.int32)) - 1
    order = jnp.arange(64, dtype=jnp.int32)
    units = jnp.sum(
        jnp.where(needed[None, :] & (slot[None, :] == order[:, None]), order[None, :], 0), axis=1
    )
    own = jnp.stack([(z - y) % 8 * 8 + y])
    plan = jnp.concatenate([own, units, jnp.stack([jnp.sum(needed.astype(jnp.int32)) + 1, c])])

    own_part, oth_part = pl.pallas_call(
        project_kernel,
        grid=(1,),
        in_specs=[VMEM, pl.BlockSpec((1024, 896), lambda i: (0, 0))],
        out_specs=[VMEM] * 2,
        out_shape=[jax.ShapeDtypeStruct((SPAN, 896), F32)] * 2,
        compiler_params=PARAMS,
        name="project",
    )(rows, w_own)
    q_send, kv_send, proj = pl.pallas_call(
        front_kernel,
        in_specs=[VMEM] * 5,
        out_specs=[VMEM] * 3,
        out_shape=[
            jax.ShapeDtypeStruct((SPAN, SPAN), BF16),
            jax.ShapeDtypeStruct((SPAN + 96, 128), BF16),
            jax.ShapeDtypeStruct((SPAN, 896), F32),
        ],
        compiler_params=PARAMS,
        name="front",
    )(own_part, swapped_cores(oth_part), cosine, sine, decay)

    queries = lax.all_gather(q_send, "z", axis=0)
    kv_send = lax.ppermute(kv_send, ("z", "y"), ROTATION)
    kv_own = copies_from(kv_send, "y")
    kv_oth = swapped_cores(kv_own)
    local, lifted = pl.pallas_call(
        local_kernel,
        in_specs=[VMEM] * 5,
        out_specs=[VMEM] * 2,
        out_shape=[jax.ShapeDtypeStruct((SPAN, 192), F32), jax.ShapeDtypeStruct((SPAN, 192), BF16)],
        compiler_params=PARAMS,
        name="local",
    )(proj, cosine, sine, decay, decay_row)
    out_own = w_own[:, 896:]
    out_oth = swapped_cores(out_own).reshape(64, 16, 384)
    out_own = out_own.reshape(64, 16, 384)
    w_out = jnp.where(
        c == 0, jnp.stack([out_own, out_oth], axis=1), jnp.stack([out_oth, out_own], axis=1)
    ).reshape(2048, 384)

    keys, values, states = pl.pallas_call(
        prepare_kernel,
        in_specs=[SMEM] + [VMEM] * 3,
        out_specs=[VMEM] * 3,
        out_shape=[
            jax.ShapeDtypeStruct((8, 2 * SPAN, 128), BF16),
            jax.ShapeDtypeStruct((8, 80, 2 * SPAN), BF16),
            jax.ShapeDtypeStruct((8, 48, SPAN), BF16),
        ],
        compiler_params=PARAMS,
        name="prepare",
    )(fade, kv_own, kv_oth, key_gate)
    partial = pl.pallas_call(
        attend_kernel,
        in_specs=[SMEM] + [VMEM] * 5,
        out_specs=VMEM,
        out_shape=jax.ShapeDtypeStruct((8, SPAN, SPAN), BF16),
        scratch_shapes=[
            pltpu.VMEM((8, 3, 128, SPAN), BF16),
            pltpu.VMEM((8, 80, 3 * SPAN), F32),
            pltpu.VMEM((2 * SPAN, 3 * SPAN), BF16),
            pltpu.VMEM((2 * SPAN, 3 * SPAN), BF16),
        ],
        compiler_params=PARAMS,
        name="attend",
    )(plan, queries, query_gate, keys, values, states)
    parts = lax.all_to_all(partial, "z", 0, 0, tiled=True)

    share = pl.pallas_call(
        back_kernel,
        in_specs=[VMEM] * 4,
        out_specs=VMEM,
        out_shape=jax.ShapeDtypeStruct((SPAN, 2048), BF16),
        scratch_shapes=[pltpu.VMEM((SPAN, 384), BF16)],
        compiler_params=PARAMS,
        name="back",
    )(parts, local, lifted, w_out)
    shares = lax.all_to_all(share.reshape(4, 64, 2048), "tp", 0, 0, tiled=True)
    return jnp.sum(shares.astype(F32), axis=0).astype(BF16)


def solution(mesh):
    finer = Mesh(mesh.devices.reshape(8, 8, 2, mesh.shape["tp"]), ("z", "y", "c", "tp"))
    everyone = ("z", "y", "c", "tp")
    placed = (
        P(everyone, None),
        P(),
        P(SP, "tp"),
        P(SP, "tp"),
        P(SP, "tp"),
        P(SP, "tp"),
        P(SP, "tp"),
        P(SP, "tp"),
        P("tp", SP),
        P("tp", SP),
        P(SP, "tp"),
        P("tp", None),
    )
    return jax.shard_map(
        body, mesh=finer, in_specs=placed, out_specs=P(everyone, None), check_vma=False
    )
```

```python
import functools

import jax
import jax.numpy as jnp
from jax import lax
from jax.experimental import pallas as pl
from jax.experimental.pallas import tpu as pltpu
from jax.sharding import Mesh
from jax.sharding import PartitionSpec as P

HEAD = 64
SPAN = 256
SP = ("z", "y", "c")
EPS = 1e-06
THETA = 10000.0
LOG2E = 1.4426950408889634
F32 = jnp.float32
BF16 = jnp.bfloat16
ROTATION = [(z * 8 + y, ((z + y) % 8) * 8 + y) for z in range(8) for y in range(8)]
NT = (((1,), (1,)), ((), ()))
TN = (((0,), (0,)), ((), ()))
VMEM = pl.BlockSpec(memory_space=pltpu.VMEM)
SMEM = pl.BlockSpec(memory_space=pltpu.SMEM)
PARAMS = pltpu.CompilerParams(vmem_limit_bytes=56 * 1024 * 1024)


def copies_from(shard, axis):
    copies = jnp.broadcast_to(shard, (lax.axis_size(axis), *shard.shape))
    return lax.all_to_all(copies, axis, split_axis=0, concat_axis=0, tiled=True)


def swapped_cores(value):
    return lax.ppermute(value, "c", [(0, 1), (1, 0)])


def three_parts(values):
    high = lax.reduce_precision(values, 8, 7)
    rest = values - high
    middle = lax.reduce_precision(rest, 8, 7)
    low = lax.reduce_precision(rest - middle, 8, 7)
    return [part.astype(BF16) for part in (high, middle, low)]


def project_kernel(rows, weights, own_out, oth_out, product):
    step = pl.program_id(0)
    part = jnp.dot(rows[...], weights[...], preferred_element_type=F32)

    @pl.when(step == 0)
    def _():
        product[...] = part

    @pl.when(step > 0)
    def _():
        product[...] += part

    @pl.when(step == pl.num_programs(0) - 1)
    def _():
        own_out[...] = product[:SPAN]
        oth_out[...] = product[SPAN:].astype(BF16)


def turned(proj, at, cos, sin):
    first = proj[:, at : at + 32]
    second = proj[:, at + 32 : at + 64]
    return jnp.concatenate([first * cos - second * sin, first * sin + second * cos], axis=1)


def front_kernel(first_part, second_part, cosine, sine, decay, q_out, kv_out, proj_out):
    proj_out[...] = first_part[...] + second_part[...].astype(F32)
    cos = cosine[...]
    sin = sine[...]
    for h in range(3):
        key = turned(proj_out, 192 + h * HEAD, cos, sin).astype(BF16)
        value = proj_out[:, 384 + h * HEAD : 384 + (h + 1) * HEAD].astype(BF16)
        column = decay[:, h : h + 1]
        last = decay[SPAN - 1 : SPAN, h : h + 1]
        faded = (key.astype(F32) * jnp.exp(last - column)).astype(BF16)
        update = lax.dot_general(faded, value, TN, preferred_element_type=F32).astype(BF16)
        kv_out[SPAN + 32 * h : SPAN + 32 * (h + 1)] = jnp.concatenate(
            [update[:32], update[32:]], axis=1
        )
    q_out[192:] = jnp.zeros((HEAD, SPAN), BF16)
    q_out[:192] = jnp.transpose(proj_out[:, 576:768] * (HEAD ** (-0.5) * LOG2E)).astype(BF16)
    both = proj_out[:, 768:896]
    flipped = jnp.transpose(both)[HEAD:, :].astype(BF16)
    kv_out[:128] = jnp.concatenate([both[:128, :HEAD], both[128:, :HEAD]], axis=1).astype(BF16)
    kv_out[128:SPAN] = jnp.concatenate([flipped[:, :128], flipped[:, 128:]], axis=0)


def local_kernel(proj, cosine, sine, decay, decay_row, local_out, lifted_out):
    cos = cosine[...]
    sin = sine[...]
    place = lax.broadcasted_iota(jnp.int32, (SPAN, SPAN), 0)
    other = lax.broadcasted_iota(jnp.int32, (SPAN, SPAN), 1)
    causal = place >= other
    for h in range(3):
        query = (turned(proj, h * HEAD, cos, sin) * HEAD ** (-0.5)).astype(BF16)
        key = turned(proj, 192 + h * HEAD, cos, sin).astype(BF16)
        value = proj[:, 384 + h * HEAD : 384 + (h + 1) * HEAD].astype(BF16)
        column = decay[:, h : h + 1]
        scores = lax.dot_general(query, key, NT, preferred_element_type=F32)
        gap = jnp.where(causal, column - decay_row[h : h + 1, :], 0.0)
        weights = jnp.where(causal, scores * jnp.exp(gap), 0.0).astype(BF16)
        local_out[:, h * HEAD : (h + 1) * HEAD] = jnp.dot(
            weights, value, preferred_element_type=F32
        )
        lifted_out[:, h * HEAD : (h + 1) * HEAD] = (
            query.astype(F32) * jnp.exp(column)
        ).astype(BF16)


def prepare_kernel(side, fade, held, key_gate, keys, values, states):
    extra = lax.broadcasted_iota(jnp.int32, (16, SPAN), 0)
    ones = jnp.where(extra == 0, 1.0, 0.0).astype(BF16)
    for y in range(8):
        packed = held[y, :128]
        keys[y, :128, :HEAD] = packed[:, :HEAD]
        keys[y, 128:, :HEAD] = packed[:, HEAD:]
        keys[y, :, HEAD:] = key_gate[side, y]
        values[y, :HEAD, :128] = held[y, 128:192]
        values[y, :HEAD, 128:] = held[y, 192:SPAN]
        values[y, HEAD:, :] = ones
    for z in range(8):
        for h in range(3):
            at = SPAN + 32 * h
            state = jnp.zeros((32, 128), F32)
            for y in range(8):
                state = state + held[y, at : at + 32].astype(F32) * fade[
                    ((z * 2 + side) * 8 + y) * 3 + h
                ]
            states[z, 32 * h : 32 * (h + 1)] = state


def attend_kernel(
    plan,
    received,
    query_gate,
    keys_own,
    keys_oth,
    values_own,
    values_oth,
    states_own,
    states_oth,
    out,
    queries,
    total,
    even,
    odd,
):
    for z in range(8):
        for h in range(3):
            queries[z, h, :HEAD] = received[z, h * HEAD : (h + 1) * HEAD]
            queries[z, h, HEAD:] = query_gate[z, h]
    total[...] = jnp.zeros_like(total)

    place = lax.broadcasted_iota(jnp.int32, (2 * SPAN, SPAN), 0)
    wanted = lax.broadcasted_iota(jnp.int32, (2 * SPAN, SPAN), 1)
    allowed = place <= jnp.where(place < SPAN, wanted, plan[66] * (4 * SPAN) - 1)

    def weigh(i, held, h):
        z, y = (plan[i] // 8, plan[i] % 8)
        at = h * SPAN
        total[z, :, at : at + SPAN] += jnp.dot(
            values_own[y], held[:SPAN, at : at + SPAN], preferred_element_type=F32
        ) + jnp.dot(values_oth[y], held[SPAN:, at : at + SPAN], preferred_element_type=F32)

    def score(i, held, h, mask=None):
        z, y = (plan[i] // 8, plan[i] % 8)
        for at, keys in ((0, keys_own), (SPAN, keys_oth)):
            weights = jnp.exp2(jnp.dot(keys[y], queries[z, h], preferred_element_type=F32))
            if mask is not None:
                weights = jnp.where(mask[at : at + SPAN], weights, 0.0)
            held[at : at + SPAN, h * SPAN : (h + 1) * SPAN] = weights.astype(BF16)

    for h in range(3):
        score(0, even, h, allowed)

    def pair(i, carry):
        for h in range(3):
            score(2 * i + 1, odd, h)
            weigh(2 * i, even, h)
        for h in range(3):
            score(2 * i + 2, even, h)
            weigh(2 * i + 1, odd, h)
        return carry

    count = plan[65]
    lax.fori_loop(0, count // 2, pair, 0)

    @pl.when(count % 2 == 1)
    def _():
        for h in range(3):
            weigh(count - 1, even, h)

    for z in range(8):
        rows = []
        for h in range(3):
            out[z, h * HEAD : (h + 1) * HEAD] = total[z, :HEAD, h * SPAN : (h + 1) * SPAN].astype(
                BF16
            )
            rows.append(total[z, HEAD : HEAD + 1, h * SPAN : (h + 1) * SPAN])
        high = [row.astype(BF16).astype(F32) for row in rows]
        low = [row - big for row, big in zip(rows, high)]
        out[z, 192:208] = jnp.concatenate(
            high + low + [jnp.zeros((10, SPAN), F32)], axis=0
        ).astype(BF16)
        sums = (states_own[z] + states_oth[z]).astype(BF16)
        out[z, 208:, :128] = sums[:48]
        out[z, 208:, 128:] = sums[48:]


def back_kernel(parts, local, lifted, w_out, out, mixed):
    total = parts[0].astype(F32)
    for z in range(1, 8):
        total = total + parts[z].astype(F32)
    states = jnp.concatenate([total[208:, :128], total[208:, 128:]], axis=0)
    for h in range(3):
        held = states[32 * h : 32 * (h + 1)]
        held = jnp.concatenate([held[:, :HEAD], held[:, HEAD:]], axis=0).astype(BF16)
        raw = local[:, h * HEAD : (h + 1) * HEAD] + jnp.dot(
            lifted[:, h * HEAD : (h + 1) * HEAD], held, preferred_element_type=F32
        )
        centred = raw - jnp.mean(raw, axis=-1, keepdims=True)
        spread = jnp.mean(centred * centred, axis=-1, keepdims=True)
        mixed[:, h * HEAD : (h + 1) * HEAD] = (centred * lax.rsqrt(spread + EPS)).astype(BF16)
        weight = total[192 + h : 193 + h] + total[195 + h : 196 + h]
        attended = total[h * HEAD : (h + 1) * HEAD] / weight
        mixed[:, 192 + h * HEAD : 192 + (h + 1) * HEAD] = jnp.transpose(attended).astype(BF16)
    out[...] = lax.dot_general(
        mixed[...], w_out[...], NT, preferred_element_type=F32
    ).astype(BF16)


def body(
    tokens,
    pre_gain,
    w_query_ret,
    w_key_ret,
    w_value_ret,
    w_query_att,
    w_key_att,
    w_value_att,
    w_out_ret,
    w_out_att,
    retain_log,
    forget_total,
):
    z, y, c = (lax.axis_index("z"), lax.axis_index("y"), lax.axis_index("c"))
    ends = jnp.concatenate(three_parts(jnp.sum(retain_log, axis=0)))
    shard = jnp.concatenate(
        [
            w_query_ret,
            w_key_ret,
            w_value_ret,
            w_query_att,
            w_key_att,
            w_value_att,
            w_out_ret.T,
            w_out_att.T,
            jnp.pad(ends[None, :], ((0, 15), (0, 119))),
        ],
        axis=1,
    )
    w_row = copies_from(shard, "y").reshape(128, 1408)
    w_own = lax.all_gather(w_row, "z", axis=0, tiled=True)

    raw = tokens.astype(F32)
    normed = (
        raw * lax.rsqrt(jnp.mean(raw * raw, axis=-1, keepdims=True) + EPS) * pre_gain
    ).astype(BF16)
    halves = jnp.transpose(normed.reshape(64, 64, 2, 16), (2, 0, 1, 3)).reshape(2, 64, 1024)
    rows = copies_from(halves, "tp")
    kept = jnp.where(c == 0, rows[:, 0], rows[:, 1]).reshape(SPAN, 1024)
    sent = jnp.where(c == 0, rows[:, 1], rows[:, 0]).reshape(SPAN, 1024)
    came = swapped_cores(sent)
    rows = jnp.concatenate([kept, came], axis=0)

    here = z * 16 + y * 2 + c
    positions = (here * SPAN + jnp.arange(SPAN, dtype=jnp.int32)).astype(F32)
    inverse = THETA ** (-jnp.arange(32, dtype=F32) / 32)
    angles = positions[:, None] * inverse[None, :]
    cosine, sine = (jnp.cos(angles), jnp.sin(angles))
    decay = jnp.cumsum(retain_log, axis=0)
    decay_row = jnp.pad(decay.T, ((0, 5), (0, 0)))
    gate = (forget_total * LOG2E).reshape(3, 8, 8, 2, SPAN)
    spans = jnp.arange(8, dtype=jnp.int32)
    key_z = (z - spans) % 8
    chosen = (spans[:, None] == key_z[None, :])[None, :, :, None, None]
    key_side = jnp.sum(jnp.where(chosen, gate, 0.0), axis=1)
    key_side = jnp.where(c == 0, key_side, key_side[:, :, ::-1])
    minus = jnp.stack(three_parts(-key_side), axis=1).reshape(9, 8, 2, SPAN)
    key_gate = jnp.concatenate(
        [minus, jnp.ones((3, 8, 2, SPAN), BF16), jnp.zeros((52, 8, 2, SPAN), BF16)], axis=0
    )
    key_gate = jnp.transpose(key_gate, (2, 1, 3, 0))
    mine = lax.dynamic_index_in_dim(
        lax.dynamic_index_in_dim(gate, y, 2, keepdims=False), c, 2, keepdims=False
    )
    plus = jnp.transpose(jnp.stack(three_parts(mine), axis=0), (2, 1, 0, 3))
    own_head = (
        jnp.arange(9, dtype=jnp.int32)[None, :] // 3 == jnp.arange(3, dtype=jnp.int32)[:, None]
    ).astype(BF16)
    query_gate = jnp.concatenate(
        [
            jnp.broadcast_to(own_head[None, :, :, None], (8, 3, 9, SPAN)),
            plus,
            jnp.zeros((8, 3, 52, SPAN), BF16),
        ],
        axis=2,
    )
    needed = (
        (key_z[None, :] < spans[:, None])
        | ((key_z[None, :] == spans[:, None]) & (spans[None, :] < y))
    ).reshape(64)
    slot = jnp.cumsum(needed.astype(jnp.int32)) - 1
    order = jnp.arange(64, dtype=jnp.int32)
    units = jnp.sum(
        jnp.where(needed[None, :] & (slot[None, :] == order[:, None]), order[None, :], 0), axis=1
    )
    own = jnp.stack([(z - y) % 8 * 8 + y])
    plan = jnp.concatenate([own, units, jnp.stack([jnp.sum(needed.astype(jnp.int32)) + 1, c])])

    own_part, oth_part = pl.pallas_call(
        project_kernel,
        grid=(2,),
        in_specs=[
            pl.BlockSpec((2 * SPAN, 512), lambda i: (0, i)),
            pl.BlockSpec((512, 896), lambda i: (i, 0)),
        ],
        out_specs=[pl.BlockSpec((SPAN, 896), lambda i: (0, 0))] * 2,
        out_shape=[
            jax.ShapeDtypeStruct((SPAN, 896), F32),
            jax.ShapeDtypeStruct((SPAN, 896), BF16),
        ],
        scratch_shapes=[pltpu.VMEM((2 * SPAN, 896), F32)],
        compiler_params=PARAMS,
        name="project",
    )(rows, w_own)
    q_send, kv_send, proj = pl.pallas_call(
        front_kernel,
        in_specs=[VMEM] * 5,
        out_specs=[VMEM] * 3,
        out_shape=[
            jax.ShapeDtypeStruct((SPAN, SPAN), BF16),
            jax.ShapeDtypeStruct((SPAN + 96, 128), BF16),
            jax.ShapeDtypeStruct((SPAN, 896), F32),
        ],
        compiler_params=PARAMS,
        name="front",
    )(own_part, swapped_cores(oth_part), cosine, sine, decay)

    queries = lax.all_gather(q_send, "z", axis=0)
    kv_send = lax.ppermute(kv_send, ("z", "y"), ROTATION)
    kv_own = copies_from(kv_send, "y")
    kv_oth = swapped_cores(kv_own)
    ends_own = w_own[:, 1280:1289].reshape(8, 8, 16, 9)[:, :, 0].astype(F32)
    ends_own = jnp.sum(ends_own.reshape(8, 8, 3, 3), axis=2)
    ends_oth = swapped_cores(ends_own)
    ends = jnp.where(
        c == 0,
        jnp.stack([ends_own, ends_oth], axis=2),
        jnp.stack([ends_oth, ends_own], axis=2),
    ).reshape(128, 3)
    blocks = key_z * 16 + spans * 2
    blocks = jnp.stack([blocks + c, blocks + 1 - c])
    targets = spans * 16 + y * 2 + c
    index = jnp.arange(128, dtype=jnp.int32)
    between = (index > blocks[None, :, :, None]) & (index < targets[:, None, None, None])
    fade = jnp.sum(jnp.where(between[..., None], ends, 0.0), axis=3)
    earlier = blocks[None] < targets[:, None, None]
    fade = jnp.where(earlier[..., None], jnp.exp(fade), 0.0).reshape(384)
    local, lifted = pl.pallas_call(
        local_kernel,
        in_specs=[VMEM] * 5,
        out_specs=[VMEM] * 2,
        out_shape=[jax.ShapeDtypeStruct((SPAN, 192), F32), jax.ShapeDtypeStruct((SPAN, 192), BF16)],
        compiler_params=PARAMS,
        name="local",
    )(proj, cosine, sine, decay, decay_row)
    out_own = w_own[:, 896:1280]
    out_oth = swapped_cores(out_own).reshape(64, 16, 384)
    out_own = out_own.reshape(64, 16, 384)
    w_out = jnp.where(
        c == 0, jnp.stack([out_own, out_oth], axis=1), jnp.stack([out_oth, out_own], axis=1)
    ).reshape(2048, 384)

    def prepared(side, held):
        return pl.pallas_call(
            functools.partial(prepare_kernel, side),
            in_specs=[SMEM] + [VMEM] * 2,
            out_specs=[VMEM] * 3,
            out_shape=[
                jax.ShapeDtypeStruct((8, SPAN, 128), BF16),
                jax.ShapeDtypeStruct((8, 80, SPAN), BF16),
                jax.ShapeDtypeStruct((8, 96, 128), F32),
            ],
            compiler_params=PARAMS,
            name="prepare",
        )(fade, held, key_gate)

    keys_own, values_own, states_own = prepared(0, kv_own)
    keys_oth, values_oth, states_oth = prepared(1, kv_oth)
    partial = pl.pallas_call(
        attend_kernel,
        in_specs=[SMEM] + [VMEM] * 8,
        out_specs=VMEM,
        out_shape=jax.ShapeDtypeStruct((8, SPAN, SPAN), BF16),
        scratch_shapes=[
            pltpu.VMEM((8, 3, 128, SPAN), BF16),
            pltpu.VMEM((8, 80, 3 * SPAN), F32),
            pltpu.VMEM((2 * SPAN, 3 * SPAN), BF16),
            pltpu.VMEM((2 * SPAN, 3 * SPAN), BF16),
        ],
        compiler_params=PARAMS,
        name="attend",
    )(
        plan,
        queries,
        query_gate,
        keys_own,
        keys_oth,
        values_own,
        values_oth,
        states_own,
        states_oth,
    )
    parts = lax.all_to_all(partial, "z", 0, 0, tiled=True)

    share = pl.pallas_call(
        back_kernel,
        in_specs=[VMEM] * 4,
        out_specs=VMEM,
        out_shape=jax.ShapeDtypeStruct((SPAN, 2048), BF16),
        scratch_shapes=[pltpu.VMEM((SPAN, 384), BF16)],
        compiler_params=PARAMS,
        name="back",
    )(parts, local, lifted, w_out)
    shares = lax.all_to_all(share.reshape(4, 64, 2048), "tp", 0, 0, tiled=True)
    return jnp.sum(shares.astype(F32), axis=0).astype(BF16)


def solution(mesh):
    finer = Mesh(mesh.devices.reshape(8, 8, 2, mesh.shape["tp"]), ("z", "y", "c", "tp"))
    everyone = ("z", "y", "c", "tp")
    placed = (
        P(everyone, None),
        P(),
        P(SP, "tp"),
        P(SP, "tp"),
        P(SP, "tp"),
        P(SP, "tp"),
        P(SP, "tp"),
        P(SP, "tp"),
        P("tp", SP),
        P("tp", SP),
        P(SP, "tp"),
        P("tp", None),
    )
    return jax.shard_map(
        body, mesh=finer, in_specs=placed, out_specs=P(everyone, None), check_vma=False
    )
```

```python
import functools

import jax
import jax.numpy as jnp
from jax import lax
from jax.experimental import pallas as pl
from jax.experimental.pallas import tpu as pltpu
from jax.sharding import Mesh
from jax.sharding import PartitionSpec as P

HEAD = 64
SPAN = 256
SP = ("z", "y", "c")
EPS = 1e-06
THETA = 10000.0
LOG2E = 1.4426950408889634
F32 = jnp.float32
BF16 = jnp.bfloat16
ROTATION = [(z * 8 + y, ((z + y) % 8) * 8 + y) for z in range(8) for y in range(8)]
NT = (((1,), (1,)), ((), ()))
TN = (((0,), (0,)), ((), ()))
VMEM = pl.BlockSpec(memory_space=pltpu.VMEM)
SMEM = pl.BlockSpec(memory_space=pltpu.SMEM)
PARAMS = pltpu.CompilerParams(vmem_limit_bytes=56 * 1024 * 1024)


def copies_from(shard, axis):
    copies = jnp.broadcast_to(shard, (lax.axis_size(axis), *shard.shape))
    return lax.all_to_all(copies, axis, split_axis=0, concat_axis=0, tiled=True)


def swapped_cores(value):
    return lax.ppermute(value, "c", [(0, 1), (1, 0)])


def three_parts(values):
    high = lax.reduce_precision(values, 8, 7)
    rest = values - high
    middle = lax.reduce_precision(rest, 8, 7)
    low = lax.reduce_precision(rest - middle, 8, 7)
    return [part.astype(BF16) for part in (high, middle, low)]


def project_kernel(rows, weights, own_out, oth_out):
    product = jnp.dot(rows[...], weights[...], preferred_element_type=F32)
    own_out[...] = product[:SPAN]
    oth_out[...] = product[SPAN:]


def share_kernel(first_part, second_part, q_out, kv_out):
    query = first_part[:, :192] + second_part[:, :192]
    q_out[192:] = jnp.zeros((HEAD, SPAN), BF16)
    q_out[:192] = jnp.transpose(query * (HEAD ** (-0.5) * LOG2E)).astype(BF16)
    both = first_part[:, 192:320] + second_part[:, 192:320]
    flipped = jnp.transpose(both)[HEAD:, :].astype(BF16)
    kv_out[:128] = jnp.concatenate([both[:128, :HEAD], both[128:, :HEAD]], axis=1).astype(BF16)
    kv_out[128:] = jnp.concatenate([flipped[:, :128], flipped[:, 128:]], axis=0)


def turned(proj, at, cos, sin):
    first = proj[:, at : at + 32]
    second = proj[:, at + 32 : at + 64]
    return jnp.concatenate([first * cos - second * sin, first * sin + second * cos], axis=1)


def front_kernel(first_part, second_part, cosine, sine, decay, state_out, proj_out):
    proj_out[...] = first_part[...] + second_part[...]
    cos = cosine[...]
    sin = sine[...]
    for h in range(3):
        key = turned(proj_out, 512 + h * HEAD, cos, sin).astype(BF16)
        value = proj_out[:, 704 + h * HEAD : 704 + (h + 1) * HEAD].astype(BF16)
        column = decay[:, h : h + 1]
        last = decay[SPAN - 1 : SPAN, h : h + 1]
        faded = (key.astype(F32) * jnp.exp(last - column)).astype(BF16)
        update = lax.dot_general(faded, value, TN, preferred_element_type=F32).astype(BF16)
        state_out[32 * h : 32 * (h + 1)] = jnp.concatenate([update[:32], update[32:]], axis=1)


def local_kernel(proj, cosine, sine, decay, decay_row, local_out, lifted_out):
    cos = cosine[...]
    sin = sine[...]
    place = lax.broadcasted_iota(jnp.int32, (SPAN, SPAN), 0)
    other = lax.broadcasted_iota(jnp.int32, (SPAN, SPAN), 1)
    causal = place >= other
    for h in range(3):
        query = (turned(proj, 320 + h * HEAD, cos, sin) * HEAD ** (-0.5)).astype(BF16)
        key = turned(proj, 512 + h * HEAD, cos, sin).astype(BF16)
        value = proj[:, 704 + h * HEAD : 704 + (h + 1) * HEAD].astype(BF16)
        column = decay[:, h : h + 1]
        scores = lax.dot_general(query, key, NT, preferred_element_type=F32)
        gap = jnp.where(causal, column - decay_row[h : h + 1, :], 0.0)
        weights = jnp.where(causal, scores * jnp.exp(gap), 0.0).astype(BF16)
        local_out[:, h * HEAD : (h + 1) * HEAD] = jnp.dot(
            weights, value, preferred_element_type=F32
        )
        lifted_out[:, h * HEAD : (h + 1) * HEAD] = (
            query.astype(F32) * jnp.exp(column)
        ).astype(BF16)


def prepare_kernel(side, fade, held, key_gate, keys, values, states):
    extra = lax.broadcasted_iota(jnp.int32, (16, SPAN), 0)
    ones = jnp.where(extra == 0, 1.0, 0.0).astype(BF16)
    for y in range(8):
        packed = held[y, :128]
        keys[y, :128, :HEAD] = packed[:, :HEAD]
        keys[y, 128:, :HEAD] = packed[:, HEAD:]
        keys[y, :, HEAD:] = key_gate[side, y]
        values[y, :HEAD, :128] = held[y, 128:192]
        values[y, :HEAD, 128:] = held[y, 192:SPAN]
        values[y, HEAD:, :] = ones
    for z in range(8):
        for h in range(3):
            at = SPAN + 32 * h
            state = jnp.zeros((32, 128), F32)
            for y in range(8):
                state = state + held[y, at : at + 32].astype(F32) * fade[
                    ((z * 2 + side) * 8 + y) * 3 + h
                ]
            states[z, 32 * h : 32 * (h + 1)] = state


def attend_kernel(
    plan,
    received,
    query_gate,
    keys_own,
    keys_oth,
    values_own,
    values_oth,
    states_own,
    states_oth,
    out,
    queries,
    total,
    even,
    odd,
):
    for z in range(8):
        for h in range(3):
            queries[z, h, :HEAD] = received[z, h * HEAD : (h + 1) * HEAD]
            queries[z, h, HEAD:] = query_gate[z, h]
    total[...] = jnp.zeros_like(total)

    place = lax.broadcasted_iota(jnp.int32, (2 * SPAN, SPAN), 0)
    wanted = lax.broadcasted_iota(jnp.int32, (2 * SPAN, SPAN), 1)
    allowed = place <= jnp.where(place < SPAN, wanted, plan[66] * (4 * SPAN) - 1)

    def weigh(i, held, h):
        z, y = (plan[i] // 8, plan[i] % 8)
        at = h * SPAN
        total[z, :, at : at + SPAN] += jnp.dot(
            values_own[y], held[:SPAN, at : at + SPAN], preferred_element_type=F32
        ) + jnp.dot(values_oth[y], held[SPAN:, at : at + SPAN], preferred_element_type=F32)

    def score(i, held, h, mask=None):
        z, y = (plan[i] // 8, plan[i] % 8)
        for at, keys in ((0, keys_own), (SPAN, keys_oth)):
            weights = jnp.exp2(jnp.dot(keys[y], queries[z, h], preferred_element_type=F32))
            if mask is not None:
                weights = jnp.where(mask[at : at + SPAN], weights, 0.0)
            held[at : at + SPAN, h * SPAN : (h + 1) * SPAN] = weights.astype(BF16)

    for h in range(3):
        score(0, even, h, allowed)

    def pair(i, carry):
        for h in range(3):
            score(2 * i + 1, odd, h)
            weigh(2 * i, even, h)
        for h in range(3):
            score(2 * i + 2, even, h)
            weigh(2 * i + 1, odd, h)
        return carry

    count = plan[65]
    lax.fori_loop(0, count // 2, pair, 0)

    @pl.when(count % 2 == 1)
    def _():
        for h in range(3):
            weigh(count - 1, even, h)

    for z in range(8):
        rows = []
        for h in range(3):
            out[z, h * HEAD : (h + 1) * HEAD] = total[z, :HEAD, h * SPAN : (h + 1) * SPAN].astype(
                BF16
            )
            rows.append(total[z, HEAD : HEAD + 1, h * SPAN : (h + 1) * SPAN])
        high = [row.astype(BF16).astype(F32) for row in rows]
        low = [row - big for row, big in zip(rows, high)]
        out[z, 192:208] = jnp.concatenate(
            high + low + [jnp.zeros((10, SPAN), F32)], axis=0
        ).astype(BF16)
        sums = (states_own[z] + states_oth[z]).astype(BF16)
        out[z, 208:, :128] = sums[:48]
        out[z, 208:, 128:] = sums[48:]


def back_kernel(parts, local, lifted, w_out, out, mixed):
    total = parts[0].astype(F32)
    for z in range(1, 8):
        total = total + parts[z].astype(F32)
    states = jnp.concatenate([total[208:, :128], total[208:, 128:]], axis=0)
    for h in range(3):
        held = states[32 * h : 32 * (h + 1)]
        held = jnp.concatenate([held[:, :HEAD], held[:, HEAD:]], axis=0).astype(BF16)
        raw = local[:, h * HEAD : (h + 1) * HEAD] + jnp.dot(
            lifted[:, h * HEAD : (h + 1) * HEAD], held, preferred_element_type=F32
        )
        centred = raw - jnp.mean(raw, axis=-1, keepdims=True)
        spread = jnp.mean(centred * centred, axis=-1, keepdims=True)
        mixed[:, h * HEAD : (h + 1) * HEAD] = (centred * lax.rsqrt(spread + EPS)).astype(BF16)
        weight = total[192 + h : 193 + h] + total[195 + h : 196 + h]
        attended = total[h * HEAD : (h + 1) * HEAD] / weight
        mixed[:, 192 + h * HEAD : 192 + (h + 1) * HEAD] = jnp.transpose(attended).astype(BF16)
    out[...] = lax.dot_general(
        mixed[...], w_out[...], NT, preferred_element_type=F32
    ).astype(BF16)


def body(
    tokens,
    pre_gain,
    w_query_ret,
    w_key_ret,
    w_value_ret,
    w_query_att,
    w_key_att,
    w_value_att,
    w_out_ret,
    w_out_att,
    retain_log,
    forget_total,
):
    z, y, c = (lax.axis_index("z"), lax.axis_index("y"), lax.axis_index("c"))
    ends = jnp.concatenate(three_parts(jnp.sum(retain_log, axis=0)))
    shard = jnp.concatenate(
        [
            w_query_att,
            w_key_att,
            w_value_att,
            w_query_ret,
            w_key_ret,
            w_value_ret,
            w_out_ret.T,
            w_out_att.T,
            jnp.pad(ends[None, :], ((0, 15), (0, 119))),
        ],
        axis=1,
    )
    w_row = copies_from(shard, "y")
    line_ends = jnp.sum(w_row[:, 0, 1280:1289].reshape(8, 3, 3).astype(F32), axis=1)
    w_row = w_row[:, :, :1280].reshape(128, 1280)
    w_own = lax.all_gather(w_row, "z", axis=0, tiled=True)

    raw = tokens.astype(F32)
    normed = (
        raw * lax.rsqrt(jnp.mean(raw * raw, axis=-1, keepdims=True) + EPS) * pre_gain
    ).astype(BF16)
    halves = jnp.transpose(normed.reshape(64, 64, 2, 16), (2, 0, 1, 3)).reshape(2, 64, 1024)
    rows = copies_from(halves, "tp")
    kept = jnp.where(c == 0, rows[:, 0], rows[:, 1]).reshape(SPAN, 1024)
    sent = jnp.where(c == 0, rows[:, 1], rows[:, 0]).reshape(SPAN, 1024)
    came = swapped_cores(sent)
    rows = jnp.concatenate([kept, came], axis=0)

    here = z * 16 + y * 2 + c
    positions = (here * SPAN + jnp.arange(SPAN, dtype=jnp.int32)).astype(F32)
    inverse = THETA ** (-jnp.arange(32, dtype=F32) / 32)
    angles = positions[:, None] * inverse[None, :]
    cosine, sine = (jnp.cos(angles), jnp.sin(angles))
    decay = jnp.cumsum(retain_log, axis=0)
    decay_row = jnp.pad(decay.T, ((0, 5), (0, 0)))
    ends_own = copies_from(line_ends, "z")
    ends_oth = swapped_cores(ends_own)
    ends = jnp.where(
        c == 0,
        jnp.stack([ends_own, ends_oth], axis=2),
        jnp.stack([ends_oth, ends_own], axis=2),
    ).reshape(128, 3)

    gate = (forget_total * LOG2E).reshape(3, 8, 8, 2, SPAN)
    spans = jnp.arange(8, dtype=jnp.int32)
    key_z = (z - spans) % 8
    chosen = (spans[:, None] == key_z[None, :])[None, :, :, None, None]
    key_side = jnp.sum(jnp.where(chosen, gate, 0.0), axis=1)
    key_side = jnp.where(c == 0, key_side, key_side[:, :, ::-1])
    minus = jnp.stack(three_parts(-key_side), axis=1).reshape(9, 8, 2, SPAN)
    key_gate = jnp.concatenate(
        [minus, jnp.ones((3, 8, 2, SPAN), BF16), jnp.zeros((52, 8, 2, SPAN), BF16)], axis=0
    )
    key_gate = jnp.transpose(key_gate, (2, 1, 3, 0))
    mine = lax.dynamic_index_in_dim(
        lax.dynamic_index_in_dim(gate, y, 2, keepdims=False), c, 2, keepdims=False
    )
    plus = jnp.transpose(jnp.stack(three_parts(mine), axis=0), (2, 1, 0, 3))
    own_head = (
        jnp.arange(9, dtype=jnp.int32)[None, :] // 3 == jnp.arange(3, dtype=jnp.int32)[:, None]
    ).astype(BF16)
    query_gate = jnp.concatenate(
        [
            jnp.broadcast_to(own_head[None, :, :, None], (8, 3, 9, SPAN)),
            plus,
            jnp.zeros((8, 3, 52, SPAN), BF16),
        ],
        axis=2,
    )
    blocks = z * 16 + spans * 2
    blocks = jnp.stack([blocks + c, blocks + 1 - c])
    targets = spans * 16 + y * 2 + c
    index = jnp.arange(128, dtype=jnp.int32)
    between = (index > blocks[None, :, :, None]) & (index < targets[:, None, None, None])
    fade = jnp.sum(jnp.where(between[..., None], ends, 0.0), axis=3)
    earlier = blocks[None] < targets[:, None, None]
    fade = jnp.where(earlier[..., None], jnp.exp(fade), 0.0).reshape(384)
    needed = (
        (key_z[None, :] < spans[:, None])
        | ((key_z[None, :] == spans[:, None]) & (spans[None, :] < y))
    ).reshape(64)
    slot = jnp.cumsum(needed.astype(jnp.int32)) - 1
    order = jnp.arange(64, dtype=jnp.int32)
    units = jnp.sum(
        jnp.where(needed[None, :] & (slot[None, :] == order[:, None]), order[None, :], 0), axis=1
    )
    own = jnp.stack([(z - y) % 8 * 8 + y])
    plan = jnp.concatenate([own, units, jnp.stack([jnp.sum(needed.astype(jnp.int32)) + 1, c])])

    own_part, oth_part = pl.pallas_call(
        project_kernel,
        grid=(1,),
        in_specs=[VMEM, pl.BlockSpec((1024, 896), lambda i: (0, 0))],
        out_specs=[VMEM] * 2,
        out_shape=[jax.ShapeDtypeStruct((SPAN, 896), F32)] * 2,
        compiler_params=PARAMS,
        name="project",
    )(rows, w_own)
    came_part = swapped_cores(oth_part)
    attention_part = pl.BlockSpec((SPAN, 384), lambda i: (0, 0))
    q_send, kv_send = pl.pallas_call(
        share_kernel,
        grid=(1,),
        in_specs=[attention_part] * 2,
        out_specs=[VMEM] * 2,
        out_shape=[
            jax.ShapeDtypeStruct((SPAN, SPAN), BF16),
            jax.ShapeDtypeStruct((SPAN, 128), BF16),
        ],
        compiler_params=PARAMS,
        name="share",
    )(own_part, came_part)
    queries = lax.all_gather(q_send, "z", axis=0)
    kv_send = lax.ppermute(kv_send, ("z", "y"), ROTATION)
    state_send, proj = pl.pallas_call(
        front_kernel,
        in_specs=[VMEM] * 5,
        out_specs=[VMEM] * 2,
        out_shape=[jax.ShapeDtypeStruct((96, 128), BF16), jax.ShapeDtypeStruct((SPAN, 896), F32)],
        compiler_params=PARAMS,
        name="front",
    )(own_part, came_part, cosine, sine, decay)
    kv_send = jnp.concatenate([kv_send, state_send], axis=0)
    kv_own = copies_from(kv_send, "y")
    kv_oth = swapped_cores(kv_own)
    local, lifted = pl.pallas_call(
        local_kernel,
        in_specs=[VMEM] * 5,
        out_specs=[VMEM] * 2,
        out_shape=[jax.ShapeDtypeStruct((SPAN, 192), F32), jax.ShapeDtypeStruct((SPAN, 192), BF16)],
        compiler_params=PARAMS,
        name="local",
    )(proj, cosine, sine, decay, decay_row)
    out_own = w_own[:, 896:1280]
    out_oth = swapped_cores(out_own).reshape(64, 16, 384)
    out_own = out_own.reshape(64, 16, 384)
    w_out = jnp.where(
        c == 0, jnp.stack([out_own, out_oth], axis=1), jnp.stack([out_oth, out_own], axis=1)
    ).reshape(2048, 384)

    def prepared(side, held):
        return pl.pallas_call(
            functools.partial(prepare_kernel, side),
            in_specs=[SMEM] + [VMEM] * 2,
            out_specs=[VMEM] * 3,
            out_shape=[
                jax.ShapeDtypeStruct((8, SPAN, 128), BF16),
                jax.ShapeDtypeStruct((8, 80, SPAN), BF16),
                jax.ShapeDtypeStruct((8, 96, 128), F32),
            ],
            compiler_params=PARAMS,
            name="prepare",
        )(fade, held, key_gate)

    keys_own, values_own, states_own = prepared(0, kv_own)
    keys_oth, values_oth, states_oth = prepared(1, kv_oth)
    partial = pl.pallas_call(
        attend_kernel,
        in_specs=[SMEM] + [VMEM] * 8,
        out_specs=VMEM,
        out_shape=jax.ShapeDtypeStruct((8, SPAN, SPAN), BF16),
        scratch_shapes=[
            pltpu.VMEM((8, 3, 128, SPAN), BF16),
            pltpu.VMEM((8, 80, 3 * SPAN), F32),
            pltpu.VMEM((2 * SPAN, 3 * SPAN), BF16),
            pltpu.VMEM((2 * SPAN, 3 * SPAN), BF16),
        ],
        compiler_params=PARAMS,
        name="attend",
    )(
        plan,
        queries,
        query_gate,
        keys_own,
        keys_oth,
        values_own,
        values_oth,
        states_own,
        states_oth,
    )
    parts = lax.all_to_all(partial, "z", 0, 0, tiled=True)

    share = pl.pallas_call(
        back_kernel,
        in_specs=[VMEM] * 4,
        out_specs=VMEM,
        out_shape=jax.ShapeDtypeStruct((SPAN, 2048), BF16),
        scratch_shapes=[pltpu.VMEM((SPAN, 384), BF16)],
        compiler_params=PARAMS,
        name="back",
    )(parts, local, lifted, w_out)
    shares = lax.all_to_all(share.reshape(4, 64, 2048), "tp", 0, 0, tiled=True)
    return jnp.sum(shares.astype(F32), axis=0).astype(BF16)


def solution(mesh):
    finer = Mesh(mesh.devices.reshape(8, 8, 2, mesh.shape["tp"]), ("z", "y", "c", "tp"))
    everyone = ("z", "y", "c", "tp")
    placed = (
        P(everyone, None),
        P(),
        P(SP, "tp"),
        P(SP, "tp"),
        P(SP, "tp"),
        P(SP, "tp"),
        P(SP, "tp"),
        P(SP, "tp"),
        P("tp", SP),
        P("tp", SP),
        P(SP, "tp"),
        P("tp", None),
    )
    return jax.shard_map(
        body, mesh=finer, in_specs=placed, out_specs=P(everyone, None), check_vma=False
    )
```

```python
import jax
import jax.numpy as jnp
from jax import lax
from jax.experimental import pallas as pl
from jax.experimental.pallas import tpu as pltpu
from jax.sharding import Mesh
from jax.sharding import PartitionSpec as P

HEAD = 64
SPAN = 256
SP = ("z", "y", "c")
EPS = 1e-06
THETA = 10000.0
LOG2E = 1.4426950408889634
F32 = jnp.float32
BF16 = jnp.bfloat16
ROTATION = [(z * 8 + y, ((z + y) % 8) * 8 + y) for z in range(8) for y in range(8)]
NT = (((1,), (1,)), ((), ()))
TN = (((0,), (0,)), ((), ()))
VMEM = pl.BlockSpec(memory_space=pltpu.VMEM)
SMEM = pl.BlockSpec(memory_space=pltpu.SMEM)
PARAMS = pltpu.CompilerParams(vmem_limit_bytes=56 * 1024 * 1024)


def copies_from(shard, axis):
    copies = jnp.broadcast_to(shard, (lax.axis_size(axis), *shard.shape))
    return lax.all_to_all(copies, axis, split_axis=0, concat_axis=0, tiled=True)


def swapped_cores(value):
    return lax.ppermute(value, "c", [(0, 1), (1, 0)])


def three_parts(values):
    high = lax.reduce_precision(values, 8, 7)
    rest = values - high
    middle = lax.reduce_precision(rest, 8, 7)
    low = lax.reduce_precision(rest - middle, 8, 7)
    return [part.astype(BF16) for part in (high, middle, low)]


def project_kernel(rows, weights, own_out, oth_out):
    product = jnp.dot(rows[...], weights[...], preferred_element_type=F32)
    own_out[...] = product[:SPAN]
    oth_out[...] = product[SPAN:]


def share_kernel(first_part, second_part, q_out, kv_out):
    query = first_part[:, :192] + second_part[:, :192]
    q_out[192:] = jnp.zeros((HEAD, SPAN), BF16)
    q_out[:192] = jnp.transpose(query * (HEAD ** (-0.5) * LOG2E)).astype(BF16)
    both = first_part[:, 192:320] + second_part[:, 192:320]
    flipped = jnp.transpose(both)[HEAD:, :].astype(BF16)
    kv_out[:128] = jnp.concatenate([both[:128, :HEAD], both[128:, :HEAD]], axis=1).astype(BF16)
    kv_out[128:] = jnp.concatenate([flipped[:, :128], flipped[:, 128:]], axis=0)


def turned(proj, at, cos, sin):
    first = proj[:, at : at + 32]
    second = proj[:, at + 32 : at + 64]
    return jnp.concatenate([first * cos - second * sin, first * sin + second * cos], axis=1)


def front_kernel(first_part, second_part, cosine, sine, decay, state_out, proj_out):
    proj_out[...] = first_part[...] + second_part[...]
    cos = cosine[...]
    sin = sine[...]
    for h in range(3):
        key = turned(proj_out, 512 + h * HEAD, cos, sin).astype(BF16)
        value = proj_out[:, 704 + h * HEAD : 704 + (h + 1) * HEAD].astype(BF16)
        column = decay[:, h : h + 1]
        last = decay[SPAN - 1 : SPAN, h : h + 1]
        faded = (key.astype(F32) * jnp.exp(last - column)).astype(BF16)
        update = lax.dot_general(faded, value, TN, preferred_element_type=F32).astype(BF16)
        state_out[32 * h : 32 * (h + 1)] = jnp.concatenate([update[:32], update[32:]], axis=1)


def local_kernel(proj, cosine, sine, decay, decay_row, local_out, lifted_out):
    cos = cosine[...]
    sin = sine[...]
    place = lax.broadcasted_iota(jnp.int32, (SPAN, SPAN), 0)
    other = lax.broadcasted_iota(jnp.int32, (SPAN, SPAN), 1)
    causal = place >= other
    for h in range(3):
        query = (turned(proj, 320 + h * HEAD, cos, sin) * HEAD ** (-0.5)).astype(BF16)
        key = turned(proj, 512 + h * HEAD, cos, sin).astype(BF16)
        value = proj[:, 704 + h * HEAD : 704 + (h + 1) * HEAD].astype(BF16)
        column = decay[:, h : h + 1]
        scores = lax.dot_general(query, key, NT, preferred_element_type=F32)
        gap = jnp.where(causal, column - decay_row[h : h + 1, :], 0.0)
        weights = jnp.where(causal, scores * jnp.exp(gap), 0.0).astype(BF16)
        local_out[:, h * HEAD : (h + 1) * HEAD] = jnp.dot(
            weights, value, preferred_element_type=F32
        )
        lifted_out[:, h * HEAD : (h + 1) * HEAD] = (
            query.astype(F32) * jnp.exp(column)
        ).astype(BF16)


def attend_kernel(
    plan,
    fade,
    received,
    query_gate,
    kv_own,
    kv_oth,
    key_gate,
    out,
    keys,
    values,
    queries,
    total,
    even,
    odd,
):
    extra = lax.broadcasted_iota(jnp.int32, (16, 2 * SPAN), 0)
    ones = jnp.where(extra == 0, 1.0, 0.0).astype(BF16)
    for y in range(8):
        for side, held in enumerate((kv_own, kv_oth)):
            packed = held[y, :128]
            at = side * SPAN
            keys[y, at : at + 128, :HEAD] = packed[:, :HEAD]
            keys[y, at + 128 : at + SPAN, :HEAD] = packed[:, HEAD:]
            keys[y, at : at + SPAN, HEAD:] = key_gate[side, y]
            values[y, :HEAD, at : at + 128] = held[y, 128:192]
            values[y, :HEAD, at + 128 : at + SPAN] = held[y, 192:SPAN]
        values[y, HEAD:, :] = ones
    for z in range(8):
        for h in range(3):
            queries[z, h, :HEAD] = received[z, h * HEAD : (h + 1) * HEAD]
            queries[z, h, HEAD:] = query_gate[z, h]
    total[...] = jnp.zeros_like(total)

    place = lax.broadcasted_iota(jnp.int32, (2 * SPAN, SPAN), 0)
    wanted = lax.broadcasted_iota(jnp.int32, (2 * SPAN, SPAN), 1)
    allowed = place <= jnp.where(place < SPAN, wanted, plan[66] * (4 * SPAN) - 1)

    def weigh(i, held, h):
        z, y = (plan[i] // 8, plan[i] % 8)
        at = h * SPAN
        total[z, :, at : at + SPAN] += jnp.dot(
            values[y], held[:, at : at + SPAN], preferred_element_type=F32
        )

    def score(i, held, h, mask=None):
        z, y = (plan[i] // 8, plan[i] % 8)
        for at in (0, SPAN):
            weights = jnp.exp2(
                jnp.dot(keys[y, at : at + SPAN], queries[z, h], preferred_element_type=F32)
            )
            if mask is not None:
                weights = jnp.where(mask[at : at + SPAN], weights, 0.0)
            held[at : at + SPAN, h * SPAN : (h + 1) * SPAN] = weights.astype(BF16)

    for h in range(3):
        score(0, even, h, allowed)

    def pair(i, carry):
        for h in range(3):
            score(2 * i + 1, odd, h)
            weigh(2 * i, even, h)
        for h in range(3):
            score(2 * i + 2, even, h)
            weigh(2 * i + 1, odd, h)
        return carry

    count = plan[65]
    lax.fori_loop(0, count // 2, pair, 0)

    @pl.when(count % 2 == 1)
    def _():
        for h in range(3):
            weigh(count - 1, even, h)

    for z in range(8):
        rows = []
        for h in range(3):
            out[z, h * HEAD : (h + 1) * HEAD] = total[z, :HEAD, h * SPAN : (h + 1) * SPAN].astype(
                BF16
            )
            rows.append(total[z, HEAD : HEAD + 1, h * SPAN : (h + 1) * SPAN])
        high = [row.astype(BF16).astype(F32) for row in rows]
        low = [row - big for row, big in zip(rows, high)]
        out[z, 192:208] = jnp.concatenate(
            high + low + [jnp.zeros((10, SPAN), F32)], axis=0
        ).astype(BF16)

    leaving = []
    here = []
    for h in range(3):
        at = SPAN + 32 * h
        left = jnp.zeros((32, 128), F32)
        kept = jnp.zeros((32, 128), F32)
        for side, held in enumerate((kv_own, kv_oth)):
            for y in range(8):
                state = held[y, at : at + 32].astype(F32)
                place = (side * 8 + y) * 3 + h
                left = left + state * fade[place]
                kept = kept + state * fade[48 + place]
        leaving.append(left)
        here.append(kept)

    def put(z, states):
        states = jnp.concatenate(states, axis=0).astype(BF16)
        out[z, 208:, :128] = states[:48]
        out[z, 208:, 128:] = states[48:]

    for z in range(8):
        put(
            z,
            [
                jnp.where(z > plan[67], leaving[h] * fade[96 + z * 3 + h], 0.0)
                for h in range(3)
            ],
        )
    put(plan[67], here)


def back_kernel(parts, local, lifted, w_out, out, mixed):
    total = parts[0].astype(F32)
    for z in range(1, 8):
        total = total + parts[z].astype(F32)
    states = jnp.concatenate([total[208:, :128], total[208:, 128:]], axis=0)
    for h in range(3):
        held = states[32 * h : 32 * (h + 1)]
        held = jnp.concatenate([held[:, :HEAD], held[:, HEAD:]], axis=0).astype(BF16)
        raw = local[:, h * HEAD : (h + 1) * HEAD] + jnp.dot(
            lifted[:, h * HEAD : (h + 1) * HEAD], held, preferred_element_type=F32
        )
        centred = raw - jnp.mean(raw, axis=-1, keepdims=True)
        spread = jnp.mean(centred * centred, axis=-1, keepdims=True)
        mixed[:, h * HEAD : (h + 1) * HEAD] = (centred * lax.rsqrt(spread + EPS)).astype(BF16)
        weight = total[192 + h : 193 + h] + total[195 + h : 196 + h]
        attended = total[h * HEAD : (h + 1) * HEAD] / weight
        mixed[:, 192 + h * HEAD : 192 + (h + 1) * HEAD] = jnp.transpose(attended).astype(BF16)
    out[...] = lax.dot_general(
        mixed[...], w_out[...], NT, preferred_element_type=F32
    ).astype(BF16)


def body(
    tokens,
    pre_gain,
    w_query_ret,
    w_key_ret,
    w_value_ret,
    w_query_att,
    w_key_att,
    w_value_att,
    w_out_ret,
    w_out_att,
    retain_log,
    forget_total,
):
    z, y, c = (lax.axis_index("z"), lax.axis_index("y"), lax.axis_index("c"))
    ends = jnp.concatenate(three_parts(jnp.sum(retain_log, axis=0)))
    shard = jnp.concatenate(
        [
            w_query_att,
            w_key_att,
            w_value_att,
            w_query_ret,
            w_key_ret,
            w_value_ret,
            w_out_ret.T,
            w_out_att.T,
            jnp.pad(ends[None, :], ((0, 15), (0, 119))),
        ],
        axis=1,
    )
    w_row = copies_from(shard, "y")
    line_ends = jnp.sum(w_row[:, 0, 1280:1289].reshape(8, 3, 3).astype(F32), axis=1)
    w_row = w_row[:, :, :1280].reshape(128, 1280)
    w_own = lax.all_gather(w_row, "z", axis=0, tiled=True)

    raw = tokens.astype(F32)
    normed = (
        raw * lax.rsqrt(jnp.mean(raw * raw, axis=-1, keepdims=True) + EPS) * pre_gain
    ).astype(BF16)
    halves = jnp.transpose(normed.reshape(64, 64, 2, 16), (2, 0, 1, 3)).reshape(2, 64, 1024)
    rows = copies_from(halves, "tp")
    kept = jnp.where(c == 0, rows[:, 0], rows[:, 1]).reshape(SPAN, 1024)
    sent = jnp.where(c == 0, rows[:, 1], rows[:, 0]).reshape(SPAN, 1024)
    came = swapped_cores(sent)
    rows = jnp.concatenate([kept, came], axis=0)

    here = z * 16 + y * 2 + c
    positions = (here * SPAN + jnp.arange(SPAN, dtype=jnp.int32)).astype(F32)
    inverse = THETA ** (-jnp.arange(32, dtype=F32) / 32)
    angles = positions[:, None] * inverse[None, :]
    cosine, sine = (jnp.cos(angles), jnp.sin(angles))
    decay = jnp.cumsum(retain_log, axis=0)
    decay_row = jnp.pad(decay.T, ((0, 5), (0, 0)))
    ends_own = copies_from(line_ends, "z")
    ends_oth = swapped_cores(ends_own)
    ends = jnp.where(
        c == 0,
        jnp.stack([ends_own, ends_oth], axis=2),
        jnp.stack([ends_oth, ends_own], axis=2),
    ).reshape(128, 3)

    gate = (forget_total * LOG2E).reshape(3, 8, 8, 2, SPAN)
    spans = jnp.arange(8, dtype=jnp.int32)
    key_z = (z - spans) % 8
    chosen = (spans[:, None] == key_z[None, :])[None, :, :, None, None]
    key_side = jnp.sum(jnp.where(chosen, gate, 0.0), axis=1)
    key_side = jnp.where(c == 0, key_side, key_side[:, :, ::-1])
    minus = jnp.stack(three_parts(-key_side), axis=1).reshape(9, 8, 2, SPAN)
    key_gate = jnp.concatenate(
        [minus, jnp.ones((3, 8, 2, SPAN), BF16), jnp.zeros((52, 8, 2, SPAN), BF16)], axis=0
    )
    key_gate = jnp.transpose(key_gate, (2, 1, 3, 0))
    mine = lax.dynamic_index_in_dim(
        lax.dynamic_index_in_dim(gate, y, 2, keepdims=False), c, 2, keepdims=False
    )
    plus = jnp.transpose(jnp.stack(three_parts(mine), axis=0), (2, 1, 0, 3))
    own_head = (
        jnp.arange(9, dtype=jnp.int32)[None, :] // 3 == jnp.arange(3, dtype=jnp.int32)[:, None]
    ).astype(BF16)
    query_gate = jnp.concatenate(
        [
            jnp.broadcast_to(own_head[None, :, :, None], (8, 3, 9, SPAN)),
            plus,
            jnp.zeros((8, 3, 52, SPAN), BF16),
        ],
        axis=2,
    )
    first = z * 16 + spans * 2
    blocks = jnp.stack([first + c, first + 1 - c])
    targets = spans * 16 + y * 2 + c
    index = jnp.arange(128, dtype=jnp.int32)
    plane_end = z * 16 + 15

    def faded(chosen, valid):
        total = jnp.sum(jnp.where(chosen[..., None], ends, 0.0), axis=-2)
        return jnp.where(valid[..., None], jnp.exp(total), 0.0).reshape(-1)

    after = index > blocks[..., None]
    fade = jnp.concatenate(
        [
            faded(after & (index <= plane_end), blocks >= 0),
            faded(after & (index < here), blocks < here),
            faded((index > plane_end) & (index < targets[:, None]), spans > z),
        ]
    )
    needed = (
        (key_z[None, :] < spans[:, None])
        | ((key_z[None, :] == spans[:, None]) & (spans[None, :] < y))
    ).reshape(64)
    slot = jnp.cumsum(needed.astype(jnp.int32)) - 1
    order = jnp.arange(64, dtype=jnp.int32)
    units = jnp.sum(
        jnp.where(needed[None, :] & (slot[None, :] == order[:, None]), order[None, :], 0), axis=1
    )
    own = jnp.stack([(z - y) % 8 * 8 + y])
    plan = jnp.concatenate([own, units, jnp.stack([jnp.sum(needed.astype(jnp.int32)) + 1, c, z])])

    own_part, oth_part = pl.pallas_call(
        project_kernel,
        grid=(1,),
        in_specs=[VMEM, pl.BlockSpec((1024, 896), lambda i: (0, 0))],
        out_specs=[VMEM] * 2,
        out_shape=[jax.ShapeDtypeStruct((SPAN, 896), F32)] * 2,
        compiler_params=PARAMS,
        name="project",
    )(rows, w_own)
    came_part = swapped_cores(oth_part)
    attention_part = pl.BlockSpec((SPAN, 384), lambda i: (0, 0))
    q_send, kv_send = pl.pallas_call(
        share_kernel,
        grid=(1,),
        in_specs=[attention_part] * 2,
        out_specs=[VMEM] * 2,
        out_shape=[
            jax.ShapeDtypeStruct((SPAN, SPAN), BF16),
            jax.ShapeDtypeStruct((SPAN, 128), BF16),
        ],
        compiler_params=PARAMS,
        name="share",
    )(own_part, came_part)
    queries = lax.all_gather(q_send, "z", axis=0)
    kv_send = lax.ppermute(kv_send, ("z", "y"), ROTATION)
    state_send, proj = pl.pallas_call(
        front_kernel,
        in_specs=[VMEM] * 5,
        out_specs=[VMEM] * 2,
        out_shape=[jax.ShapeDtypeStruct((96, 128), BF16), jax.ShapeDtypeStruct((SPAN, 896), F32)],
        compiler_params=PARAMS,
        name="front",
    )(own_part, came_part, cosine, sine, decay)
    kv_send = jnp.concatenate([kv_send, state_send], axis=0)
    kv_own = copies_from(kv_send, "y")
    kv_oth = swapped_cores(kv_own)
    local, lifted = pl.pallas_call(
        local_kernel,
        in_specs=[VMEM] * 5,
        out_specs=[VMEM] * 2,
        out_shape=[jax.ShapeDtypeStruct((SPAN, 192), F32), jax.ShapeDtypeStruct((SPAN, 192), BF16)],
        compiler_params=PARAMS,
        name="local",
    )(proj, cosine, sine, decay, decay_row)
    out_own = w_own[:, 896:1280]
    out_oth = swapped_cores(out_own).reshape(64, 16, 384)
    out_own = out_own.reshape(64, 16, 384)
    w_out = jnp.where(
        c == 0, jnp.stack([out_own, out_oth], axis=1), jnp.stack([out_oth, out_own], axis=1)
    ).reshape(2048, 384)

    partial = pl.pallas_call(
        attend_kernel,
        in_specs=[SMEM] * 2 + [VMEM] * 5,
        out_specs=VMEM,
        out_shape=jax.ShapeDtypeStruct((8, SPAN, SPAN), BF16),
        scratch_shapes=[
            pltpu.VMEM((8, 2 * SPAN, 128), BF16),
            pltpu.VMEM((8, 80, 2 * SPAN), BF16),
            pltpu.VMEM((8, 3, 128, SPAN), BF16),
            pltpu.VMEM((8, 80, 3 * SPAN), F32),
            pltpu.VMEM((2 * SPAN, 3 * SPAN), BF16),
            pltpu.VMEM((2 * SPAN, 3 * SPAN), BF16),
        ],
        compiler_params=PARAMS,
        name="attend",
    )(plan, fade, queries, query_gate, kv_own, kv_oth, key_gate)
    parts = lax.all_to_all(partial, "z", 0, 0, tiled=True)

    share = pl.pallas_call(
        back_kernel,
        in_specs=[VMEM] * 4,
        out_specs=VMEM,
        out_shape=jax.ShapeDtypeStruct((SPAN, 2048), BF16),
        scratch_shapes=[pltpu.VMEM((SPAN, 384), BF16)],
        compiler_params=PARAMS,
        name="back",
    )(parts, local, lifted, w_out)
    shares = lax.all_to_all(share.reshape(4, 64, 2048), "tp", 0, 0, tiled=True)
    return jnp.sum(shares.astype(F32), axis=0).astype(BF16)


def solution(mesh):
    finer = Mesh(mesh.devices.reshape(8, 8, 2, mesh.shape["tp"]), ("z", "y", "c", "tp"))
    everyone = ("z", "y", "c", "tp")
    placed = (
        P(everyone, None),
        P(),
        P(SP, "tp"),
        P(SP, "tp"),
        P(SP, "tp"),
        P(SP, "tp"),
        P(SP, "tp"),
        P(SP, "tp"),
        P("tp", SP),
        P("tp", SP),
        P(SP, "tp"),
        P("tp", None),
    )
    return jax.shard_map(
        body, mesh=finer, in_specs=placed, out_specs=P(everyone, None), check_vma=False
    )
```

```python
import jax
import jax.numpy as jnp
from jax import lax
from jax.experimental import pallas as pl
from jax.experimental.pallas import tpu as pltpu
from jax.sharding import Mesh
from jax.sharding import PartitionSpec as P

HEAD = 64
SPAN = 256
SP = ("z", "y", "c")
EPS = 1e-06
THETA = 10000.0
LOG2E = 1.4426950408889634
F32 = jnp.float32
BF16 = jnp.bfloat16
MIRROR = [(z * 8 + y, (7 - z if y % 2 else z) * 8 + y) for z in range(8) for y in range(8)]
NT = (((1,), (1,)), ((), ()))
TN = (((0,), (0,)), ((), ()))
VMEM = pl.BlockSpec(memory_space=pltpu.VMEM)
SMEM = pl.BlockSpec(memory_space=pltpu.SMEM)
PARAMS = pltpu.CompilerParams(vmem_limit_bytes=56 * 1024 * 1024)


def copies_from(shard, axis):
    copies = jnp.broadcast_to(shard, (lax.axis_size(axis), *shard.shape))
    return lax.all_to_all(copies, axis, split_axis=0, concat_axis=0, tiled=True)


def swapped_cores(value):
    return lax.ppermute(value, "c", [(0, 1), (1, 0)])


def three_parts(values):
    high = lax.reduce_precision(values, 8, 7)
    rest = values - high
    middle = lax.reduce_precision(rest, 8, 7)
    low = lax.reduce_precision(rest - middle, 8, 7)
    return [part.astype(BF16) for part in (high, middle, low)]


def project_kernel(rows, weights, own_out, oth_out):
    product = jnp.dot(rows[...], weights[...], preferred_element_type=F32)
    own_out[...] = product[:SPAN]
    oth_out[...] = product[SPAN:]


def share_kernel(first_part, second_part, q_out, kv_out):
    query = first_part[:, :192] + second_part[:, :192]
    q_out[192:] = jnp.zeros((HEAD, SPAN), BF16)
    q_out[:192] = jnp.transpose(query * (HEAD ** (-0.5) * LOG2E)).astype(BF16)
    both = first_part[:, 192:320] + second_part[:, 192:320]
    flipped = jnp.transpose(both)[HEAD:, :].astype(BF16)
    kv_out[:128] = jnp.concatenate([both[:128, :HEAD], both[128:, :HEAD]], axis=1).astype(BF16)
    kv_out[128:] = jnp.concatenate([flipped[:, :128], flipped[:, 128:]], axis=0)


def turned(proj, at, cos, sin):
    first = proj[:, at : at + 32]
    second = proj[:, at + 32 : at + 64]
    return jnp.concatenate([first * cos - second * sin, first * sin + second * cos], axis=1)


def front_kernel(first_part, second_part, cosine, sine, decay, state_out, proj_out):
    proj_out[...] = first_part[...] + second_part[...]
    cos = cosine[...]
    sin = sine[...]
    for h in range(3):
        key = turned(proj_out, 512 + h * HEAD, cos, sin).astype(BF16)
        value = proj_out[:, 704 + h * HEAD : 704 + (h + 1) * HEAD].astype(BF16)
        column = decay[:, h : h + 1]
        last = decay[SPAN - 1 : SPAN, h : h + 1]
        faded = (key.astype(F32) * jnp.exp(last - column)).astype(BF16)
        update = lax.dot_general(faded, value, TN, preferred_element_type=F32).astype(BF16)
        state_out[32 * h : 32 * (h + 1)] = jnp.concatenate([update[:32], update[32:]], axis=1)


def spread_kernel(pairs, states, out):
    for y in range(8):
        out[y, :SPAN] = pairs[...]
        out[y, SPAN:] = states[...]


def local_kernel(proj, cosine, sine, decay, decay_row, local_out, lifted_out):
    cos = cosine[...]
    sin = sine[...]
    place = lax.broadcasted_iota(jnp.int32, (SPAN, SPAN), 0)
    other = lax.broadcasted_iota(jnp.int32, (SPAN, SPAN), 1)
    causal = place >= other
    for h in range(3):
        query = (turned(proj, 320 + h * HEAD, cos, sin) * HEAD ** (-0.5)).astype(BF16)
        key = turned(proj, 512 + h * HEAD, cos, sin).astype(BF16)
        value = proj[:, 704 + h * HEAD : 704 + (h + 1) * HEAD].astype(BF16)
        column = decay[:, h : h + 1]
        scores = lax.dot_general(query, key, NT, preferred_element_type=F32)
        gap = jnp.where(causal, column - decay_row[h : h + 1, :], 0.0)
        weights = jnp.where(causal, scores * jnp.exp(gap), 0.0).astype(BF16)
        local_out[:, h * HEAD : (h + 1) * HEAD] = jnp.dot(
            weights, value, preferred_element_type=F32
        )
        lifted_out[:, h * HEAD : (h + 1) * HEAD] = (
            query.astype(F32) * jnp.exp(column)
        ).astype(BF16)


def attend_kernel(
    plan,
    fade,
    received,
    query_gate,
    kv_own,
    kv_oth,
    key_gate,
    out,
    keys,
    values,
    queries,
    total,
    even,
    odd,
):
    extra = lax.broadcasted_iota(jnp.int32, (16, 2 * SPAN), 0)
    ones = jnp.where(extra == 0, 1.0, 0.0).astype(BF16)
    for y in range(8):
        for side, held in enumerate((kv_own, kv_oth)):
            packed = held[y, :128]
            at = side * SPAN
            keys[y, at : at + 128, :HEAD] = packed[:, :HEAD]
            keys[y, at + 128 : at + SPAN, :HEAD] = packed[:, HEAD:]
            keys[y, at : at + SPAN, HEAD:] = key_gate[side, y]
            values[y, :HEAD, at : at + 128] = held[y, 128:192]
            values[y, :HEAD, at + 128 : at + SPAN] = held[y, 192:SPAN]
        values[y, HEAD:, :] = ones
    for z in range(8):
        for h in range(3):
            queries[z, h, :HEAD] = received[z, h * HEAD : (h + 1) * HEAD]
            queries[z, h, HEAD:] = query_gate[z, h]
    total[...] = jnp.zeros_like(total)

    place = lax.broadcasted_iota(jnp.int32, (2 * SPAN, SPAN), 0)
    wanted = lax.broadcasted_iota(jnp.int32, (2 * SPAN, SPAN), 1)
    allowed = place <= jnp.where(place < SPAN, wanted, plan[66] * (4 * SPAN) - 1)

    def weigh(i, held, h):
        z, y = (plan[i] // 8, plan[i] % 8)
        at = h * SPAN
        total[z, :, at : at + SPAN] += jnp.dot(
            values[y], held[:, at : at + SPAN], preferred_element_type=F32
        )

    def score(i, held, h, mask=None):
        z, y = (plan[i] // 8, plan[i] % 8)
        for at in (0, SPAN):
            weights = jnp.exp2(
                jnp.dot(keys[y, at : at + SPAN], queries[z, h], preferred_element_type=F32)
            )
            if mask is not None:
                weights = jnp.where(mask[at : at + SPAN], weights, 0.0)
            held[at : at + SPAN, h * SPAN : (h + 1) * SPAN] = weights.astype(BF16)

    for h in range(3):
        score(0, even, h, allowed)

    def pair(i, carry):
        for h in range(3):
            score(2 * i + 1, odd, h)
            weigh(2 * i, even, h)
        for h in range(3):
            score(2 * i + 2, even, h)
            weigh(2 * i + 1, odd, h)
        return carry

    count = plan[65]
    lax.fori_loop(0, count // 2, pair, 0)

    @pl.when(count % 2 == 1)
    def _():
        for h in range(3):
            weigh(count - 1, even, h)

    for z in range(8):
        rows = []
        for h in range(3):
            out[z, h * HEAD : (h + 1) * HEAD] = total[z, :HEAD, h * SPAN : (h + 1) * SPAN].astype(
                BF16
            )
            rows.append(total[z, HEAD : HEAD + 1, h * SPAN : (h + 1) * SPAN])
        high = [row.astype(BF16).astype(F32) for row in rows]
        low = [row - big for row, big in zip(rows, high)]
        out[z, 192:208] = jnp.concatenate(
            high + low + [jnp.zeros((10, SPAN), F32)], axis=0
        ).astype(BF16)

    leaving = []
    here = []
    for h in range(3):
        at = SPAN + 32 * h
        left = jnp.zeros((32, 128), F32)
        kept = jnp.zeros((32, 128), F32)
        for side, held in enumerate((kv_own, kv_oth)):
            for y in range(8):
                state = held[y, at : at + 32].astype(F32)
                place = (side * 8 + y) * 3 + h
                left = left + state * fade[place]
                kept = kept + state * fade[48 + place]
        leaving.append(left)
        here.append(kept)

    def put(z, states):
        states = jnp.concatenate(states, axis=0).astype(BF16)
        out[z, 208:, :128] = states[:48]
        out[z, 208:, 128:] = states[48:]

    for z in range(8):
        put(
            z,
            [
                jnp.where(z > plan[67], leaving[h] * fade[96 + z * 3 + h], 0.0)
                for h in range(3)
            ],
        )
    put(plan[67], here)


def back_kernel(parts, local, lifted, w_out, out, mixed):
    @pl.when(pl.program_id(0) == 0)
    def _():
        total = parts[0].astype(F32)
        for z in range(1, 8):
            total = total + parts[z].astype(F32)
        states = jnp.concatenate([total[208:, :128], total[208:, 128:]], axis=0)
        for h in range(3):
            held = states[32 * h : 32 * (h + 1)]
            held = jnp.concatenate([held[:, :HEAD], held[:, HEAD:]], axis=0).astype(BF16)
            raw = local[:, h * HEAD : (h + 1) * HEAD] + jnp.dot(
                lifted[:, h * HEAD : (h + 1) * HEAD], held, preferred_element_type=F32
            )
            centred = raw - jnp.mean(raw, axis=-1, keepdims=True)
            spread = jnp.mean(centred * centred, axis=-1, keepdims=True)
            mixed[:, h * HEAD : (h + 1) * HEAD] = (centred * lax.rsqrt(spread + EPS)).astype(BF16)
            weight = total[192 + h : 193 + h] + total[195 + h : 196 + h]
            attended = total[h * HEAD : (h + 1) * HEAD] / weight
            mixed[:, 192 + h * HEAD : 192 + (h + 1) * HEAD] = jnp.transpose(attended).astype(BF16)

    out[...] = lax.dot_general(
        mixed[...], w_out[...], NT, preferred_element_type=F32
    ).astype(BF16)


def body(
    tokens,
    pre_gain,
    w_query_ret,
    w_key_ret,
    w_value_ret,
    w_query_att,
    w_key_att,
    w_value_att,
    w_out_ret,
    w_out_att,
    retain_log,
    forget_total,
):
    z, y, c = (lax.axis_index("z"), lax.axis_index("y"), lax.axis_index("c"))
    ends = jnp.concatenate(three_parts(jnp.sum(retain_log, axis=0)))
    shard = jnp.concatenate(
        [
            w_query_att,
            w_key_att,
            w_value_att,
            w_query_ret,
            w_key_ret,
            w_value_ret,
            w_out_ret.T,
            w_out_att.T,
            jnp.pad(ends[None, :], ((0, 15), (0, 119))),
        ],
        axis=1,
    )
    w_row = copies_from(shard, "y")
    line_ends = jnp.sum(w_row[:, 0, 1280:1289].reshape(8, 3, 3).astype(F32), axis=1)
    w_row = w_row[:, :, :1280].reshape(128, 1280)
    w_own = lax.all_gather(w_row, "z", axis=0, tiled=True)

    raw = tokens.astype(F32)
    normed = (
        raw * lax.rsqrt(jnp.mean(raw * raw, axis=-1, keepdims=True) + EPS) * pre_gain
    ).astype(BF16)
    halves = jnp.transpose(normed.reshape(64, 64, 2, 16), (2, 0, 1, 3)).reshape(2, 64, 1024)
    rows = copies_from(halves, "tp")
    kept = jnp.where(c == 0, rows[:, 0], rows[:, 1]).reshape(SPAN, 1024)
    sent = jnp.where(c == 0, rows[:, 1], rows[:, 0]).reshape(SPAN, 1024)
    came = swapped_cores(sent)
    rows = jnp.concatenate([kept, came], axis=0)

    here = z * 16 + y * 2 + c
    positions = (here * SPAN + jnp.arange(SPAN, dtype=jnp.int32)).astype(F32)
    inverse = THETA ** (-jnp.arange(32, dtype=F32) / 32)
    angles = positions[:, None] * inverse[None, :]
    cosine, sine = (jnp.cos(angles), jnp.sin(angles))
    decay = jnp.cumsum(retain_log, axis=0)
    decay_row = jnp.pad(decay.T, ((0, 5), (0, 0)))
    ends_own = copies_from(line_ends, "z")
    ends_oth = swapped_cores(ends_own)
    ends = jnp.where(
        c == 0,
        jnp.stack([ends_own, ends_oth], axis=2),
        jnp.stack([ends_oth, ends_own], axis=2),
    ).reshape(128, 3)

    gate = (forget_total * LOG2E).reshape(3, 8, 8, 2, SPAN)
    spans = jnp.arange(8, dtype=jnp.int32)
    key_z = jnp.where(spans % 2 == 0, z, 7 - z)
    chosen = (spans[:, None] == key_z[None, :])[None, :, :, None, None]
    key_side = jnp.sum(jnp.where(chosen, gate, 0.0), axis=1)
    key_side = jnp.where(c == 0, key_side, key_side[:, :, ::-1])
    minus = jnp.stack(three_parts(-key_side), axis=1).reshape(9, 8, 2, SPAN)
    key_gate = jnp.concatenate(
        [minus, jnp.ones((3, 8, 2, SPAN), BF16), jnp.zeros((52, 8, 2, SPAN), BF16)], axis=0
    )
    key_gate = jnp.transpose(key_gate, (2, 1, 3, 0))
    mine = lax.dynamic_index_in_dim(
        lax.dynamic_index_in_dim(gate, y, 2, keepdims=False), c, 2, keepdims=False
    )
    plus = jnp.transpose(jnp.stack(three_parts(mine), axis=0), (2, 1, 0, 3))
    own_head = (
        jnp.arange(9, dtype=jnp.int32)[None, :] // 3 == jnp.arange(3, dtype=jnp.int32)[:, None]
    ).astype(BF16)
    query_gate = jnp.concatenate(
        [
            jnp.broadcast_to(own_head[None, :, :, None], (8, 3, 9, SPAN)),
            plus,
            jnp.zeros((8, 3, 52, SPAN), BF16),
        ],
        axis=2,
    )
    first = z * 16 + spans * 2
    blocks = jnp.stack([first + c, first + 1 - c])
    targets = spans * 16 + y * 2 + c
    index = jnp.arange(128, dtype=jnp.int32)
    plane_end = z * 16 + 15

    def faded(chosen, valid):
        total = jnp.sum(jnp.where(chosen[..., None], ends, 0.0), axis=-2)
        return jnp.where(valid[..., None], jnp.exp(total), 0.0).reshape(-1)

    after = index > blocks[..., None]
    fade = jnp.concatenate(
        [
            faded(after & (index <= plane_end), blocks >= 0),
            faded(after & (index < here), blocks < here),
            faded((index > plane_end) & (index < targets[:, None]), spans > z),
        ]
    )
    needed = (
        (key_z[None, :] < spans[:, None])
        | ((key_z[None, :] == spans[:, None]) & (spans[None, :] < y))
    ).reshape(64)
    slot = jnp.cumsum(needed.astype(jnp.int32)) - 1
    order = jnp.arange(64, dtype=jnp.int32)
    units = jnp.sum(
        jnp.where(needed[None, :] & (slot[None, :] == order[:, None]), order[None, :], 0), axis=1
    )
    own = jnp.stack([jnp.where(y % 2 == 0, z, 7 - z) * 8 + y])
    plan = jnp.concatenate([own, units, jnp.stack([jnp.sum(needed.astype(jnp.int32)) + 1, c, z])])

    own_part, oth_part = pl.pallas_call(
        project_kernel,
        grid=(1,),
        in_specs=[VMEM, pl.BlockSpec((1024, 896), lambda i: (0, 0))],
        out_specs=[VMEM] * 2,
        out_shape=[jax.ShapeDtypeStruct((SPAN, 896), F32)] * 2,
        compiler_params=PARAMS,
        name="project",
    )(rows, w_own)
    came_part = swapped_cores(oth_part)
    attention_part = pl.BlockSpec((SPAN, 384), lambda i: (0, 0))
    q_send, kv_send = pl.pallas_call(
        share_kernel,
        grid=(1,),
        in_specs=[attention_part] * 2,
        out_specs=[VMEM] * 2,
        out_shape=[
            jax.ShapeDtypeStruct((SPAN, SPAN), BF16),
            jax.ShapeDtypeStruct((SPAN, 128), BF16),
        ],
        compiler_params=PARAMS,
        name="share",
    )(own_part, came_part)
    queries = lax.all_gather(q_send, "z", axis=0)
    kv_send = lax.ppermute(kv_send, ("z", "y"), MIRROR)
    state_send, proj = pl.pallas_call(
        front_kernel,
        in_specs=[VMEM] * 5,
        out_specs=[VMEM] * 2,
        out_shape=[jax.ShapeDtypeStruct((96, 128), BF16), jax.ShapeDtypeStruct((SPAN, 896), F32)],
        compiler_params=PARAMS,
        name="front",
    )(own_part, came_part, cosine, sine, decay)
    kv_send = pl.pallas_call(
        spread_kernel,
        in_specs=[VMEM] * 2,
        out_specs=VMEM,
        out_shape=jax.ShapeDtypeStruct((8, SPAN + 96, 128), BF16),
        compiler_params=PARAMS,
        name="spread",
    )(kv_send, state_send)
    kv_own = lax.all_to_all(kv_send, "y", 0, 0, tiled=True)
    kv_oth = swapped_cores(kv_own)
    local, lifted = pl.pallas_call(
        local_kernel,
        in_specs=[VMEM] * 5,
        out_specs=[VMEM] * 2,
        out_shape=[jax.ShapeDtypeStruct((SPAN, 192), F32), jax.ShapeDtypeStruct((SPAN, 192), BF16)],
        compiler_params=PARAMS,
        name="local",
    )(proj, cosine, sine, decay, decay_row)
    out_own = w_own[:, 896:1280]
    out_oth = swapped_cores(out_own).reshape(64, 16, 384)
    out_own = out_own.reshape(64, 16, 384)
    w_out = jnp.where(
        c == 0, jnp.stack([out_own, out_oth], axis=1), jnp.stack([out_oth, out_own], axis=1)
    ).reshape(2048, 384)

    partial = pl.pallas_call(
        attend_kernel,
        in_specs=[SMEM] * 2 + [VMEM] * 5,
        out_specs=VMEM,
        out_shape=jax.ShapeDtypeStruct((8, SPAN, SPAN), BF16),
        scratch_shapes=[
            pltpu.VMEM((8, 2 * SPAN, 128), BF16),
            pltpu.VMEM((8, 80, 2 * SPAN), BF16),
            pltpu.VMEM((8, 3, 128, SPAN), BF16),
            pltpu.VMEM((8, 80, 3 * SPAN), F32),
            pltpu.VMEM((2 * SPAN, 3 * SPAN), BF16),
            pltpu.VMEM((2 * SPAN, 3 * SPAN), BF16),
        ],
        compiler_params=PARAMS,
        name="attend",
    )(plan, fade, queries, query_gate, kv_own, kv_oth, key_gate)
    parts = lax.all_to_all(partial, "z", 0, 0, tiled=True)

    share = pl.pallas_call(
        back_kernel,
        grid=(2,),
        in_specs=[VMEM] * 3 + [pl.BlockSpec((1024, 384), lambda i: (i, 0))],
        out_specs=pl.BlockSpec((SPAN, 1024), lambda i: (0, i)),
        out_shape=jax.ShapeDtypeStruct((SPAN, 2048), BF16),
        scratch_shapes=[pltpu.VMEM((SPAN, 384), BF16)],
        compiler_params=PARAMS,
        name="back",
    )(parts, local, lifted, w_out)
    shares = lax.all_to_all(share.reshape(4, 64, 2048), "tp", 0, 0, tiled=True)
    return jnp.sum(shares.astype(F32), axis=0).astype(BF16)


def solution(mesh):
    finer = Mesh(mesh.devices.reshape(8, 8, 2, mesh.shape["tp"]), ("z", "y", "c", "tp"))
    everyone = ("z", "y", "c", "tp")
    placed = (
        P(everyone, None),
        P(),
        P(SP, "tp"),
        P(SP, "tp"),
        P(SP, "tp"),
        P(SP, "tp"),
        P(SP, "tp"),
        P(SP, "tp"),
        P("tp", SP),
        P("tp", SP),
        P(SP, "tp"),
        P("tp", None),
    )
    return jax.shard_map(
        body, mesh=finer, in_specs=placed, out_specs=P(everyone, None), check_vma=False
    )
```

```python
import jax
import jax.numpy as jnp
from jax import lax
from jax.experimental import pallas as pl
from jax.experimental.pallas import tpu as pltpu
from jax.sharding import Mesh
from jax.sharding import PartitionSpec as P

HEAD = 64
SPAN = 256
SP = ("z", "y", "c")
EPS = 1e-06
THETA = 10000.0
LOG2E = 1.4426950408889634
F32 = jnp.float32
BF16 = jnp.bfloat16
MIRROR = [(z * 8 + y, (7 - z if y % 2 else z) * 8 + y) for z in range(8) for y in range(8)]
NT = (((1,), (1,)), ((), ()))
TN = (((0,), (0,)), ((), ()))
VMEM = pl.BlockSpec(memory_space=pltpu.VMEM)
SMEM = pl.BlockSpec(memory_space=pltpu.SMEM)
PARAMS = pltpu.CompilerParams(vmem_limit_bytes=56 * 1024 * 1024)


def copies_from(shard, axis):
    copies = jnp.broadcast_to(shard, (lax.axis_size(axis), *shard.shape))
    return lax.all_to_all(copies, axis, split_axis=0, concat_axis=0, tiled=True)


def swapped_cores(value):
    return lax.ppermute(value, "c", [(0, 1), (1, 0)])


def three_parts(values):
    high = lax.reduce_precision(values, 8, 7)
    rest = values - high
    middle = lax.reduce_precision(rest, 8, 7)
    low = lax.reduce_precision(rest - middle, 8, 7)
    return [part.astype(BF16) for part in (high, middle, low)]


def project_kernel(rows, weights, own_out, oth_out):
    product = jnp.dot(rows[...], weights[...], preferred_element_type=F32)
    own_out[...] = product[:SPAN]
    oth_out[...] = product[SPAN:]


def share_kernel(first_part, second_part, q_out, kv_out):
    query = first_part[:, :192] + second_part[:, :192]
    q_out[192:] = jnp.zeros((HEAD, SPAN), BF16)
    q_out[:192] = jnp.transpose(query * (HEAD ** (-0.5) * LOG2E)).astype(BF16)
    both = first_part[:, 192:320] + second_part[:, 192:320]
    flipped = jnp.transpose(both)[HEAD:, :].astype(BF16)
    kv_out[:128] = jnp.concatenate([both[:128, :HEAD], both[128:, :HEAD]], axis=1).astype(BF16)
    kv_out[128:] = jnp.concatenate([flipped[:, :128], flipped[:, 128:]], axis=0)


def turned(proj, at, cos, sin):
    first = proj[:, at : at + 32]
    second = proj[:, at + 32 : at + 64]
    return jnp.concatenate([first * cos - second * sin, first * sin + second * cos], axis=1)


def front_kernel(first_part, second_part, cosine, sine, decay, state_out, proj_out):
    proj_out[...] = first_part[...] + second_part[...]
    cos = cosine[...]
    sin = sine[...]
    for h in range(3):
        key = turned(proj_out, 512 + h * HEAD, cos, sin).astype(BF16)
        value = proj_out[:, 704 + h * HEAD : 704 + (h + 1) * HEAD].astype(BF16)
        column = decay[:, h : h + 1]
        last = decay[SPAN - 1 : SPAN, h : h + 1]
        faded = (key.astype(F32) * jnp.exp(last - column)).astype(BF16)
        update = lax.dot_general(faded, value, TN, preferred_element_type=F32).astype(BF16)
        state_out[32 * h : 32 * (h + 1)] = jnp.concatenate([update[:32], update[32:]], axis=1)


def spread_kernel(pairs, states, out):
    for y in range(8):
        out[y, :SPAN] = pairs[...]
        out[y, SPAN:] = states[...]


def local_kernel(proj, cosine, sine, decay, decay_row, local_out, lifted_out):
    cos = cosine[...]
    sin = sine[...]
    place = lax.broadcasted_iota(jnp.int32, (SPAN, SPAN), 0)
    other = lax.broadcasted_iota(jnp.int32, (SPAN, SPAN), 1)
    causal = place >= other
    for h in range(3):
        query = (turned(proj, 320 + h * HEAD, cos, sin) * HEAD ** (-0.5)).astype(BF16)
        key = turned(proj, 512 + h * HEAD, cos, sin).astype(BF16)
        value = proj[:, 704 + h * HEAD : 704 + (h + 1) * HEAD].astype(BF16)
        column = decay[:, h : h + 1]
        scores = lax.dot_general(query, key, NT, preferred_element_type=F32)
        gap = jnp.where(causal, column - decay_row[h : h + 1, :], 0.0)
        weights = jnp.where(causal, scores * jnp.exp(gap), 0.0).astype(BF16)
        local_out[:, h * HEAD : (h + 1) * HEAD] = jnp.dot(
            weights, value, preferred_element_type=F32
        )
        lifted_out[:, h * HEAD : (h + 1) * HEAD] = (
            query.astype(F32) * jnp.exp(column)
        ).astype(BF16)


def attend_kernel(
    plan,
    fade,
    received,
    query_gate,
    kv_own,
    kv_oth,
    key_gate,
    out,
    keys,
    values,
    queries,
    total,
    even,
    odd,
):
    extra = lax.broadcasted_iota(jnp.int32, (16, 2 * SPAN), 0)
    ones = jnp.where(extra == 0, 1.0, 0.0).astype(BF16)
    for y in range(8):
        for side, held in enumerate((kv_own, kv_oth)):
            packed = held[y, :128]
            at = side * SPAN
            keys[y, at : at + 128, :HEAD] = packed[:, :HEAD]
            keys[y, at + 128 : at + SPAN, :HEAD] = packed[:, HEAD:]
            keys[y, at : at + SPAN, HEAD:] = key_gate[side, y]
            values[y, :HEAD, at : at + 128] = held[y, 128:192]
            values[y, :HEAD, at + 128 : at + SPAN] = held[y, 192:SPAN]
        values[y, HEAD:, :] = ones
    for z in range(8):
        for h in range(3):
            queries[z, h, :HEAD] = received[z, h * HEAD : (h + 1) * HEAD]
            queries[z, h, HEAD:] = query_gate[z, h]
    total[...] = jnp.zeros_like(total)

    place = lax.broadcasted_iota(jnp.int32, (2 * SPAN, SPAN), 0)
    wanted = lax.broadcasted_iota(jnp.int32, (2 * SPAN, SPAN), 1)
    allowed = place <= jnp.where(place < SPAN, wanted, plan[66] * (4 * SPAN) - 1)

    def weigh(i, held, h):
        z, y = (plan[i] // 8, plan[i] % 8)
        at = h * SPAN
        total[z, :, at : at + SPAN] += jnp.dot(
            values[y], held[:, at : at + SPAN], preferred_element_type=F32
        )

    def score(i, held, h, mask=None):
        z, y = (plan[i] // 8, plan[i] % 8)
        for at in (0, SPAN):
            weights = jnp.exp2(
                jnp.dot(keys[y, at : at + SPAN], queries[z, h], preferred_element_type=F32)
            )
            if mask is not None:
                weights = jnp.where(mask[at : at + SPAN], weights, 0.0)
            held[at : at + SPAN, h * SPAN : (h + 1) * SPAN] = weights.astype(BF16)

    for h in range(3):
        score(0, even, h, allowed)

    def pair(i, carry):
        for h in range(3):
            score(2 * i + 1, odd, h)
            weigh(2 * i, even, h)
        for h in range(3):
            score(2 * i + 2, even, h)
            weigh(2 * i + 1, odd, h)
        return carry

    count = plan[65]
    lax.fori_loop(0, count // 2, pair, 0)

    @pl.when(count % 2 == 1)
    def _():
        for h in range(3):
            weigh(count - 1, even, h)

    for z in range(8):
        rows = []
        for h in range(3):
            out[z, h * HEAD : (h + 1) * HEAD] = total[z, :HEAD, h * SPAN : (h + 1) * SPAN].astype(
                BF16
            )
            rows.append(total[z, HEAD : HEAD + 1, h * SPAN : (h + 1) * SPAN])
        high = [row.astype(BF16).astype(F32) for row in rows]
        low = [row - big for row, big in zip(rows, high)]
        out[z, 192:208] = jnp.concatenate(
            high + low + [jnp.zeros((10, SPAN), F32)], axis=0
        ).astype(BF16)

    leaving = []
    here = []
    for h in range(3):
        at = SPAN + 32 * h
        left = jnp.zeros((32, 128), F32)
        kept = jnp.zeros((32, 128), F32)
        for side, held in enumerate((kv_own, kv_oth)):
            for y in range(8):
                state = held[y, at : at + 32].astype(F32)
                place = (side * 8 + y) * 3 + h
                left = left + state * fade[place]
                kept = kept + state * fade[48 + place]
        leaving.append(left)
        here.append(kept)

    def put(z, states):
        states = jnp.concatenate(states, axis=0).astype(BF16)
        out[z, 208:, :128] = states[:48]
        out[z, 208:, 128:] = states[48:]

    for z in range(8):
        put(
            z,
            [
                jnp.where(z > plan[67], leaving[h] * fade[96 + z * 3 + h], 0.0)
                for h in range(3)
            ],
        )
    put(plan[67], here)


def back_kernel(turn, parts, local, lifted, w_out, far, mixed):
    total = parts[0].astype(F32)
    for z in range(1, 8):
        total = total + parts[z].astype(F32)
    states = jnp.concatenate([total[208:, :128], total[208:, 128:]], axis=0)
    for h in range(3):
        held = states[32 * h : 32 * (h + 1)]
        held = jnp.concatenate([held[:, :HEAD], held[:, HEAD:]], axis=0).astype(BF16)
        raw = local[:, h * HEAD : (h + 1) * HEAD] + jnp.dot(
            lifted[:, h * HEAD : (h + 1) * HEAD], held, preferred_element_type=F32
        )
        centred = raw - jnp.mean(raw, axis=-1, keepdims=True)
        spread = jnp.mean(centred * centred, axis=-1, keepdims=True)
        mixed[:, h * HEAD : (h + 1) * HEAD] = (centred * lax.rsqrt(spread + EPS)).astype(BF16)
        weight = total[192 + h : 193 + h] + total[195 + h : 196 + h]
        attended = total[h * HEAD : (h + 1) * HEAD] / weight
        mixed[:, 192 + h * HEAD : 192 + (h + 1) * HEAD] = jnp.transpose(attended).astype(BF16)

    far[...] = lax.dot_general(
        mixed[pl.ds((turn[0] + 2) % 4 * 64, 64)], w_out[...], NT, preferred_element_type=F32
    ).astype(BF16)


def rest_kernel(turn, mixed, w_out, ahead, behind, own):
    rows = [mixed[pl.ds((turn[0] + k) % 4 * 64, 64)] for k in (1, 3, 0)]
    product = lax.dot_general(
        jnp.concatenate(rows, axis=0), w_out[...], NT, preferred_element_type=F32
    ).astype(BF16)
    ahead[...] = product[:64]
    behind[...] = product[64:128]
    own[...] = product[128:]


def body(
    tokens,
    pre_gain,
    w_query_ret,
    w_key_ret,
    w_value_ret,
    w_query_att,
    w_key_att,
    w_value_att,
    w_out_ret,
    w_out_att,
    retain_log,
    forget_total,
):
    z, y, c = (lax.axis_index("z"), lax.axis_index("y"), lax.axis_index("c"))
    ends = jnp.concatenate(three_parts(jnp.sum(retain_log, axis=0)))
    shard = jnp.concatenate(
        [
            w_query_att,
            w_key_att,
            w_value_att,
            w_query_ret,
            w_key_ret,
            w_value_ret,
            w_out_ret.T,
            w_out_att.T,
            jnp.pad(ends[None, :], ((0, 15), (0, 119))),
        ],
        axis=1,
    )
    w_row = copies_from(shard, "y")
    line_ends = jnp.sum(w_row[:, 0, 1280:1289].reshape(8, 3, 3).astype(F32), axis=1)
    w_row = w_row[:, :, :1280].reshape(128, 1280)
    w_own = lax.all_gather(w_row, "z", axis=0, tiled=True)

    raw = tokens.astype(F32)
    normed = (
        raw * lax.rsqrt(jnp.mean(raw * raw, axis=-1, keepdims=True) + EPS) * pre_gain
    ).astype(BF16)
    halves = jnp.transpose(normed.reshape(64, 64, 2, 16), (2, 0, 1, 3)).reshape(2, 64, 1024)
    rows = copies_from(halves, "tp")
    kept = jnp.where(c == 0, rows[:, 0], rows[:, 1]).reshape(SPAN, 1024)
    sent = jnp.where(c == 0, rows[:, 1], rows[:, 0]).reshape(SPAN, 1024)
    came = swapped_cores(sent)
    rows = jnp.concatenate([kept, came], axis=0)

    here = z * 16 + y * 2 + c
    positions = (here * SPAN + jnp.arange(SPAN, dtype=jnp.int32)).astype(F32)
    inverse = THETA ** (-jnp.arange(32, dtype=F32) / 32)
    angles = positions[:, None] * inverse[None, :]
    cosine, sine = (jnp.cos(angles), jnp.sin(angles))
    decay = jnp.cumsum(retain_log, axis=0)
    decay_row = jnp.pad(decay.T, ((0, 5), (0, 0)))
    ends_own = copies_from(line_ends, "z")
    ends_oth = swapped_cores(ends_own)
    ends = jnp.where(
        c == 0,
        jnp.stack([ends_own, ends_oth], axis=2),
        jnp.stack([ends_oth, ends_own], axis=2),
    ).reshape(128, 3)

    gate = (forget_total * LOG2E).reshape(3, 8, 8, 2, SPAN)
    spans = jnp.arange(8, dtype=jnp.int32)
    key_z = jnp.where(spans % 2 == 0, z, 7 - z)
    chosen = (spans[:, None] == key_z[None, :])[None, :, :, None, None]
    key_side = jnp.sum(jnp.where(chosen, gate, 0.0), axis=1)
    key_side = jnp.where(c == 0, key_side, key_side[:, :, ::-1])
    minus = jnp.stack(three_parts(-key_side), axis=1).reshape(9, 8, 2, SPAN)
    key_gate = jnp.concatenate(
        [minus, jnp.ones((3, 8, 2, SPAN), BF16), jnp.zeros((52, 8, 2, SPAN), BF16)], axis=0
    )
    key_gate = jnp.transpose(key_gate, (2, 1, 3, 0))
    mine = lax.dynamic_index_in_dim(
        lax.dynamic_index_in_dim(gate, y, 2, keepdims=False), c, 2, keepdims=False
    )
    plus = jnp.transpose(jnp.stack(three_parts(mine), axis=0), (2, 1, 0, 3))
    own_head = (
        jnp.arange(9, dtype=jnp.int32)[None, :] // 3 == jnp.arange(3, dtype=jnp.int32)[:, None]
    ).astype(BF16)
    query_gate = jnp.concatenate(
        [
            jnp.broadcast_to(own_head[None, :, :, None], (8, 3, 9, SPAN)),
            plus,
            jnp.zeros((8, 3, 52, SPAN), BF16),
        ],
        axis=2,
    )
    first = z * 16 + spans * 2
    blocks = jnp.stack([first + c, first + 1 - c])
    targets = spans * 16 + y * 2 + c
    index = jnp.arange(128, dtype=jnp.int32)
    plane_end = z * 16 + 15

    def faded(chosen, valid):
        total = jnp.sum(jnp.where(chosen[..., None], ends, 0.0), axis=-2)
        return jnp.where(valid[..., None], jnp.exp(total), 0.0).reshape(-1)

    after = index > blocks[..., None]
    fade = jnp.concatenate(
        [
            faded(after & (index <= plane_end), blocks >= 0),
            faded(after & (index < here), blocks < here),
            faded((index > plane_end) & (index < targets[:, None]), spans > z),
        ]
    )
    needed = (
        (key_z[None, :] < spans[:, None])
        | ((key_z[None, :] == spans[:, None]) & (spans[None, :] < y))
    ).reshape(64)
    slot = jnp.cumsum(needed.astype(jnp.int32)) - 1
    order = jnp.arange(64, dtype=jnp.int32)
    units = jnp.sum(
        jnp.where(needed[None, :] & (slot[None, :] == order[:, None]), order[None, :], 0), axis=1
    )
    own = jnp.stack([jnp.where(y % 2 == 0, z, 7 - z) * 8 + y])
    plan = jnp.concatenate([own, units, jnp.stack([jnp.sum(needed.astype(jnp.int32)) + 1, c, z])])

    own_part, oth_part = pl.pallas_call(
        project_kernel,
        grid=(1,),
        in_specs=[VMEM, pl.BlockSpec((1024, 896), lambda i: (0, 0))],
        out_specs=[VMEM] * 2,
        out_shape=[jax.ShapeDtypeStruct((SPAN, 896), F32)] * 2,
        compiler_params=PARAMS,
        name="project",
    )(rows, w_own)
    came_part = swapped_cores(oth_part)
    attention_part = pl.BlockSpec((SPAN, 384), lambda i: (0, 0))
    q_send, kv_send = pl.pallas_call(
        share_kernel,
        grid=(1,),
        in_specs=[attention_part] * 2,
        out_specs=[VMEM] * 2,
        out_shape=[
            jax.ShapeDtypeStruct((SPAN, SPAN), BF16),
            jax.ShapeDtypeStruct((SPAN, 128), BF16),
        ],
        compiler_params=PARAMS,
        name="share",
    )(own_part, came_part)
    queries = lax.all_gather(q_send, "z", axis=0)
    kv_send = lax.ppermute(kv_send, ("z", "y"), MIRROR)
    state_send, proj = pl.pallas_call(
        front_kernel,
        in_specs=[VMEM] * 5,
        out_specs=[VMEM] * 2,
        out_shape=[jax.ShapeDtypeStruct((96, 128), BF16), jax.ShapeDtypeStruct((SPAN, 896), F32)],
        compiler_params=PARAMS,
        name="front",
    )(own_part, came_part, cosine, sine, decay)
    kv_send = pl.pallas_call(
        spread_kernel,
        in_specs=[VMEM] * 2,
        out_specs=VMEM,
        out_shape=jax.ShapeDtypeStruct((8, SPAN + 96, 128), BF16),
        compiler_params=PARAMS,
        name="spread",
    )(kv_send, state_send)
    kv_own = lax.all_to_all(kv_send, "y", 0, 0, tiled=True)
    kv_oth = swapped_cores(kv_own)
    local, lifted = pl.pallas_call(
        local_kernel,
        in_specs=[VMEM] * 5,
        out_specs=[VMEM] * 2,
        out_shape=[jax.ShapeDtypeStruct((SPAN, 192), F32), jax.ShapeDtypeStruct((SPAN, 192), BF16)],
        compiler_params=PARAMS,
        name="local",
    )(proj, cosine, sine, decay, decay_row)
    out_own = w_own[:, 896:1280]
    out_oth = swapped_cores(out_own).reshape(64, 16, 384)
    out_own = out_own.reshape(64, 16, 384)
    w_out = jnp.where(
        c == 0, jnp.stack([out_own, out_oth], axis=1), jnp.stack([out_oth, out_own], axis=1)
    ).reshape(2048, 384)

    partial = pl.pallas_call(
        attend_kernel,
        in_specs=[SMEM] * 2 + [VMEM] * 5,
        out_specs=VMEM,
        out_shape=jax.ShapeDtypeStruct((8, SPAN, SPAN), BF16),
        scratch_shapes=[
            pltpu.VMEM((8, 2 * SPAN, 128), BF16),
            pltpu.VMEM((8, 80, 2 * SPAN), BF16),
            pltpu.VMEM((8, 3, 128, SPAN), BF16),
            pltpu.VMEM((8, 80, 3 * SPAN), F32),
            pltpu.VMEM((2 * SPAN, 3 * SPAN), BF16),
            pltpu.VMEM((2 * SPAN, 3 * SPAN), BF16),
        ],
        compiler_params=PARAMS,
        name="attend",
    )(plan, fade, queries, query_gate, kv_own, kv_oth, key_gate)
    parts = lax.all_to_all(partial, "z", 0, 0, tiled=True)

    turn = lax.axis_index("tp").reshape(1)
    chunk = jax.ShapeDtypeStruct((64, 2048), BF16)
    far, mixed = pl.pallas_call(
        back_kernel,
        in_specs=[SMEM] + [VMEM] * 4,
        out_specs=[VMEM] * 2,
        out_shape=[chunk, jax.ShapeDtypeStruct((SPAN, 384), BF16)],
        compiler_params=PARAMS,
        name="back",
    )(turn, parts, local, lifted, w_out)
    far = lax.ppermute(far, "tp", [(i, (i + 2) % 4) for i in range(4)])
    ahead, behind, own = pl.pallas_call(
        rest_kernel,
        in_specs=[SMEM] + [VMEM] * 2,
        out_specs=[VMEM] * 3,
        out_shape=[chunk] * 3,
        compiler_params=PARAMS,
        name="rest",
    )(turn, mixed, w_out)
    ahead = lax.ppermute(ahead, "tp", [(i, (i + 1) % 4) for i in range(4)])
    behind = lax.ppermute(behind, "tp", [(i, (i + 3) % 4) for i in range(4)])
    total = own.astype(F32) + far.astype(F32) + ahead.astype(F32) + behind.astype(F32)
    return total.astype(BF16)


def solution(mesh):
    finer = Mesh(mesh.devices.reshape(8, 8, 2, mesh.shape["tp"]), ("z", "y", "c", "tp"))
    everyone = ("z", "y", "c", "tp")
    placed = (
        P(everyone, None),
        P(),
        P(SP, "tp"),
        P(SP, "tp"),
        P(SP, "tp"),
        P(SP, "tp"),
        P(SP, "tp"),
        P(SP, "tp"),
        P("tp", SP),
        P("tp", SP),
        P(SP, "tp"),
        P("tp", None),
    )
    return jax.shard_map(
        body, mesh=finer, in_specs=placed, out_specs=P(everyone, None), check_vma=False
    )
```

```python
import jax
import jax.numpy as jnp
from jax import lax
from jax.experimental import pallas as pl
from jax.experimental.pallas import tpu as pltpu
from jax.sharding import Mesh
from jax.sharding import PartitionSpec as P

HEAD = 64
SPAN = 256
SP = ("z", "y", "c")
EPS = 1e-06
THETA = 10000.0
LOG2E = 1.4426950408889634
F32 = jnp.float32
BF16 = jnp.bfloat16
MIRROR = [(z * 8 + y, (7 - z if y % 2 else z) * 8 + y) for z in range(8) for y in range(8)]
NT = (((1,), (1,)), ((), ()))
TN = (((0,), (0,)), ((), ()))
VMEM = pl.BlockSpec(memory_space=pltpu.VMEM)
SMEM = pl.BlockSpec(memory_space=pltpu.SMEM)
PARAMS = pltpu.CompilerParams(vmem_limit_bytes=56 * 1024 * 1024)


def copies_from(shard, axis):
    copies = jnp.broadcast_to(shard, (lax.axis_size(axis), *shard.shape))
    return lax.all_to_all(copies, axis, split_axis=0, concat_axis=0, tiled=True)


def swapped_cores(value):
    return lax.ppermute(value, "c", [(0, 1), (1, 0)])


def three_parts(values):
    high = lax.reduce_precision(values, 8, 7)
    rest = values - high
    middle = lax.reduce_precision(rest, 8, 7)
    low = lax.reduce_precision(rest - middle, 8, 7)
    return [part.astype(BF16) for part in (high, middle, low)]


def project_kernel(rows, weights, own_out, oth_out):
    product = jnp.dot(rows[...], weights[...], preferred_element_type=F32)
    own_out[...] = product[:SPAN]
    oth_out[...] = product[SPAN:]


def share_kernel(first_part, second_part, q_out, kv_out):
    query = first_part[:, :192] + second_part[:, :192]
    q_out[192:] = jnp.zeros((HEAD, SPAN), BF16)
    q_out[:192] = jnp.transpose(query * (HEAD ** (-0.5) * LOG2E)).astype(BF16)
    both = first_part[:, 192:320] + second_part[:, 192:320]
    flipped = jnp.transpose(both)[HEAD:, :].astype(BF16)
    kv_out[:128] = jnp.concatenate([both[:128, :HEAD], both[128:, :HEAD]], axis=1).astype(BF16)
    kv_out[128:] = jnp.concatenate([flipped[:, :128], flipped[:, 128:]], axis=0)


def turned(proj, at, cos, sin):
    first = proj[:, at : at + 32]
    second = proj[:, at + 32 : at + 64]
    return jnp.concatenate([first * cos - second * sin, first * sin + second * cos], axis=1)


def front_kernel(first_part, second_part, cosine, sine, decay, state_out, proj):
    proj[...] = first_part[:, 512:] + second_part[:, 512:]
    cos = cosine[...]
    sin = sine[...]
    for h in range(3):
        key = turned(proj, h * HEAD, cos, sin).astype(BF16)
        value = proj[:, 192 + h * HEAD : 192 + (h + 1) * HEAD].astype(BF16)
        column = decay[:, h : h + 1]
        last = decay[SPAN - 1 : SPAN, h : h + 1]
        faded = (key.astype(F32) * jnp.exp(last - column)).astype(BF16)
        update = lax.dot_general(faded, value, TN, preferred_element_type=F32).astype(BF16)
        state_out[32 * h : 32 * (h + 1)] = jnp.concatenate([update[:32], update[32:]], axis=1)


def spread_kernel(pairs, states, out):
    for y in range(8):
        out[y, :SPAN] = pairs[...]
        out[y, SPAN:] = states[...]


def local_kernel(
    first_part, second_part, cosine, sine, decay, decay_row, local_out, lifted_out, proj
):
    proj[...] = first_part[...] + second_part[...]
    cos = cosine[...]
    sin = sine[...]
    place = lax.broadcasted_iota(jnp.int32, (SPAN, SPAN), 0)
    other = lax.broadcasted_iota(jnp.int32, (SPAN, SPAN), 1)
    causal = place >= other
    for h in range(3):
        query = (turned(proj, 320 + h * HEAD, cos, sin) * HEAD ** (-0.5)).astype(BF16)
        key = turned(proj, 512 + h * HEAD, cos, sin).astype(BF16)
        value = proj[:, 704 + h * HEAD : 704 + (h + 1) * HEAD].astype(BF16)
        column = decay[:, h : h + 1]
        scores = lax.dot_general(query, key, NT, preferred_element_type=F32)
        gap = jnp.where(causal, column - decay_row[h : h + 1, :], 0.0)
        weights = jnp.where(causal, scores * jnp.exp(gap), 0.0).astype(BF16)
        local_out[:, h * HEAD : (h + 1) * HEAD] = jnp.dot(
            weights, value, preferred_element_type=F32
        )
        lifted_out[:, h * HEAD : (h + 1) * HEAD] = (
            query.astype(F32) * jnp.exp(column)
        ).astype(BF16)


def attend_kernel(
    plan,
    fade,
    received,
    query_gate,
    kv_own,
    kv_oth,
    key_gate,
    out,
    keys,
    values,
    queries,
    total,
    even,
    odd,
):
    extra = lax.broadcasted_iota(jnp.int32, (16, 2 * SPAN), 0)
    ones = jnp.where(extra == 0, 1.0, 0.0).astype(BF16)
    for y in range(8):
        for side, held in enumerate((kv_own, kv_oth)):
            packed = held[y, :128]
            at = side * SPAN
            keys[y, at : at + 128, :HEAD] = packed[:, :HEAD]
            keys[y, at + 128 : at + SPAN, :HEAD] = packed[:, HEAD:]
            keys[y, at : at + SPAN, HEAD:] = key_gate[side, y]
            values[y, :HEAD, at : at + 128] = held[y, 128:192]
            values[y, :HEAD, at + 128 : at + SPAN] = held[y, 192:SPAN]
        values[y, HEAD:, :] = ones
    for z in range(8):
        for h in range(3):
            queries[z, h, :HEAD] = received[z, h * HEAD : (h + 1) * HEAD]
            queries[z, h, HEAD:] = query_gate[z, h]
    total[...] = jnp.zeros_like(total)

    place = lax.broadcasted_iota(jnp.int32, (2 * SPAN, SPAN), 0)
    wanted = lax.broadcasted_iota(jnp.int32, (2 * SPAN, SPAN), 1)
    allowed = place <= jnp.where(place < SPAN, wanted, plan[66] * (4 * SPAN) - 1)

    def weigh(i, held, h):
        z, y = (plan[i] // 8, plan[i] % 8)
        at = h * SPAN
        total[z, :, at : at + SPAN] += jnp.dot(
            values[y], held[:, at : at + SPAN], preferred_element_type=F32
        )

    def score(i, held, h, mask=None):
        z, y = (plan[i] // 8, plan[i] % 8)
        for at in (0, SPAN):
            weights = jnp.exp2(
                jnp.dot(keys[y, at : at + SPAN], queries[z, h], preferred_element_type=F32)
            )
            if mask is not None:
                weights = jnp.where(mask[at : at + SPAN], weights, 0.0)
            held[at : at + SPAN, h * SPAN : (h + 1) * SPAN] = weights.astype(BF16)

    for h in range(3):
        score(0, even, h, allowed)

    def advance(first):
        for h in range(3):
            score(first + 1, odd, h)
            weigh(first, even, h)
        for h in range(3):
            score(first + 2, even, h)
            weigh(first + 1, odd, h)

    def four(i, carry):
        advance(4 * i)
        advance(4 * i + 2)
        return carry

    count = plan[65]
    lax.fori_loop(0, count // 4, four, 0)

    @pl.when(count % 4 >= 2)
    def _():
        advance(count // 4 * 4)

    @pl.when(count % 2 == 1)
    def _():
        for h in range(3):
            weigh(count - 1, even, h)

    for z in range(8):
        rows = []
        for h in range(3):
            out[z, h * HEAD : (h + 1) * HEAD] = total[z, :HEAD, h * SPAN : (h + 1) * SPAN].astype(
                BF16
            )
            rows.append(total[z, HEAD : HEAD + 1, h * SPAN : (h + 1) * SPAN])
        high = [row.astype(BF16).astype(F32) for row in rows]
        low = [row - big for row, big in zip(rows, high)]
        out[z, 192:208] = jnp.concatenate(
            high + low + [jnp.zeros((10, SPAN), F32)], axis=0
        ).astype(BF16)

    leaving = []
    here = []
    for h in range(3):
        at = SPAN + 32 * h
        left = jnp.zeros((32, 128), F32)
        kept = jnp.zeros((32, 128), F32)
        for side, held in enumerate((kv_own, kv_oth)):
            for y in range(8):
                state = held[y, at : at + 32].astype(F32)
                place = (side * 8 + y) * 3 + h
                left = left + state * fade[place]
                kept = kept + state * fade[48 + place]
        leaving.append(left)
        here.append(kept)

    def put(z, states):
        states = jnp.concatenate(states, axis=0).astype(BF16)
        out[z, 208:, :128] = states[:48]
        out[z, 208:, 128:] = states[48:]

    for z in range(8):
        put(
            z,
            [
                jnp.where(z > plan[67], leaving[h] * fade[96 + z * 3 + h], 0.0)
                for h in range(3)
            ],
        )
    put(plan[67], here)


def back_kernel(parts, local, lifted, w_out, out, mixed):
    @pl.when(pl.program_id(0) == 0)
    def _():
        total = parts[0].astype(F32)
        for z in range(1, 8):
            total = total + parts[z].astype(F32)
        states = jnp.concatenate([total[208:, :128], total[208:, 128:]], axis=0)
        for h in range(3):
            held = states[32 * h : 32 * (h + 1)]
            held = jnp.concatenate([held[:, :HEAD], held[:, HEAD:]], axis=0).astype(BF16)
            raw = local[:, h * HEAD : (h + 1) * HEAD] + jnp.dot(
                lifted[:, h * HEAD : (h + 1) * HEAD], held, preferred_element_type=F32
            )
            centred = raw - jnp.mean(raw, axis=-1, keepdims=True)
            spread = jnp.mean(centred * centred, axis=-1, keepdims=True)
            mixed[:, h * HEAD : (h + 1) * HEAD] = (centred * lax.rsqrt(spread + EPS)).astype(BF16)
            weight = total[192 + h : 193 + h] + total[195 + h : 196 + h]
            attended = total[h * HEAD : (h + 1) * HEAD] / weight
            mixed[:, 192 + h * HEAD : 192 + (h + 1) * HEAD] = jnp.transpose(attended).astype(BF16)

    out[...] = lax.dot_general(
        mixed[...], w_out[...], NT, preferred_element_type=F32
    ).astype(BF16)


def body(
    tokens,
    pre_gain,
    w_query_ret,
    w_key_ret,
    w_value_ret,
    w_query_att,
    w_key_att,
    w_value_att,
    w_out_ret,
    w_out_att,
    retain_log,
    forget_total,
):
    z, y, c = (lax.axis_index("z"), lax.axis_index("y"), lax.axis_index("c"))
    ends = jnp.concatenate(three_parts(jnp.sum(retain_log, axis=0)))
    shard = jnp.concatenate(
        [
            w_query_att,
            w_key_att,
            w_value_att,
            w_query_ret,
            w_key_ret,
            w_value_ret,
            w_out_ret.T,
            w_out_att.T,
            jnp.pad(ends[None, :], ((0, 15), (0, 119))),
        ],
        axis=1,
    )
    w_row = copies_from(shard, "y")
    line_ends = jnp.sum(w_row[:, 0, 1280:1289].reshape(8, 3, 3).astype(F32), axis=1)
    w_row = w_row[:, :, :1280].reshape(128, 1280)
    w_own = lax.all_gather(w_row, "z", axis=0, tiled=True)

    raw = tokens.astype(F32)
    normed = (
        raw * lax.rsqrt(jnp.mean(raw * raw, axis=-1, keepdims=True) + EPS) * pre_gain
    ).astype(BF16)
    halves = jnp.transpose(normed.reshape(64, 64, 2, 16), (2, 0, 1, 3)).reshape(2, 64, 1024)
    rows = copies_from(halves, "tp")
    kept = jnp.where(c == 0, rows[:, 0], rows[:, 1]).reshape(SPAN, 1024)
    sent = jnp.where(c == 0, rows[:, 1], rows[:, 0]).reshape(SPAN, 1024)
    came = swapped_cores(sent)
    rows = jnp.concatenate([kept, came], axis=0)

    here = z * 16 + y * 2 + c
    positions = (here * SPAN + jnp.arange(SPAN, dtype=jnp.int32)).astype(F32)
    inverse = THETA ** (-jnp.arange(32, dtype=F32) / 32)
    angles = positions[:, None] * inverse[None, :]
    cosine, sine = (jnp.cos(angles), jnp.sin(angles))
    decay = jnp.cumsum(retain_log, axis=0)
    decay_row = jnp.pad(decay.T, ((0, 5), (0, 0)))
    ends_own = copies_from(line_ends, "z")
    ends_oth = swapped_cores(ends_own)
    ends = jnp.where(
        c == 0,
        jnp.stack([ends_own, ends_oth], axis=2),
        jnp.stack([ends_oth, ends_own], axis=2),
    ).reshape(128, 3)

    gate = (forget_total * LOG2E).reshape(3, 8, 8, 2, SPAN)
    spans = jnp.arange(8, dtype=jnp.int32)
    key_z = jnp.where(spans % 2 == 0, z, 7 - z)
    chosen = (spans[:, None] == key_z[None, :])[None, :, :, None, None]
    key_side = jnp.sum(jnp.where(chosen, gate, 0.0), axis=1)
    key_side = jnp.where(c == 0, key_side, key_side[:, :, ::-1])
    minus = jnp.stack(three_parts(-key_side), axis=1).reshape(9, 8, 2, SPAN)
    key_gate = jnp.concatenate(
        [minus, jnp.ones((3, 8, 2, SPAN), BF16), jnp.zeros((52, 8, 2, SPAN), BF16)], axis=0
    )
    key_gate = jnp.transpose(key_gate, (2, 1, 3, 0))
    mine = lax.dynamic_index_in_dim(
        lax.dynamic_index_in_dim(gate, y, 2, keepdims=False), c, 2, keepdims=False
    )
    plus = jnp.transpose(jnp.stack(three_parts(mine), axis=0), (2, 1, 0, 3))
    own_head = (
        jnp.arange(9, dtype=jnp.int32)[None, :] // 3 == jnp.arange(3, dtype=jnp.int32)[:, None]
    ).astype(BF16)
    query_gate = jnp.concatenate(
        [
            jnp.broadcast_to(own_head[None, :, :, None], (8, 3, 9, SPAN)),
            plus,
            jnp.zeros((8, 3, 52, SPAN), BF16),
        ],
        axis=2,
    )
    first = z * 16 + spans * 2
    blocks = jnp.stack([first + c, first + 1 - c])
    targets = spans * 16 + y * 2 + c
    index = jnp.arange(128, dtype=jnp.int32)
    plane_end = z * 16 + 15

    def faded(chosen, valid):
        total = jnp.sum(jnp.where(chosen[..., None], ends, 0.0), axis=-2)
        return jnp.where(valid[..., None], jnp.exp(total), 0.0).reshape(-1)

    after = index > blocks[..., None]
    fade = jnp.concatenate(
        [
            faded(after & (index <= plane_end), blocks >= 0),
            faded(after & (index < here), blocks < here),
            faded((index > plane_end) & (index < targets[:, None]), spans > z),
        ]
    )
    needed = (
        (key_z[None, :] < spans[:, None])
        | ((key_z[None, :] == spans[:, None]) & (spans[None, :] < y))
    ).reshape(64)
    slot = jnp.cumsum(needed.astype(jnp.int32)) - 1
    order = jnp.arange(64, dtype=jnp.int32)
    units = jnp.sum(
        jnp.where(needed[None, :] & (slot[None, :] == order[:, None]), order[None, :], 0), axis=1
    )
    own = jnp.stack([jnp.where(y % 2 == 0, z, 7 - z) * 8 + y])
    plan = jnp.concatenate([own, units, jnp.stack([jnp.sum(needed.astype(jnp.int32)) + 1, c, z])])

    own_part, oth_part = pl.pallas_call(
        project_kernel,
        grid=(1,),
        in_specs=[VMEM, pl.BlockSpec((1024, 896), lambda i: (0, 0))],
        out_specs=[VMEM] * 2,
        out_shape=[jax.ShapeDtypeStruct((SPAN, 896), F32)] * 2,
        compiler_params=PARAMS,
        name="project",
    )(rows, w_own)
    came_part = swapped_cores(oth_part)
    attention_part = pl.BlockSpec((SPAN, 384), lambda i: (0, 0))
    q_send, kv_send = pl.pallas_call(
        share_kernel,
        grid=(1,),
        in_specs=[attention_part] * 2,
        out_specs=[VMEM] * 2,
        out_shape=[
            jax.ShapeDtypeStruct((SPAN, SPAN), BF16),
            jax.ShapeDtypeStruct((SPAN, 128), BF16),
        ],
        compiler_params=PARAMS,
        name="share",
    )(own_part, came_part)
    queries = lax.all_gather(q_send, "z", axis=0)
    kv_send = lax.ppermute(kv_send, ("z", "y"), MIRROR)
    state_send = pl.pallas_call(
        front_kernel,
        in_specs=[VMEM] * 5,
        out_specs=VMEM,
        out_shape=jax.ShapeDtypeStruct((96, 128), BF16),
        scratch_shapes=[pltpu.VMEM((SPAN, 384), F32)],
        compiler_params=PARAMS,
        name="front",
    )(own_part, came_part, cosine, sine, decay)
    kv_send = pl.pallas_call(
        spread_kernel,
        in_specs=[VMEM] * 2,
        out_specs=VMEM,
        out_shape=jax.ShapeDtypeStruct((8, SPAN + 96, 128), BF16),
        compiler_params=PARAMS,
        name="spread",
    )(kv_send, state_send)
    kv_own = lax.all_to_all(kv_send, "y", 0, 0, tiled=True)
    kv_oth = swapped_cores(kv_own)
    local, lifted = pl.pallas_call(
        local_kernel,
        in_specs=[VMEM] * 6,
        out_specs=[VMEM] * 2,
        out_shape=[jax.ShapeDtypeStruct((SPAN, 192), F32), jax.ShapeDtypeStruct((SPAN, 192), BF16)],
        scratch_shapes=[pltpu.VMEM((SPAN, 896), F32)],
        compiler_params=PARAMS,
        name="local",
    )(own_part, came_part, cosine, sine, decay, decay_row)
    out_own = w_own[:, 896:1280]
    out_oth = swapped_cores(out_own).reshape(64, 16, 384)
    out_own = out_own.reshape(64, 16, 384)
    w_out = jnp.where(
        c == 0, jnp.stack([out_own, out_oth], axis=1), jnp.stack([out_oth, out_own], axis=1)
    ).reshape(2048, 384)

    partial = pl.pallas_call(
        attend_kernel,
        in_specs=[SMEM] * 2 + [VMEM] * 5,
        out_specs=VMEM,
        out_shape=jax.ShapeDtypeStruct((8, SPAN, SPAN), BF16),
        scratch_shapes=[
            pltpu.VMEM((8, 2 * SPAN, 128), BF16),
            pltpu.VMEM((8, 80, 2 * SPAN), BF16),
            pltpu.VMEM((8, 3, 128, SPAN), BF16),
            pltpu.VMEM((8, 80, 3 * SPAN), F32),
            pltpu.VMEM((2 * SPAN, 3 * SPAN), BF16),
            pltpu.VMEM((2 * SPAN, 3 * SPAN), BF16),
        ],
        compiler_params=PARAMS,
        name="attend",
    )(plan, fade, queries, query_gate, kv_own, kv_oth, key_gate)
    parts = lax.all_to_all(partial, "z", 0, 0, tiled=True)

    share = pl.pallas_call(
        back_kernel,
        grid=(2,),
        in_specs=[VMEM] * 3 + [pl.BlockSpec((1024, 384), lambda i: (i, 0))],
        out_specs=pl.BlockSpec((SPAN, 1024), lambda i: (0, i)),
        out_shape=jax.ShapeDtypeStruct((SPAN, 2048), BF16),
        scratch_shapes=[pltpu.VMEM((SPAN, 384), BF16)],
        compiler_params=PARAMS,
        name="back",
    )(parts, local, lifted, w_out)
    shares = lax.all_to_all(share.reshape(4, 64, 2048), "tp", 0, 0, tiled=True)
    return jnp.sum(shares.astype(F32), axis=0).astype(BF16)


def solution(mesh):
    finer = Mesh(mesh.devices.reshape(8, 8, 2, mesh.shape["tp"]), ("z", "y", "c", "tp"))
    everyone = ("z", "y", "c", "tp")
    placed = (
        P(everyone, None),
        P(),
        P(SP, "tp"),
        P(SP, "tp"),
        P(SP, "tp"),
        P(SP, "tp"),
        P(SP, "tp"),
        P(SP, "tp"),
        P("tp", SP),
        P("tp", SP),
        P(SP, "tp"),
        P("tp", None),
    )
    return jax.shard_map(
        body, mesh=finer, in_specs=placed, out_specs=P(everyone, None), check_vma=False
    )
```

```python
import jax
import jax.numpy as jnp
from jax import lax
from jax.experimental import pallas as pl
from jax.experimental.pallas import tpu as pltpu
from jax.sharding import Mesh
from jax.sharding import PartitionSpec as P

HEAD = 64
SPAN = 256
SP = ("z", "y", "c")
EPS = 1e-06
THETA = 10000.0
LOG2E = 1.4426950408889634
F32 = jnp.float32
BF16 = jnp.bfloat16
MIRROR = [(z * 8 + y, (7 - z if y % 2 else z) * 8 + y) for z in range(8) for y in range(8)]
NT = (((1,), (1,)), ((), ()))
TN = (((0,), (0,)), ((), ()))
VMEM = pl.BlockSpec(memory_space=pltpu.VMEM)
SMEM = pl.BlockSpec(memory_space=pltpu.SMEM)
PARAMS = pltpu.CompilerParams(vmem_limit_bytes=56 * 1024 * 1024)


def copies_from(shard, axis):
    copies = jnp.broadcast_to(shard, (lax.axis_size(axis), *shard.shape))
    return lax.all_to_all(copies, axis, split_axis=0, concat_axis=0, tiled=True)


def swapped_cores(value):
    return lax.ppermute(value, "c", [(0, 1), (1, 0)])


def three_parts(values):
    high = lax.reduce_precision(values, 8, 7)
    rest = values - high
    middle = lax.reduce_precision(rest, 8, 7)
    low = lax.reduce_precision(rest - middle, 8, 7)
    return [part.astype(BF16) for part in (high, middle, low)]


def project_kernel(rows, weights, own_out, oth_out):
    product = jnp.dot(rows[...], weights[...], preferred_element_type=F32)
    own_out[...] = product[:SPAN]
    oth_out[...] = product[SPAN:]


def share_kernel(first_part, second_part, q_out, kv_out):
    query = first_part[:, :192] + second_part[:, :192]
    q_out[192:] = jnp.zeros((HEAD, SPAN), BF16)
    q_out[:192] = jnp.transpose(query * (HEAD ** (-0.5) * LOG2E)).astype(BF16)
    both = first_part[:, 192:320] + second_part[:, 192:320]
    flipped = jnp.transpose(both)[HEAD:, :].astype(BF16)
    kv_out[:128] = jnp.concatenate([both[:128, :HEAD], both[128:, :HEAD]], axis=1).astype(BF16)
    kv_out[128:] = jnp.concatenate([flipped[:, :128], flipped[:, 128:]], axis=0)


def turned(proj, at, cos, sin):
    first = proj[:, at : at + 32]
    second = proj[:, at + 32 : at + 64]
    return jnp.concatenate([first * cos - second * sin, first * sin + second * cos], axis=1)


def front_kernel(first_part, second_part, cosine, sine, decay, state_out, proj):
    proj[...] = first_part[:, 512:] + second_part[:, 512:]
    cos = cosine[...]
    sin = sine[...]
    for h in range(3):
        key = turned(proj, h * HEAD, cos, sin).astype(BF16)
        value = proj[:, 192 + h * HEAD : 192 + (h + 1) * HEAD].astype(BF16)
        column = decay[:, h : h + 1]
        last = decay[SPAN - 1 : SPAN, h : h + 1]
        faded = (key.astype(F32) * jnp.exp(last - column)).astype(BF16)
        update = lax.dot_general(faded, value, TN, preferred_element_type=F32).astype(BF16)
        state_out[32 * h : 32 * (h + 1)] = jnp.concatenate([update[:32], update[32:]], axis=1)


def spread_kernel(pairs, states, out):
    for y in range(8):
        out[y, :SPAN] = pairs[...]
        out[y, SPAN:] = states[...]


def local_kernel(
    first_part, second_part, cosine, sine, decay, decay_row, local_out, lifted_out, proj
):
    proj[...] = first_part[...] + second_part[...]
    cos = cosine[...]
    sin = sine[...]
    place = lax.broadcasted_iota(jnp.int32, (SPAN, SPAN), 0)
    other = lax.broadcasted_iota(jnp.int32, (SPAN, SPAN), 1)
    causal = place >= other
    for h in range(3):
        query = (turned(proj, 320 + h * HEAD, cos, sin) * HEAD ** (-0.5)).astype(BF16)
        key = turned(proj, 512 + h * HEAD, cos, sin).astype(BF16)
        value = proj[:, 704 + h * HEAD : 704 + (h + 1) * HEAD].astype(BF16)
        column = decay[:, h : h + 1]
        scores = lax.dot_general(query, key, NT, preferred_element_type=F32)
        gap = jnp.where(causal, column - decay_row[h : h + 1, :], 0.0)
        weights = jnp.where(causal, scores * jnp.exp(gap), 0.0).astype(BF16)
        local_out[:, h * HEAD : (h + 1) * HEAD] = jnp.dot(
            weights, value, preferred_element_type=F32
        )
        lifted_out[:, h * HEAD : (h + 1) * HEAD] = (
            query.astype(F32) * jnp.exp(column)
        ).astype(BF16)


def attend_kernel(
    plan,
    fade,
    received,
    query_gate,
    kv_own,
    kv_oth,
    key_gate,
    out,
    keys,
    values,
    queries,
    total,
    even,
    odd,
):
    extra = lax.broadcasted_iota(jnp.int32, (16, 2 * SPAN), 0)
    ones = jnp.where(extra == 0, 1.0, 0.0).astype(BF16)
    for y in range(8):
        for side, held in enumerate((kv_own, kv_oth)):
            packed = held[y, :128]
            at = side * SPAN
            keys[y, at : at + 128, :HEAD] = packed[:, :HEAD]
            keys[y, at + 128 : at + SPAN, :HEAD] = packed[:, HEAD:]
            keys[y, at : at + SPAN, HEAD:] = key_gate[side, y]
            values[y, :HEAD, at : at + 128] = held[y, 128:192]
            values[y, :HEAD, at + 128 : at + SPAN] = held[y, 192:SPAN]
        values[y, HEAD:, :] = ones
    for z in range(8):
        for h in range(3):
            queries[z, h, :HEAD] = received[z, h * HEAD : (h + 1) * HEAD]
            queries[z, h, HEAD:] = query_gate[z, h]
    total[...] = jnp.zeros_like(total)

    place = lax.broadcasted_iota(jnp.int32, (2 * SPAN, SPAN), 0)
    wanted = lax.broadcasted_iota(jnp.int32, (2 * SPAN, SPAN), 1)
    allowed = place <= jnp.where(place < SPAN, wanted, plan[66] * (4 * SPAN) - 1)

    def weigh(i, held, h):
        z, y = (plan[i] // 8, plan[i] % 8)
        at = h * SPAN
        total[z, :, at : at + SPAN] += jnp.dot(
            values[y], held[:, at : at + SPAN], preferred_element_type=F32
        )

    def score(i, held, h, mask=None):
        z, y = (plan[i] // 8, plan[i] % 8)
        for at in (0, SPAN):
            weights = jnp.exp2(
                jnp.dot(keys[y, at : at + SPAN], queries[z, h], preferred_element_type=F32)
            )
            if mask is not None:
                weights = jnp.where(mask[at : at + SPAN], weights, 0.0)
            held[at : at + SPAN, h * SPAN : (h + 1) * SPAN] = weights.astype(BF16)

    for h in range(3):
        score(0, even, h, allowed)

    def advance(first):
        for h in range(3):
            score(first + 1, odd, h)
            weigh(first, even, h)
        for h in range(3):
            score(first + 2, even, h)
            weigh(first + 1, odd, h)

    def eight(i, carry):
        for k in range(0, 8, 2):
            advance(8 * i + k)
        return carry

    count = plan[65]
    lax.fori_loop(0, count // 8, eight, 0)

    @pl.when(count % 8 >= 4)
    def _():
        advance(count // 8 * 8)
        advance(count // 8 * 8 + 2)

    @pl.when(count % 4 >= 2)
    def _():
        advance(count // 4 * 4)

    @pl.when(count % 2 == 1)
    def _():
        for h in range(3):
            weigh(count - 1, even, h)

    for z in range(8):
        rows = []
        for h in range(3):
            out[z, h * HEAD : (h + 1) * HEAD] = total[z, :HEAD, h * SPAN : (h + 1) * SPAN].astype(
                BF16
            )
            rows.append(total[z, HEAD : HEAD + 1, h * SPAN : (h + 1) * SPAN])
        high = [row.astype(BF16).astype(F32) for row in rows]
        low = [row - big for row, big in zip(rows, high)]
        out[z, 192:208] = jnp.concatenate(
            high + low + [jnp.zeros((10, SPAN), F32)], axis=0
        ).astype(BF16)

    leaving = []
    here = []
    for h in range(3):
        at = SPAN + 32 * h
        left = jnp.zeros((32, 128), F32)
        kept = jnp.zeros((32, 128), F32)
        for side, held in enumerate((kv_own, kv_oth)):
            for y in range(8):
                state = held[y, at : at + 32].astype(F32)
                place = (side * 8 + y) * 3 + h
                left = left + state * fade[place]
                kept = kept + state * fade[48 + place]
        leaving.append(left)
        here.append(kept)

    def put(z, states):
        states = jnp.concatenate(states, axis=0).astype(BF16)
        out[z, 208:, :128] = states[:48]
        out[z, 208:, 128:] = states[48:]

    for z in range(8):
        put(
            z,
            [
                jnp.where(z > plan[67], leaving[h] * fade[96 + z * 3 + h], 0.0)
                for h in range(3)
            ],
        )
    put(plan[67], here)


def back_kernel(parts, local, lifted, w_out, out, mixed):
    @pl.when(pl.program_id(0) == 0)
    def _():
        total = parts[0].astype(F32)
        for z in range(1, 8):
            total = total + parts[z].astype(F32)
        states = jnp.concatenate([total[208:, :128], total[208:, 128:]], axis=0)
        for h in range(3):
            held = states[32 * h : 32 * (h + 1)]
            held = jnp.concatenate([held[:, :HEAD], held[:, HEAD:]], axis=0).astype(BF16)
            raw = local[:, h * HEAD : (h + 1) * HEAD] + jnp.dot(
                lifted[:, h * HEAD : (h + 1) * HEAD], held, preferred_element_type=F32
            )
            centred = raw - jnp.mean(raw, axis=-1, keepdims=True)
            spread = jnp.mean(centred * centred, axis=-1, keepdims=True)
            mixed[:, h * HEAD : (h + 1) * HEAD] = (centred * lax.rsqrt(spread + EPS)).astype(BF16)
            weight = total[192 + h : 193 + h] + total[195 + h : 196 + h]
            attended = total[h * HEAD : (h + 1) * HEAD] / weight
            mixed[:, 192 + h * HEAD : 192 + (h + 1) * HEAD] = jnp.transpose(attended).astype(BF16)

    out[...] = lax.dot_general(
        mixed[...], w_out[...], NT, preferred_element_type=F32
    ).astype(BF16)


def body(
    tokens,
    pre_gain,
    w_query_ret,
    w_key_ret,
    w_value_ret,
    w_query_att,
    w_key_att,
    w_value_att,
    w_out_ret,
    w_out_att,
    retain_log,
    forget_total,
):
    z, y, c = (lax.axis_index("z"), lax.axis_index("y"), lax.axis_index("c"))
    ends = jnp.concatenate(three_parts(jnp.sum(retain_log, axis=0)))
    shard = jnp.concatenate(
        [
            w_query_att,
            w_key_att,
            w_value_att,
            w_query_ret,
            w_key_ret,
            w_value_ret,
            w_out_ret.T,
            w_out_att.T,
            jnp.pad(ends[None, :], ((0, 15), (0, 119))),
        ],
        axis=1,
    )
    w_row = copies_from(shard, "y")
    line_ends = jnp.sum(w_row[:, 0, 1280:1289].reshape(8, 3, 3).astype(F32), axis=1)
    w_row = w_row[:, :, :1280].reshape(128, 1280)
    w_own = lax.all_gather(w_row, "z", axis=0, tiled=True)

    raw = tokens.astype(F32)
    normed = (
        raw * lax.rsqrt(jnp.mean(raw * raw, axis=-1, keepdims=True) + EPS) * pre_gain
    ).astype(BF16)
    halves = jnp.transpose(normed.reshape(64, 64, 2, 16), (2, 0, 1, 3)).reshape(2, 64, 1024)
    rows = copies_from(halves, "tp")
    kept = jnp.where(c == 0, rows[:, 0], rows[:, 1]).reshape(SPAN, 1024)
    sent = jnp.where(c == 0, rows[:, 1], rows[:, 0]).reshape(SPAN, 1024)
    came = swapped_cores(sent)
    rows = jnp.concatenate([kept, came], axis=0)

    here = z * 16 + y * 2 + c
    positions = (here * SPAN + jnp.arange(SPAN, dtype=jnp.int32)).astype(F32)
    inverse = THETA ** (-jnp.arange(32, dtype=F32) / 32)
    angles = positions[:, None] * inverse[None, :]
    cosine, sine = (jnp.cos(angles), jnp.sin(angles))
    decay = jnp.cumsum(retain_log, axis=0)
    decay_row = jnp.pad(decay.T, ((0, 5), (0, 0)))
    ends_own = copies_from(line_ends, "z")
    ends_oth = swapped_cores(ends_own)
    ends = jnp.where(
        c == 0,
        jnp.stack([ends_own, ends_oth], axis=2),
        jnp.stack([ends_oth, ends_own], axis=2),
    ).reshape(128, 3)

    gate = (forget_total * LOG2E).reshape(3, 8, 8, 2, SPAN)
    spans = jnp.arange(8, dtype=jnp.int32)
    key_z = jnp.where(spans % 2 == 0, z, 7 - z)
    chosen = (spans[:, None] == key_z[None, :])[None, :, :, None, None]
    key_side = jnp.sum(jnp.where(chosen, gate, 0.0), axis=1)
    key_side = jnp.where(c == 0, key_side, key_side[:, :, ::-1])
    minus = jnp.stack(three_parts(-key_side), axis=1).reshape(9, 8, 2, SPAN)
    key_gate = jnp.concatenate(
        [minus, jnp.ones((3, 8, 2, SPAN), BF16), jnp.zeros((52, 8, 2, SPAN), BF16)], axis=0
    )
    key_gate = jnp.transpose(key_gate, (2, 1, 3, 0))
    mine = lax.dynamic_index_in_dim(
        lax.dynamic_index_in_dim(gate, y, 2, keepdims=False), c, 2, keepdims=False
    )
    plus = jnp.transpose(jnp.stack(three_parts(mine), axis=0), (2, 1, 0, 3))
    own_head = (
        jnp.arange(9, dtype=jnp.int32)[None, :] // 3 == jnp.arange(3, dtype=jnp.int32)[:, None]
    ).astype(BF16)
    query_gate = jnp.concatenate(
        [
            jnp.broadcast_to(own_head[None, :, :, None], (8, 3, 9, SPAN)),
            plus,
            jnp.zeros((8, 3, 52, SPAN), BF16),
        ],
        axis=2,
    )
    first = z * 16 + spans * 2
    blocks = jnp.stack([first + c, first + 1 - c])
    targets = spans * 16 + y * 2 + c
    index = jnp.arange(128, dtype=jnp.int32)
    plane_end = z * 16 + 15

    def faded(chosen, valid):
        total = jnp.sum(jnp.where(chosen[..., None], ends, 0.0), axis=-2)
        return jnp.where(valid[..., None], jnp.exp(total), 0.0).reshape(-1)

    after = index > blocks[..., None]
    fade = jnp.concatenate(
        [
            faded(after & (index <= plane_end), blocks >= 0),
            faded(after & (index < here), blocks < here),
            faded((index > plane_end) & (index < targets[:, None]), spans > z),
        ]
    )
    needed = (
        (key_z[None, :] < spans[:, None])
        | ((key_z[None, :] == spans[:, None]) & (spans[None, :] < y))
    ).reshape(64)
    slot = jnp.cumsum(needed.astype(jnp.int32)) - 1
    order = jnp.arange(64, dtype=jnp.int32)
    units = jnp.sum(
        jnp.where(needed[None, :] & (slot[None, :] == order[:, None]), order[None, :], 0), axis=1
    )
    own = jnp.stack([jnp.where(y % 2 == 0, z, 7 - z) * 8 + y])
    plan = jnp.concatenate([own, units, jnp.stack([jnp.sum(needed.astype(jnp.int32)) + 1, c, z])])

    own_part, oth_part = pl.pallas_call(
        project_kernel,
        grid=(1,),
        in_specs=[VMEM, pl.BlockSpec((1024, 896), lambda i: (0, 0))],
        out_specs=[VMEM] * 2,
        out_shape=[jax.ShapeDtypeStruct((SPAN, 896), F32)] * 2,
        compiler_params=PARAMS,
        name="project",
    )(rows, w_own)
    came_part = swapped_cores(oth_part)
    attention_part = pl.BlockSpec((SPAN, 384), lambda i: (0, 0))
    q_send, kv_send = pl.pallas_call(
        share_kernel,
        grid=(1,),
        in_specs=[attention_part] * 2,
        out_specs=[VMEM] * 2,
        out_shape=[
            jax.ShapeDtypeStruct((SPAN, SPAN), BF16),
            jax.ShapeDtypeStruct((SPAN, 128), BF16),
        ],
        compiler_params=PARAMS,
        name="share",
    )(own_part, came_part)
    queries = lax.all_gather(q_send, "z", axis=0)
    kv_send = lax.ppermute(kv_send, ("z", "y"), MIRROR)
    state_send = pl.pallas_call(
        front_kernel,
        in_specs=[VMEM] * 5,
        out_specs=VMEM,
        out_shape=jax.ShapeDtypeStruct((96, 128), BF16),
        scratch_shapes=[pltpu.VMEM((SPAN, 384), F32)],
        compiler_params=PARAMS,
        name="front",
    )(own_part, came_part, cosine, sine, decay)
    kv_send = pl.pallas_call(
        spread_kernel,
        in_specs=[VMEM] * 2,
        out_specs=VMEM,
        out_shape=jax.ShapeDtypeStruct((8, SPAN + 96, 128), BF16),
        compiler_params=PARAMS,
        name="spread",
    )(kv_send, state_send)
    kv_own = lax.all_to_all(kv_send, "y", 0, 0, tiled=True)
    kv_oth = swapped_cores(kv_own)
    local, lifted = pl.pallas_call(
        local_kernel,
        in_specs=[VMEM] * 6,
        out_specs=[VMEM] * 2,
        out_shape=[jax.ShapeDtypeStruct((SPAN, 192), F32), jax.ShapeDtypeStruct((SPAN, 192), BF16)],
        scratch_shapes=[pltpu.VMEM((SPAN, 896), F32)],
        compiler_params=PARAMS,
        name="local",
    )(own_part, came_part, cosine, sine, decay, decay_row)
    out_own = w_own[:, 896:1280]
    out_oth = swapped_cores(out_own).reshape(64, 16, 384)
    out_own = out_own.reshape(64, 16, 384)
    w_out = jnp.where(
        c == 0, jnp.stack([out_own, out_oth], axis=1), jnp.stack([out_oth, out_own], axis=1)
    ).reshape(2048, 384)

    partial = pl.pallas_call(
        attend_kernel,
        in_specs=[SMEM] * 2 + [VMEM] * 5,
        out_specs=VMEM,
        out_shape=jax.ShapeDtypeStruct((8, SPAN, SPAN), BF16),
        scratch_shapes=[
            pltpu.VMEM((8, 2 * SPAN, 128), BF16),
            pltpu.VMEM((8, 80, 2 * SPAN), BF16),
            pltpu.VMEM((8, 3, 128, SPAN), BF16),
            pltpu.VMEM((8, 80, 3 * SPAN), F32),
            pltpu.VMEM((2 * SPAN, 3 * SPAN), BF16),
            pltpu.VMEM((2 * SPAN, 3 * SPAN), BF16),
        ],
        compiler_params=PARAMS,
        name="attend",
    )(plan, fade, queries, query_gate, kv_own, kv_oth, key_gate)
    parts = lax.all_to_all(partial, "z", 0, 0, tiled=True)

    share = pl.pallas_call(
        back_kernel,
        grid=(2,),
        in_specs=[VMEM] * 3 + [pl.BlockSpec((1024, 384), lambda i: (i, 0))],
        out_specs=pl.BlockSpec((SPAN, 1024), lambda i: (0, i)),
        out_shape=jax.ShapeDtypeStruct((SPAN, 2048), BF16),
        scratch_shapes=[pltpu.VMEM((SPAN, 384), BF16)],
        compiler_params=PARAMS,
        name="back",
    )(parts, local, lifted, w_out)
    shares = lax.all_to_all(share.reshape(4, 64, 2048), "tp", 0, 0, tiled=True)
    return jnp.sum(shares.astype(F32), axis=0).astype(BF16)


def solution(mesh):
    finer = Mesh(mesh.devices.reshape(8, 8, 2, mesh.shape["tp"]), ("z", "y", "c", "tp"))
    everyone = ("z", "y", "c", "tp")
    placed = (
        P(everyone, None),
        P(),
        P(SP, "tp"),
        P(SP, "tp"),
        P(SP, "tp"),
        P(SP, "tp"),
        P(SP, "tp"),
        P(SP, "tp"),
        P("tp", SP),
        P("tp", SP),
        P(SP, "tp"),
        P("tp", None),
    )
    return jax.shard_map(
        body, mesh=finer, in_specs=placed, out_specs=P(everyone, None), check_vma=False
    )
```
